128 devices in a mesh: sp: 16 (over z, x), tp: 8 (over y, core).
Axes of the slice: x: 4, y: 4, z: 4, core: 2. Of those that a mesh axis runs over, the one named last changes fastest.
Arguments:
- tokens: bfloat16 [6144, 2048], P('sp', 'tp'), may hold values from -6 to 6
- norm_gain: bfloat16 [2048], replicated, may hold values from 0.099609375 to 1.8984375
- lin_query: bfloat16 [2048, 1024], P(None, 'tp'), may hold values from -0.125 to 0.125
- lin_key: bfloat16 [2048, 1024], P(None, 'tp'), may hold values from -0.125 to 0.125
- lin_value: bfloat16 [2048, 1024], P(None, 'tp'), may hold values from -0.125 to 0.125
- lin_gate: bfloat16 [2048, 1024], P(None, 'tp'), may hold values from -0.125 to 0.125
- gate_down: bfloat16 [2048, 32], replicated, may hold values from -0.125 to 0.125
- gate_up_weight: bfloat16 [32, 1024], replicated, may hold values from -1 to 1
- decay_offset_bias: float32 [6144, 1024], P('sp', 'tp'), may hold values from -16 to 11
- lin_norm_gain: float32 [128], replicated, may hold values from 0.1 to 1.9
- stick_query: bfloat16 [2048, 1024], P(None, 'tp'), may hold values from -0.25 to 0.25
- stick_key: bfloat16 [2048, 1024], P(None, 'tp'), may hold values from -0.25 to 0.25
- stick_value: bfloat16 [2048, 1024], P(None, 'tp'), may hold values from -0.125 to 0.125
- key_bias: bfloat16 [8, 6144], P('tp', 'sp'), may hold values from -20 to -2
- out_linear: bfloat16 [1024, 2048], replicated, may hold values from -0.125 to 0.125
- out_stick: bfloat16 [1024, 2048], replicated, may hold values from -0.125 to 0.125
Outputs:
- mixed: bfloat16 [6144, 2048], P(('sp', 'tp'))
The draws below stay inside these ranges and needn't reach their ends.
All inputs are finite; a program needn't handle non-finite values.
Results may differ from the reference program's by a relative error of at most 0.012.
Values may be sent and summed in bfloat16 or wider, within the bound.
A program may use at most 64 MiB of HBM per device.

```python
import math
import jax
import jax.numpy as jnp
from jax import lax

D = 2048
GH = 8
HS = 8
DK = 128
RANK = 32
BLK = 32
TOK_DEV = 384
SEQUENCE_LENGTH = 6144


def segment_rows(key_segment):
    position_index = jax.random.randint(key_segment, (4,), 0, SEQUENCE_LENGTH)
    return jnp.any(jnp.arange(SEQUENCE_LENGTH)[:, None] == position_index[None, :], axis=1)


def draw_decay_offset_bias(key, part):
    key_rows = jax.random.split(jax.random.fold_in(key, 11), 5)
    slow_heads = jax.random.randint(key_rows[0], (GH,), 0, 2) > 0
    span_count = SEQUENCE_LENGTH // TOK_DEV
    offsets = jax.random.uniform(key_rows[1], (span_count, GH), jnp.float32, -0.7, 0.7)
    span_of = jnp.arange(SEQUENCE_LENGTH) // TOK_DEV
    fast_level = jax.random.uniform(key_rows[2], (GH,), jnp.float32, -0.5, 1.5)
    level = jnp.where(slow_heads, 9.5, fast_level)
    head_wise = level[None, :] + offsets[span_of]
    random_jitter = jax.random.uniform(key_rows[3], (SEQUENCE_LENGTH, GH, DK), jnp.float32, -0.5, 0.5)
    segment_list = segment_rows(key_rows[4]).astype(jnp.float32)
    value_rows = head_wise[:, :, None] + random_jitter - 14.0 * segment_list[:, None, None]
    return value_rows.reshape(SEQUENCE_LENGTH, GH * DK)


def draw_key_bias(key, part):
    key_rows = jax.random.split(jax.random.fold_in(key, 23), 5)
    slow_heads = jax.random.randint(key_rows[0], (HS,), 0, 2) > 0
    span_count = SEQUENCE_LENGTH // TOK_DEV
    offsets = jax.random.uniform(key_rows[1], (HS, span_count), jnp.float32, -0.7, 0.7)
    span_of = jnp.arange(SEQUENCE_LENGTH) // TOK_DEV
    fast_level = jax.random.uniform(key_rows[2], (HS,), jnp.float32, -12.5, -11.5)
    level = jnp.where(slow_heads, -8.0 - math.log(SEQUENCE_LENGTH), fast_level)
    head_wise = level[:, None] + offsets[:, span_of]
    random_jitter = jax.random.uniform(key_rows[3], (HS, SEQUENCE_LENGTH), jnp.float32, -0.5, 0.5)
    segment_list = segment_rows(key_rows[4]).astype(jnp.float32)
    value_rows = head_wise + random_jitter + 8.0 * segment_list[None, :]
    return value_rows.astype(jnp.bfloat16)


def shard_levels(rng, extent, pieces, low, largest):
    factor_of = 1.0
    for axis_at, blocks in pieces:
        draws = jax.random.uniform(jax.random.fold_in(jax.random.fold_in(rng, 6), axis_at), (blocks,), jnp.float32, low / len(pieces), largest / len(pieces))
        factor_of = factor_of * jnp.repeat(jnp.exp(draws), extent[axis_at] // blocks).reshape((-1,) + (1,) * (len(extent) - 1 - axis_at))
    return factor_of


def noise(stream_key, shape, scale, bound, pieces=(), held_as=jnp.bfloat16):
    factor_of = shard_levels(stream_key, shape, pieces, -0.22, 0.18) if pieces else 1.0
    values = jax.random.normal(stream_key, shape, jnp.float32) * scale * factor_of
    return jnp.minimum(jnp.maximum(values, -bound), bound).astype(held_as)


def setup_inputs(seed: int = 0) -> dict:
    splits = jax.random.split(jax.random.key(seed), 17)
    tokens = noise(splits[0], (SEQUENCE_LENGTH, D), 1.0, 6.0, ((0, 16), (1, 8)))
    norm_gain = jnp.clip(1.0 + 0.18 * jax.random.normal(splits[1], (D,), jnp.float32), 0.099609375, 1.8984375).astype(jnp.bfloat16)
    lin_query = noise(splits[2], (D, GH * DK), D ** -0.5, 0.125, ((1, 8),))
    lin_key = noise(splits[3], (D, GH * DK), D ** -0.5, 0.125, ((1, 8),))
    lin_value = noise(splits[4], (D, GH * DK), D ** -0.5, 0.125, ((1, 8),))
    lin_gate = noise(splits[5], (D, GH * DK), D ** -0.5, 0.125, ((1, 8),))
    gate_down = noise(splits[6], (D, RANK), D ** -0.5, 0.125)
    gate_up_weight = noise(splits[7], (RANK, GH * DK), RANK ** -0.5, 1.0)
    decay_offset_bias = draw_decay_offset_bias(jax.random.fold_in(splits[16], 71), 0)
    lin_norm_gain = jnp.clip(1.0 + 0.18 * jax.random.normal(splits[9], (DK,), jnp.float32), 0.1, 1.9)
    stick_query = noise(splits[10], (D, HS * DK), (D // 4) ** -0.5, 0.25, ((1, 8),))
    stick_key = noise(splits[11], (D, HS * DK), (D // 4) ** -0.5, 0.25, ((1, 8),))
    stick_value = noise(splits[12], (D, HS * DK), D ** -0.5, 0.125, ((1, 8),))
    key_bias = draw_key_bias(jax.random.fold_in(splits[16], 71), 0)
    out_linear = noise(splits[14], (GH * DK, D), (GH * DK + HS * DK) ** -0.5, 0.125)
    out_stick = noise(splits[15], (HS * DK, D), (GH * DK + HS * DK) ** -0.5, 0.125)
    return {"tokens": tokens, "norm_gain": norm_gain, "lin_query": lin_query, "lin_key": lin_key, "lin_value": lin_value, "lin_gate": lin_gate, "gate_down": gate_down, "gate_up_weight": gate_up_weight, "decay_offset_bias": decay_offset_bias, "lin_norm_gain": lin_norm_gain, "stick_query": stick_query, "stick_key": stick_key, "stick_value": stick_value, "key_bias": key_bias, "out_linear": out_linear, "out_stick": out_stick}


norm_eps = 1e-06
gate_softness = 16.0

def linear_attention(queries, keys_in, values_in, decay_logarithm, gate_in, head_gain):
    blocks = SEQUENCE_LENGTH // BLK
    highest_precision = lax.Precision.HIGHEST

    def blocked(matrix):
        return matrix.reshape(blocks, BLK, GH, DK).transpose(0, 2, 1, 3)
    causal = jnp.tril(jnp.ones((BLK, BLK), dtype=bool))

    def advance(running_state, inputs):
        query_block, key_block, value_block, decay_blk = inputs
        within_segment = jnp.cumsum(decay_blk, axis=1)
        carried_state = jnp.einsum('cgw,cwz->cgz', query_block * jnp.exp(within_segment), running_state, precision=highest_precision)
        spread = within_segment[:, :, None, :] - within_segment[:, None, :, :]
        fading = jnp.exp(jnp.where(causal[:, :, None], spread, -jnp.inf))
        scores = jnp.einsum('htk,hsk,htsk->hts', query_block, key_block, fading, precision=highest_precision)
        rounded = lax.optimization_barrier(scores.astype(jnp.bfloat16))
        inner = jnp.einsum('hts,hsv->htv', rounded.astype(jnp.float32), value_block.astype(jnp.float32), precision=highest_precision)
        last_position = within_segment[:, -1, :]
        fresh_state = jnp.einsum('iga,igl->ial', key_block * jnp.exp(last_position[:, None, :] - within_segment), value_block.astype(jnp.float32), precision=highest_precision)
        new_state = running_state * jnp.exp(last_position)[:, :, None] + fresh_state
        return (new_state, carried_state + inner)
    scaled_queries = blocked(queries).astype(jnp.float32) * DK ** (-0.5)
    start_state = jnp.zeros((GH, DK, DK), jnp.float32)
    _, outputs = lax.scan(advance, start_state, (scaled_queries, blocked(keys_in).astype(jnp.float32), blocked(values_in), blocked(decay_logarithm)))
    combined = outputs.transpose(0, 2, 1, 3).reshape(SEQUENCE_LENGTH, GH, DK)
    normed = combined * lax.rsqrt(lax.optimization_barrier(jnp.mean(combined * combined, axis=-1, keepdims=True)) + norm_eps) * head_gain
    return (normed.reshape(SEQUENCE_LENGTH, GH * DK) * jax.nn.silu(gate_in.astype(jnp.float32))).astype(jnp.bfloat16)

def stick_attention(queries, keys_in, values_in, key_bias):
    span_count = SEQUENCE_LENGTH // TOK_DEV
    key_pos = jnp.arange(SEQUENCE_LENGTH, dtype=jnp.int32)

    def head_wise(matrix):
        return matrix.reshape(SEQUENCE_LENGTH, HS, DK).transpose(1, 0, 2)

    def one_head(inputs):
        head_query, head_key, head_value, head_bias = inputs
        starts = jnp.arange(span_count, dtype=jnp.int32) * TOK_DEV

        def one_span(span_in):
            span_query, first = span_in
            logits = jnp.dot(span_query, head_key.T, preferred_element_type=jnp.float32) * DK ** (-0.5) + head_bias.astype(jnp.float32)[None, :]
            query_pos = first + jnp.arange(TOK_DEV, dtype=jnp.int32)
            visible = key_pos[None, :] < query_pos[:, None]
            falling = jnp.where(visible, jax.nn.log_sigmoid(-logits), 0.0)
            behind = lax.cumsum(falling, axis=1, reverse=True) - falling
            shares = jnp.where(visible, jnp.exp(jax.nn.log_sigmoid(logits) + behind), 0.0).astype(jnp.bfloat16)
            return jnp.dot(shares, head_value, preferred_element_type=jnp.float32)
        spans = lax.map(one_span, (head_query.reshape(span_count, TOK_DEV, DK), starts))
        return spans.reshape(SEQUENCE_LENGTH, DK)
    heads_out = lax.map(one_head, (head_wise(queries), head_wise(keys_in), head_wise(values_in), key_bias))
    return heads_out.transpose(1, 0, 2).reshape(SEQUENCE_LENGTH, HS * DK).astype(jnp.bfloat16)

def reference(tokens, norm_gain, lin_query, lin_key, lin_value, lin_gate, gate_down, gate_up_weight, decay_offset_bias, lin_norm_gain, stick_query, stick_key, stick_value, key_bias, out_linear, out_stick):
    widened = tokens.astype(jnp.float32)
    inv_rms = lax.rsqrt(lax.optimization_barrier(jnp.mean(widened * widened, axis=1)) + norm_eps)[:, None]
    scaled = (widened * norm_gain.astype(jnp.float32)).astype(jnp.bfloat16)

    def project(weight):
        return (jnp.dot(scaled, weight, preferred_element_type=jnp.float32) * inv_rms).astype(jnp.bfloat16)
    reduced_rank = project(gate_down)
    decay_logarithm = jax.nn.log_sigmoid(jnp.dot(reduced_rank, gate_up_weight, preferred_element_type=jnp.float32) + decay_offset_bias) / gate_softness
    linear_out = linear_attention(project(lin_query), project(lin_key), project(lin_value), decay_logarithm, project(lin_gate), lin_norm_gain)
    stick_out = stick_attention(project(stick_query), project(stick_key), project(stick_value), key_bias)
    total = jnp.dot(linear_out, out_linear, preferred_element_type=jnp.float32) + jnp.dot(stick_out, out_stick, preferred_element_type=jnp.float32)
    return total.astype(jnp.bfloat16)
```

```python
import jax
import jax.numpy as jnp
from jax import lax
from jax.experimental import pallas as pl
from jax.experimental.pallas import tpu as pltpu
from jax.sharding import Mesh
from jax.sharding import PartitionSpec as P

MESH = pl.DeviceIdType.MESH
F32 = jnp.float32
BF16 = jnp.bfloat16
LOG2E = 1.4426950408889634
EPS = 1e-6
SOFT = 16.0
TOK = 384
D = 2048
HD = 128
PARTS = 3
ROWS = TOK // PARTS
CH = TOK // 128
LEVELS = 7
OUT_ROWS = TOK // 8

M_A, M_B, M_P0, M_C, M_D, M_P1, M_P2, M_P3, M_P4 = [PARTS * i for i in range(9)]
M_K = 9 * PARTS
M_SX = M_K + 6
M_Q = M_SX + 4
M_SZ = M_Q + 4
M_PO = M_SZ + 4
M_LA = M_PO + 4
M_ST = M_LA + 8
N_MSG = M_ST + 8


def nt(a, b):
    return lax.dot_general(a, b, (((1,), (1,)), ((), ())), preferred_element_type=F32)


def tn(a, b):
    return lax.dot_general(a, b, (((0,), (0,)), ((), ())), preferred_element_type=F32)


def mm(a, b):
    return jnp.dot(a, b, preferred_element_type=F32)


def iota(shape, dim):
    return lax.broadcasted_iota(jnp.int32, shape, dim)


def split(x):
    hi = x.astype(BF16)
    return hi, (x - hi.astype(F32)).astype(BF16)


def rows_of(pieces):
    io = iota((16, 128), 0)
    out = jnp.zeros((16, 128), F32)
    for r, piece in enumerate(pieces):
        out = jnp.where(io == r, piece.astype(F32), out)
    return out.astype(BF16)


def kernel(
    tokens, gain, w_lq, w_lk, w_lv, w_lg, w_gd, w_gu, dob, lgain, w_sq, w_sk, w_sv, kbias, w_ol, w_os,
    out,
    tok, wbuf, gd, gu, gf, acc, ss, dbuf, kb, lng, ol, os_,
    mcon, tri, kbuf, vbuf, qbuf, lq, lk, lv, lg, lacc, qx, sx, sz, pbuf, tbuf, sbuf, rbuf, stk, ctot,
    linb, stb, xl, xs, oacc,
    lsem, ssem, rsem,
):
    a, b = lax.axis_index("z"), lax.axis_index("x")
    y, c = lax.axis_index("y"), lax.axis_index("c")
    tp = 2 * y + c
    oc = 1 - c

    def local(src, dst, i):
        cp = pltpu.make_async_copy(src, dst, lsem.at[i])
        cp.start()
        return cp

    def remote(src, dst, i, **dev):
        return pltpu.make_async_remote_copy(
            src_ref=src, dst_ref=dst, send_sem=ssem.at[i], recv_sem=rsem.at[i],
            device_id=dev, device_id_type=MESH,
        )

    def arrived(dst, i):
        remote(dst, dst, i, c=oc).wait_recv()

    def sent(src, i):
        remote(src, src, i, c=oc).wait_send()

    base = 4 * y + 2 * c
    loads = [
        local(tokens.at[:, pl.ds(0, 128)], tok.at[base], 0),
        local(tokens.at[:, pl.ds(128, 128)], tok.at[base + 1], 1),
    ]
    weights = [w_sk, w_sv, w_sq, w_lk, w_lv, w_lq, w_lg]
    wloads = [local(w, wbuf.at[:, pl.ds(128 * i, 128)], 2 + i) for i, w in enumerate(weights)]
    gdl = local(w_gd, gd, 9)
    gainl = local(gain, gf, 10)
    kbl = local(kbias, kb, 11)
    gul = local(w_gu.at[:, pl.ds(pl.multiple_of(128 * tp, 128), 128)], gu, 12)
    dobl = local(dob, dbuf, 13)
    lngl = local(lgain, lng, 14)
    oll = local(w_ol, ol, 15)
    osl = local(w_os, os_, 16)

    barrier = pltpu.get_barrier_semaphore()
    for k in range(1, 4):
        pl.semaphore_signal(barrier, inc=1, device_id={"x": lax.rem(b + k, 4)}, device_id_type=MESH)
        pl.semaphore_signal(barrier, inc=1, device_id={"z": lax.rem(a + k, 4)}, device_id_type=MESH)
    for k in range(1, 8):
        r = lax.rem(tp + k, 8)
        pl.semaphore_signal(
            barrier, inc=1, device_id={"y": r // 2, "c": lax.rem(r, 2)}, device_id_type=MESH
        )

    t_i, s_i = iota((128, 128), 0), iota((128, 128), 1)
    for lev in range(LEVELS):
        same = (t_i >> lev) == (s_i >> lev)
        second = ((t_i >> lev) & 1) == 1
        m = jnp.where(same, jnp.where(second, jnp.where(s_i <= t_i, 1.0, 0.0), jnp.where(s_i > t_i, 1.0, 0.0)), 0.0)
        mcon[pl.ds(128 * lev, 128), :] = m.astype(BF16)
    mcon[pl.ds(128 * LEVELS, 128), :] = jnp.where(s_i <= t_i, 1.0, 0.0).astype(BF16)
    mcon[pl.ds(128 * LEVELS + 128, 128), :] = jnp.where(s_i > t_i, 1.0, 0.0).astype(BF16)
    tri[...] = jnp.where(iota((256, 256), 0) > iota((256, 256), 1), 1.0, 0.0).astype(BF16)
    for g in range(4):
        pbuf[g, 0] = jnp.zeros((TOK, HD), F32)
        tbuf[g, 0] = jnp.zeros((TOK, HD), F32)

    for cp in loads:
        cp.wait()
    pl.semaphore_wait(barrier, 13)

    yp, ym, yo = lax.rem(y + 1, 4), lax.rem(y + 3, 4), lax.rem(y + 2, 4)

    def part(first, count, r):
        return tok.at[pl.ds(first, count), pl.ds(ROWS * r, ROWS), :]

    started = []

    def send(src, dst, i, **dev):
        remote(src, dst, i, **dev).start()
        started.append((src, i))

    for r in range(PARTS):
        mine = part(base, 2, r)
        send(mine, mine, M_A + r, y=yp)
        send(mine, mine, M_B + r, y=ym)
        send(mine, mine, M_P0 + r, c=oc)

    gainl.wait()
    kbl.wait()
    kbuf[b, pl.ds(TOK, 16), :] = rows_of([kb[:, pl.ds(128 * r, 128)] for r in range(CH)])
    for cp in wloads:
        cp.wait()
    gdl.wait()
    wbuf[:, pl.ds(896, 128)] = jnp.zeros((D, 128), BF16)
    wbuf[:, pl.ds(896, 32)] = gd[...]

    def scaled(chip, first=False):
        pieces = []
        for j in range(4):
            x = tok[4 * chip + j].astype(F32)
            sq = x * x
            ss[...] = sq if (first and j == 0) else ss[...] + sq
            pieces.append((x * gf[pl.ds(4 * chip + j, 1), :]).astype(BF16))
        return jnp.concatenate(pieces, axis=1)

    def weight_rows(chip):
        return pl.ds(pl.multiple_of(512 * chip, 512), 512)

    def fold(chip, first=False):
        lhs = scaled(chip, first)
        for n in range(4):
            cols = pl.ds(256 * n, 256)
            add = mm(lhs, wbuf[weight_rows(chip), cols])
            acc[:, cols] = add if first else acc[:, cols] + add

    for r in range(PARTS):
        arrived(part(4 * y + 2 * oc, 2, r), M_P0 + r)
    fold(y, True)
    for r in range(PARTS):
        arrived(part(4 * ym + 2 * c, 2, r), M_A + r)
        one = part(4 * ym + 2 * c, 1, r)
        send(one, one, M_C + r, y=yp)
        both = part(4 * ym + 2 * c, 2, r)
        send(both, both, M_P1 + r, c=oc)
        arrived(part(4 * yp + 2 * c, 2, r), M_B + r)
        one = part(4 * yp + 2 * c + 1, 1, r)
        send(one, one, M_D + r, y=ym)
        both = part(4 * yp + 2 * c, 2, r)
        send(both, both, M_P2 + r, c=oc)
    for r in range(PARTS):
        arrived(part(4 * ym + 2 * oc, 2, r), M_P1 + r)
    fold(ym)
    for r in range(PARTS):
        arrived(part(4 * yp + 2 * oc, 2, r), M_P2 + r)
    fold(yp)
    for r in range(PARTS):
        one = part(4 * yo + 2 * c, 1, r)
        arrived(one, M_C + r)
        send(one, one, M_P3 + r, c=oc)
        one = part(4 * yo + 2 * c + 1, 1, r)
        arrived(one, M_D + r)
        send(one, one, M_P4 + r, c=oc)
    for r in range(PARTS):
        arrived(part(4 * yo + 2 * oc, 1, r), M_P3 + r)
        arrived(part(4 * yo + 2 * oc + 1, 1, r), M_P4 + r)

    lhs = scaled(yo)
    inv = lax.rsqrt(jnp.sum(ss[...], axis=1, keepdims=True) * (1.0 / D) + EPS)

    def finish(n):
        cols = pl.ds(256 * n, 256)
        total = acc[:, cols] + mm(lhs, wbuf[weight_rows(yo), cols])
        return (total * inv).astype(BF16)

    xp, xm, xo = lax.rem(b + 1, 4), lax.rem(b + 3, 4), lax.rem(b + 2, 4)
    got = finish(0)
    kbuf[b, pl.ds(0, TOK), :] = got[:, :128]
    vbuf[b] = got[:, 128:]
    send(kbuf.at[b], kbuf.at[b], M_K, x=xp)
    send(kbuf.at[b], kbuf.at[b], M_K + 1, x=xm)
    send(vbuf.at[b], vbuf.at[b], M_K + 2, x=xp)
    send(vbuf.at[b], vbuf.at[b], M_K + 3, x=xm)
    got = finish(1)
    qbuf[0] = got[:, :128]
    lk[...] = got[:, 128:]
    for d in range(1, 4):

        @pl.when(a >= d)
        def _():
            remote(qbuf.at[0], qbuf.at[d], M_Q + d, z=a - d).start()

    got = finish(2)
    lv[...] = got[:, :128]
    lq[...] = got[:, 128:]
    got = finish(3)
    lg[...] = got[:, :128]
    low = got[:, 128:160]

    gul.wait()
    dobl.wait()
    pre = (mm(low, gu[...]) + dbuf[...]) * LOG2E
    decay = (jnp.minimum(pre, 0.0) - jnp.log2(1.0 + jnp.exp2(-jnp.abs(pre)))) * (1.0 / SOFT)
    ghi, glo = split(decay)
    gboth = jnp.concatenate([ghi, glo], axis=1)
    scale = HD ** (-0.5)
    apart = t_i ^ s_i
    state = jnp.zeros((HD, HD), F32)
    before = jnp.zeros((1, HD), F32)
    for n in range(CH):
        rows = slice(128 * n, 128 * n + 128)
        both = mm(mcon[...], gboth[rows])
        dist = both[:, :128] + both[:, 128:]
        fade = jnp.exp2(dist)
        qh, kh, vh = lq[rows, :], lk[rows, :], lv[rows, :]
        qf, kf = qh.astype(F32) * scale, kh.astype(F32)
        score = jnp.where(apart == 0, nt(qh, kh) * scale, 0.0)
        for lev in range(LEVELS):
            e = fade[128 * lev : 128 * lev + 128]
            part_score = nt((qf * e).astype(BF16), (kf * e).astype(BF16))
            score = jnp.where(((apart >> lev) == 1) & (t_i > s_i), part_score, score)
        inner = mm(score.astype(BF16), vh)
        from_start = fade[128 * LEVELS : 128 * LEVELS + 128]
        to_end = fade[128 * LEVELS + 128 :]
        qs = qf * from_start
        if n:
            inner = inner + nt(qs.astype(BF16), state.astype(BF16))
        lacc[rows, :] = inner
        qx[rows, :] = (qs * jnp.exp2(before)).astype(BF16)
        length = dist[128 * LEVELS + 127 : 128 * LEVELS + 128]
        state = state * jnp.exp2(length) + tn(vh, (kf * to_end).astype(BF16))
        before = before + length
    sx[b, pl.ds(0, HD), :] = state.astype(BF16)
    sx[b, pl.ds(HD, 16), :] = rows_of(split(before))
    for k in range(1, 4):
        send(sx.at[b], sx.at[b], M_SX + k, x=lax.rem(b + k, 4))

    def pair(d, g, diagonal):
        head = kbuf[g, pl.ds(TOK, 16), :].astype(F32) * LOG2E
        bias = jnp.concatenate([head[r : r + 1] for r in range(CH)], axis=1)
        z = nt(qbuf[d], kbuf[g, pl.ds(0, TOK), :]) * (scale * LOG2E) + bias
        soft = jnp.maximum(z, 0.0) + jnp.log2(1.0 + jnp.exp2(-jnp.abs(z)))
        own = z - soft
        if diagonal:
            seen = iota((TOK, TOK), 1) < iota((TOK, TOK), 0)
            soft = jnp.where(seen, soft, 0.0)
        sb = soft.astype(BF16)
        near = mm(sb[:, 256:], tri[pl.ds(0, 128), pl.ds(0, 128)])
        near_total = near[:, :1] + soft[:, 256:257]
        far = mm(sb[:, :256], tri[...]) + near_total
        whole = far[:, :1] + soft[:, :1]
        share = jnp.exp2(own - jnp.concatenate([far, near], axis=1))
        if diagonal:
            share = jnp.where(seen, share, 0.0)
        pbuf[g, d] = mm(share.astype(BF16), vbuf[g])
        tbuf[g, d] = jnp.broadcast_to(whole, (TOK, HD))

    def pairs(g, first):
        def body(d, carry):
            pair(d, g, False)
            return carry

        lax.fori_loop(first, 4 - a, body, 0)

    pair(0, b, True)
    for d in range(1, 4):

        @pl.when(a + d <= 3)
        def _():
            arrived(qbuf.at[d], M_Q + d)

    pairs(b, 1)
    arrived(kbuf.at[xm], M_K)
    send(kbuf.at[xm], kbuf.at[xm], M_K + 4, x=xp)
    arrived(kbuf.at[xp], M_K + 1)
    arrived(vbuf.at[xp], M_K + 3)
    send(vbuf.at[xp], vbuf.at[xp], M_K + 5, x=xm)
    arrived(vbuf.at[xm], M_K + 2)
    pairs(xm, jnp.where(xm < b, 0, 1))
    pairs(xp, jnp.where(xp < b, 0, 1))

    for k in range(1, 4):
        arrived(sx.at[lax.rem(b + 4 - k, 4)], M_SX + k)
    run = jnp.zeros((HD, HD), F32)
    run_len = jnp.zeros((1, HD), F32)
    pre_state, pre_len = run, run_len
    for g in range(4):
        pre_state = jnp.where(b == g, run, pre_state)
        pre_len = jnp.where(b == g, run_len, pre_len)
        tail = sx[g, pl.ds(HD, 16), :].astype(F32)
        length = tail[0:1] + tail[1:2]
        run = run * jnp.exp2(length) + sx[g, pl.ds(0, HD), :].astype(F32)
        run_len = run_len + length
    sz[a, pl.ds(0, HD), :] = run.astype(BF16)
    sz[a, pl.ds(HD, 16), :] = rows_of(split(run_len))
    for d in range(1, 4):

        @pl.when(a + d <= 3)
        def _():
            remote(sz.at[a], sz.at[a], M_SZ + d, z=a + d).start()

    arrived(kbuf.at[xo], M_K + 4)
    arrived(vbuf.at[xo], M_K + 5)
    pairs(xo, jnp.where(xo < b, 0, 1))

    def joined(d):
        total = jnp.zeros((TOK, HD), F32)
        behind = jnp.zeros((TOK, HD), F32)
        for g in range(3, -1, -1):
            total = total + jnp.exp2(-behind) * pbuf[g, d]
            behind = behind + tbuf[g, d]
        return total, behind

    for d in (2, 3, 1):

        @pl.when(a + d <= 3)
        def _():
            total, behind = joined(d)
            sbuf[d, pl.ds(0, TOK), :] = total.astype(BF16)
            lines = [jnp.transpose(behind[128 * r : 128 * r + 128])[0:1] for r in range(CH)]
            parts = [split(line) for line in lines]
            sbuf[d, pl.ds(TOK, 16), :] = rows_of([p[0] for p in parts] + [p[1] for p in parts])
            remote(sbuf.at[d], rbuf.at[d], M_PO + d, z=a + d).start()

    for d in range(1, 4):

        @pl.when(a >= d)
        def _():
            arrived(sz.at[a - d], M_SZ + d)

    def add_group(g, carried):
        tail = sz[g, pl.ds(HD, 16), :].astype(F32)
        return carried * jnp.exp2(tail[0:1] + tail[1:2]) + sz[g, pl.ds(0, HD), :].astype(F32)

    older = lax.fori_loop(0, a, add_group, jnp.zeros((HD, HD), F32))
    incoming = pre_state + older * jnp.exp2(pre_len)
    raw = lacc[...] + nt(qx[...], incoming.astype(BF16))
    lngl.wait()
    normed = raw * lax.rsqrt(jnp.mean(raw * raw, axis=1, keepdims=True) + EPS) * lng[...]
    gate = lg[...].astype(F32)
    linb[...] = (normed * (gate / (1.0 + jnp.exp2(gate * (-LOG2E))))).astype(BF16)

    def span(r):
        return pl.ds(pl.multiple_of(OUT_ROWS * r, 16), OUT_ROWS)

    def exchange(src, dst, first):
        for k in range(1, 8):
            r = lax.rem(tp + k, 8)
            send(src.at[span(r)], dst.at[tp], first + k, y=r // 2, c=lax.rem(r, 2))
        dst[tp] = src[span(tp), :]

    def collected(dst, first):
        for k in range(1, 8):
            arrived(dst.at[lax.rem(tp + 8 - k, 8)], first + k)
        return jnp.concatenate([dst[i] for i in range(8)], axis=1)

    exchange(linb, xl, M_LA)
    total, behind = joined(0)
    stk[...] = total
    ctot[...] = behind
    oll.wait()
    lhs = collected(xl, M_LA)
    for n in range(4):
        cols = pl.ds(512 * n, 512)
        oacc[:, cols] = mm(lhs, ol[:, cols])

    for d in range(1, 4):

        @pl.when(a >= d)
        def _():
            arrived(rbuf.at[d], M_PO + d)
            stk[...] += jnp.exp2(-ctot[...]) * rbuf[d, pl.ds(0, TOK), :].astype(F32)
            if d < 3:
                tail = rbuf[d, pl.ds(TOK, 16), :].astype(F32)
                for r in range(CH):
                    line = tail[r : r + 1] + tail[CH + r : CH + r + 1]
                    ctot[pl.ds(128 * r, 128), :] += jnp.transpose(jnp.broadcast_to(line, (128, 128)))

    stb[...] = stk[...].astype(BF16)
    exchange(stb, xs, M_ST)
    osl.wait()
    lhs = collected(xs, M_ST)
    for n in range(4):
        cols = pl.ds(512 * n, 512)
        out[:, cols] = (oacc[:, cols] + mm(lhs, os_[:, cols])).astype(BF16)

    for src, i in started:
        sent(src, i)
    for d in range(1, 4):

        @pl.when(a >= d)
        def _():
            sent(qbuf.at[0], M_Q + d)

        @pl.when(a + d <= 3)
        def _():
            sent(sz.at[a], M_SZ + d)
            sent(sbuf.at[d], M_PO + d)


def per_device(*args):
    args = list(args)
    args[1] = args[1].astype(F32).reshape(16, 128)
    args[9] = args[9].reshape(1, HD)
    vm = pltpu.VMEM
    return pl.pallas_call(
        kernel,
        out_shape=jax.ShapeDtypeStruct((OUT_ROWS, D), BF16),
        in_specs=[pl.BlockSpec(memory_space=pl.ANY)] * 16,
        out_specs=pl.BlockSpec(memory_space=pltpu.VMEM),
        scratch_shapes=[
            vm((16, TOK, 128), BF16),
            vm((D, 1024), BF16),
            vm((D, 32), BF16),
            vm((32, 128), BF16),
            vm((16, 128), F32),
            vm((TOK, 1024), F32),
            vm((TOK, 128), F32),
            vm((TOK, 128), F32),
            vm((1, TOK), BF16),
            vm((1, 128), F32),
            vm((1024, D), BF16),
            vm((1024, D), BF16),
            vm((128 * (LEVELS + 2), 128), BF16),
            vm((256, 256), BF16),
            vm((4, TOK + 16, 128), BF16),
            vm((4, TOK, 128), BF16),
            vm((4, TOK, 128), BF16),
            vm((TOK, 128), BF16),
            vm((TOK, 128), BF16),
            vm((TOK, 128), BF16),
            vm((TOK, 128), BF16),
            vm((TOK, 128), F32),
            vm((TOK, 128), BF16),
            vm((4, 144, 128), BF16),
            vm((4, 144, 128), BF16),
            vm((4, 4, TOK, 128), F32),
            vm((4, 4, TOK, 128), F32),
            vm((4, TOK + 16, 128), BF16),
            vm((4, TOK + 16, 128), BF16),
            vm((TOK, 128), F32),
            vm((TOK, 128), F32),
            vm((TOK, 128), BF16),
            vm((TOK, 128), BF16),
            vm((8, OUT_ROWS, 128), BF16),
            vm((8, OUT_ROWS, 128), BF16),
            vm((OUT_ROWS, D), F32),
            pltpu.SemaphoreType.DMA((17,)),
            pltpu.SemaphoreType.DMA((N_MSG,)),
            pltpu.SemaphoreType.DMA((N_MSG,)),
        ],
        compiler_params=pltpu.CompilerParams(collective_id=0, has_side_effects=True),
        name="layer",
    )(*args)


def solution(mesh):
    torus = Mesh(mesh.devices.reshape(4, 4, 4, 2), ("z", "x", "y", "c"))
    sp, tp = ("z", "x"), ("y", "c")
    placed = (
        P(sp, tp), P(), P(None, tp), P(None, tp), P(None, tp), P(None, tp), P(), P(), P(sp, tp), P(),
        P(None, tp), P(None, tp), P(None, tp), P(tp, sp), P(), P(),
    )
    return jax.shard_map(
        per_device, mesh=torus, in_specs=placed, out_specs=P(sp + tp, None), check_vma=False
    )
```

```python
import jax
import jax.numpy as jnp
from jax import lax
from jax.experimental import pallas as pl
from jax.experimental.pallas import tpu as pltpu
from jax.sharding import Mesh
from jax.sharding import PartitionSpec as P

MESH = pl.DeviceIdType.MESH
F32 = jnp.float32
BF16 = jnp.bfloat16
LOG2E = 1.4426950408889634
EPS = 1e-6
SOFT = 16.0
TOK = 384
D = 2048
HD = 128
PARTS = 3
ROWS = TOK // PARTS
CH = TOK // 128
LEVELS = 7
OUT_ROWS = TOK // 8

M_A0, M_A1, M_B0, M_B1, M_P0, M_C, M_D, M_P1, M_P2, M_P3, M_P4, M_P5, M_P6 = [PARTS * i for i in range(13)]
M_K = 13 * PARTS
M_SX = M_K + 6
M_Q = M_SX + 4
M_SZ = M_Q + 4
M_LA = M_SZ + 4
M_R = M_LA + 8
N_MSG = M_R + 32


PROFILE = False


class Marks:
    current = None

    def __call__(self, name):
        if not PROFILE:
            return
        if self.current is not None:
            self.current.__exit__(None, None, None)
        self.current = jax.named_scope(name) if name else None
        if name:
            self.current.__enter__()


def nt(a, b):
    return lax.dot_general(a, b, (((1,), (1,)), ((), ())), preferred_element_type=F32)


def tn(a, b):
    return lax.dot_general(a, b, (((0,), (0,)), ((), ())), preferred_element_type=F32)


def mm(a, b):
    return jnp.dot(a, b, preferred_element_type=F32)


def iota(shape, dim):
    return lax.broadcasted_iota(jnp.int32, shape, dim)


def split(x):
    hi = x.astype(BF16)
    return hi, (x - hi.astype(F32)).astype(BF16)


def rows_of(pieces):
    io = iota((16, 128), 0)
    out = jnp.zeros((16, 128), F32)
    for r, piece in enumerate(pieces):
        out = jnp.where(io == r, piece.astype(F32), out)
    return out.astype(BF16)


def kernel(
    tokens, gain, w_lq, w_lk, w_lv, w_lg, w_gd, w_gu, dob, lgain, w_sq, w_sk, w_sv, kbias, w_ol, w_os,
    out,
    tok, wbuf, gd, gu, gb, gf, acc, ss, dbuf, kb, lng, ol, os_,
    mcon, tri, kbuf, vbuf, qbuf, lq, lk, lv, lg, gs, ffrom, fall, sthis, lacc, qx, sx, sz, pbuf, tbuf, sbuf, rbuf,
    linb, xl, oacc,
    lsem, ssem, rsem,
):
    mark = Marks()
    a, b = lax.axis_index("z"), lax.axis_index("x")
    y, c = lax.axis_index("y"), lax.axis_index("c")
    tp = 2 * y + c
    oc = 1 - c
    scale = HD ** (-0.5)

    def local(src, dst, i):
        cp = pltpu.make_async_copy(src, dst, lsem.at[i])
        cp.start()
        return cp

    def remote(src, dst, i, **dev):
        return pltpu.make_async_remote_copy(
            src_ref=src, dst_ref=dst, send_sem=ssem.at[i], recv_sem=rsem.at[i],
            device_id=dev, device_id_type=MESH,
        )

    def arrived(dst, i):
        remote(dst, dst, i, c=oc).wait_recv()

    def sent(src, i):
        remote(src, src, i, c=oc).wait_send()

    started = []

    def send(src, dst, i, **dev):
        remote(src, dst, i, **dev).start()
        started.append((src, i))

    mark("load")
    base = 4 * y + 2 * c
    loads = [
        local(tokens.at[:, pl.ds(0, 128)], tok.at[base], 0),
        local(tokens.at[:, pl.ds(128, 128)], tok.at[base + 1], 1),
    ]
    barrier = pltpu.get_barrier_semaphore()
    for k in range(1, 4):
        pl.semaphore_signal(barrier, inc=1, device_id={"x": lax.rem(b + k, 4)}, device_id_type=MESH)
        pl.semaphore_signal(barrier, inc=1, device_id={"z": lax.rem(a + k, 4)}, device_id_type=MESH)
    for k in range(1, 8):
        r = lax.rem(tp + k, 8)
        pl.semaphore_signal(
            barrier, inc=1, device_id={"y": r // 2, "c": lax.rem(r, 2)}, device_id_type=MESH
        )
    weights = [w_sk, w_sq, w_sv, w_lk, w_lv, None, w_lq, w_lg]
    wloads = [
        local(w, wbuf.at[:, pl.ds(128 * i, 128)], 2 + i) for i, w in enumerate(weights) if w is not None
    ]
    gdl = local(w_gd, gd, 7)
    gainl = local(gain, gb, 10)
    kbl = local(kbias, kb, 11)
    gul = local(w_gu.at[:, pl.ds(pl.multiple_of(128 * tp, 128), 128)], gu, 12)
    dobl = local(dob, dbuf, 13)
    lngl = local(lgain, lng, 14)
    oll = local(w_ol, ol, 15)
    osl = local(w_os, os_, 16)

    t_i, s_i = iota((128, 128), 0), iota((128, 128), 1)
    mcon[pl.ds(0, 128), :] = jnp.where(s_i <= t_i, 1.0, 0.0).astype(BF16)
    mcon[pl.ds(128, 128), :] = jnp.where(s_i > t_i, 1.0, 0.0).astype(BF16)
    mark("barrier")
    for cp in loads:
        cp.wait()
    pl.semaphore_wait(barrier, 13)

    mark("send")
    yp, ym, yo = lax.rem(y + 1, 4), lax.rem(y + 3, 4), lax.rem(y + 2, 4)

    def part(first, count, r):
        return tok.at[pl.ds(first, count), pl.ds(ROWS * r, ROWS), :]

    def send_part(first, count, r, m, **dev):
        ref = part(first, count, r)
        send(ref, ref, m + r, **dev)

    for r in range(PARTS):
        send_part(base, 1, r, M_A0, y=yp)
        send_part(base + 1, 1, r, M_B1, y=ym)
    for r in range(PARTS):
        send_part(base, 2, r, M_P0, c=oc)
    send_part(base + 1, 1, 0, M_A1, y=yp)
    send_part(base, 1, 0, M_B0, y=ym)

    for lev in range(LEVELS):
        same = (t_i >> lev) == (s_i >> lev)
        second = ((t_i >> lev) & 1) == 1
        m = jnp.where(same, jnp.where(second, jnp.where(s_i <= t_i, 1.0, 0.0), jnp.where(s_i > t_i, 1.0, 0.0)), 0.0)
        mcon[pl.ds(256 + 128 * lev, 128), :] = m.astype(BF16)
    tri[...] = jnp.where(iota((256, 256), 0) > iota((256, 256), 1), 1.0, 0.0).astype(BF16)
    for g in range(4):
        pbuf[g, 0] = jnp.zeros((TOK, HD), F32)
        tbuf[g, 0] = jnp.zeros((TOK, HD), F32)
    gainl.wait()
    gf[...] = gb[...].astype(F32)
    kbl.wait()
    kbuf[b, pl.ds(TOK, 16), :] = rows_of([kb[:, pl.ds(128 * r, 128)] for r in range(CH)])
    gdl.wait()
    for i in range(16):
        down = gd[:, pl.ds(128 * i, 128)].astype(F32)
        square = jnp.concatenate([down, jnp.zeros((96, 128), F32)], axis=0)
        wbuf[pl.ds(128 * i, 128), pl.ds(640, 128)] = jnp.transpose(square).astype(BF16)
    for cp in wloads:
        cp.wait()

    def scaled(chip, first=False):
        pieces = []
        for j in range(4):
            x = tok[4 * chip + j].astype(F32)
            sq = x * x
            ss[...] = sq if (first and j == 0) else ss[...] + sq
            pieces.append((x * gf[pl.ds(4 * chip + j, 1), :]).astype(BF16))
        return jnp.concatenate(pieces, axis=1)

    def weight_rows(chip):
        return pl.ds(pl.multiple_of(512 * chip, 512), 512)

    def fold(chip, first=False):
        lhs = scaled(chip, first)
        for n in range(4):
            cols = pl.ds(256 * n, 256)
            add = mm(lhs, wbuf[weight_rows(chip), cols])
            acc[:, cols] = add if first else acc[:, cols] + add

    mark("own")
    for r in range(PARTS):
        arrived(part(4 * y + 2 * oc, 2, r), M_P0 + r)
    fold(y, True)
    mark("fwd")
    for r in range(PARTS):
        arrived(part(4 * ym + 2 * c, 1, r), M_A0 + r)
        send_part(4 * ym + 2 * c, 1, r, M_C, y=yp)
        arrived(part(4 * yp + 2 * c + 1, 1, r), M_B1 + r)
        send_part(4 * yp + 2 * c + 1, 1, r, M_D, y=ym)
        if r + 1 < PARTS:
            send_part(base + 1, 1, r + 1, M_A1, y=yp)
            send_part(base, 1, r + 1, M_B0, y=ym)
        send_part(4 * ym + 2 * c, 1, r, M_P1, c=oc)
        send_part(4 * yp + 2 * c + 1, 1, r, M_P2, c=oc)
    mark("fwd1")
    for r in range(PARTS):
        arrived(part(4 * ym + 2 * c + 1, 1, r), M_A1 + r)
        send_part(4 * ym + 2 * c + 1, 1, r, M_P3, c=oc)
        arrived(part(4 * yp + 2 * c, 1, r), M_B0 + r)
        send_part(4 * yp + 2 * c, 1, r, M_P4, c=oc)
        if r + 1 < PARTS:
            arrived(part(4 * yo + 2 * c, 1, r), M_C + r)
            send_part(4 * yo + 2 * c, 1, r, M_P5, c=oc)
            arrived(part(4 * yo + 2 * c + 1, 1, r), M_D + r)
            send_part(4 * yo + 2 * c + 1, 1, r, M_P6, c=oc)
    mark("fold2")
    for r in range(PARTS):
        arrived(part(4 * ym + 2 * oc, 1, r), M_P1 + r)
        arrived(part(4 * ym + 2 * oc + 1, 1, r), M_P3 + r)
    fold(ym)
    r = PARTS - 1
    arrived(part(4 * yo + 2 * c, 1, r), M_C + r)
    send_part(4 * yo + 2 * c, 1, r, M_P5, c=oc)
    arrived(part(4 * yo + 2 * c + 1, 1, r), M_D + r)
    send_part(4 * yo + 2 * c + 1, 1, r, M_P6, c=oc)
    for r in range(PARTS):
        arrived(part(4 * yp + 2 * oc, 1, r), M_P4 + r)
        arrived(part(4 * yp + 2 * oc + 1, 1, r), M_P2 + r)
    fold(yp)
    mark("fwd2")
    for r in range(PARTS):
        arrived(part(4 * yo + 2 * oc, 1, r), M_P5 + r)
        arrived(part(4 * yo + 2 * oc + 1, 1, r), M_P6 + r)

    mark("finish")
    lhs = scaled(yo)
    inv = lax.rsqrt(jnp.sum(ss[...], axis=1, keepdims=True) * (1.0 / D) + EPS)

    def finish(n):
        cols = pl.ds(256 * n, 256)
        total = acc[:, cols] + mm(lhs, wbuf[weight_rows(yo), cols])
        return (total * inv).astype(BF16)

    xp, xm, xo = lax.rem(b + 1, 4), lax.rem(b + 3, 4), lax.rem(b + 2, 4)
    got = finish(0)
    kbuf[b, pl.ds(0, TOK), :] = got[:, :128]
    qbuf[0] = got[:, 128:]
    send(kbuf.at[b], kbuf.at[b], M_K, x=xp)
    send(kbuf.at[b], kbuf.at[b], M_K + 1, x=xm)

    @pl.when(a >= 1)
    def _():
        remote(qbuf.at[0], qbuf.at[1], M_Q + 1, z=a - 1).start()

    @pl.when(a == 3)
    def _():
        remote(qbuf.at[0], qbuf.at[3], M_Q + 3, z=0).start()

    got = finish(1)
    vbuf[b] = got[:, :128]
    lk[...] = got[:, 128:]
    send(vbuf.at[b], vbuf.at[b], M_K + 3, x=xm)
    send(vbuf.at[b], vbuf.at[b], M_K + 2, x=xp)
    got = finish(2)
    lv[...] = got[:, :128]
    low = got[:, 128:160]
    got = finish(3)
    lq[...] = got[:, :128]
    lg[...] = got[:, 128:]

    mark("lstate")
    gul.wait()
    dobl.wait()
    pre = (mm(low, gu[...]) + dbuf[...]) * LOG2E
    decay = (jnp.minimum(pre, 0.0) - jnp.log2(1.0 + jnp.exp2(-jnp.abs(pre)))) * (1.0 / SOFT)
    ghi, glo = split(decay)
    gboth = jnp.concatenate([ghi, glo], axis=1)
    gs[...] = gboth
    state = jnp.zeros((HD, HD), F32)
    before = jnp.zeros((1, HD), F32)
    for n in range(CH):
        rows = slice(128 * n, 128 * n + 128)
        both = mm(mcon[pl.ds(0, 256), :], gboth[rows])
        dist = both[:, :128] + both[:, 128:]
        fade = jnp.exp2(dist)
        ffrom[rows, :] = fade[:128]
        fall[rows, :] = fade[:128] * jnp.exp2(before)
        if n:
            sthis[n] = state.astype(BF16)
        length = dist[127:128]
        ke = (lk[rows, :].astype(F32) * fade[128:]).astype(BF16)
        state = state * jnp.exp2(length) + tn(lv[rows, :], ke)
        before = before + length
    sx[b, pl.ds(0, HD), :] = state.astype(BF16)
    sx[b, pl.ds(HD, 16), :] = rows_of(split(before))
    for k in range(1, 4):
        send(sx.at[b], sx.at[b], M_SX + k, x=lax.rem(b + k, 4))

    def linear_inside():
        apart = t_i ^ s_i
        for n in range(CH):
            rows = slice(128 * n, 128 * n + 128)
            both = mm(mcon[pl.ds(256, 128 * LEVELS), :], gs[rows, :])
            fade = jnp.exp2(both[:, :128] + both[:, 128:])
            qh, kh, vh = lq[rows, :], lk[rows, :], lv[rows, :]
            qf, kf = qh.astype(F32) * scale, kh.astype(F32)
            score = jnp.where(apart == 0, nt(qh, kh) * scale, 0.0)
            for lev in range(LEVELS):
                e = fade[128 * lev : 128 * lev + 128]
                part_score = nt((qf * e).astype(BF16), (kf * e).astype(BF16))
                score = jnp.where(((apart >> lev) == 1) & (t_i > s_i), part_score, score)
            inner = mm(score.astype(BF16), vh)
            if n:
                inner = inner + nt((qf * ffrom[rows, :]).astype(BF16), sthis[n])
            lacc[rows, :] = inner
            qx[rows, :] = (qf * fall[rows, :]).astype(BF16)

    mark("diag")
    def bias_of(g):
        head = kbuf[g, pl.ds(TOK, 16), :].astype(F32) * LOG2E
        return jnp.concatenate([head[r : r + 1] for r in range(CH)], axis=1)

    def pair(d, g, diagonal=False):
        z = nt(qbuf[d], kbuf[g, pl.ds(0, TOK), :]) * (scale * LOG2E) + bias_of(g)
        soft = jnp.maximum(jnp.log2(1.0 + jnp.exp2(jnp.minimum(z, 126.0))), z)
        own = z - soft
        if diagonal:
            seen = iota((TOK, TOK), 1) < iota((TOK, TOK), 0)
            soft = jnp.where(seen, soft, 0.0)
        sb = soft.astype(BF16)
        near = mm(sb[:, 256:], tri[pl.ds(0, 128), pl.ds(0, 128)])
        near_total = near[:, :1] + soft[:, 256:257]
        far = mm(sb[:, :256], tri[...]) + near_total
        whole = far[:, :1] + soft[:, :1]
        share = jnp.exp2(own - jnp.concatenate([far, near], axis=1))
        if diagonal:
            share = jnp.where(seen, share, 0.0)
        pbuf[g, d] = mm(share.astype(BF16), vbuf[g])
        tbuf[g, d] = jnp.broadcast_to(whole, (TOK, HD))

    pair(0, b, True)

    mark("linear1")

    @pl.when(a >= 1)
    def _():
        linear_inside()

    mark("qwait")

    @pl.when(a <= 2)
    def _():
        arrived(qbuf.at[1], M_Q + 1)

    @pl.when((a >= 1) & (a <= 2))
    def _():
        remote(qbuf.at[1], qbuf.at[2], M_Q + 2, z=a - 1).start()

    @pl.when(a <= 2)
    def _():
        pair(1, b)

    mark("kvwait")
    arrived(kbuf.at[xm], M_K)
    send(kbuf.at[xm], kbuf.at[xm], M_K + 4, x=xp)
    arrived(kbuf.at[xp], M_K + 1)
    arrived(vbuf.at[xp], M_K + 3)
    send(vbuf.at[xp], vbuf.at[xp], M_K + 5, x=xm)
    arrived(vbuf.at[xm], M_K + 2)

    mark("pairs1")

    def both_pairs(d, carry):
        pair(d, xm)
        pair(d, xp)
        return carry

    lax.fori_loop(0, jnp.where(a <= 2, 2, 1), both_pairs, 0)

    mark("states")
    for k in range(1, 4):
        arrived(sx.at[lax.rem(b + 4 - k, 4)], M_SX + k)
    run = jnp.zeros((HD, HD), F32)
    run_len = jnp.zeros((1, HD), F32)
    pre_state, pre_len = run, run_len
    for g in range(4):
        pre_state = jnp.where(b == g, run, pre_state)
        pre_len = jnp.where(b == g, run_len, pre_len)
        tail = sx[g, pl.ds(HD, 16), :].astype(F32)
        length = tail[0:1] + tail[1:2]
        run = run * jnp.exp2(length) + sx[g, pl.ds(0, HD), :].astype(F32)
        run_len = run_len + length
    sz[a, pl.ds(0, HD), :] = run.astype(BF16)
    sz[a, pl.ds(HD, 16), :] = rows_of(split(run_len))
    for d in range(1, 4):

        @pl.when(a + d <= 3)
        def _():
            remote(sz.at[a], sz.at[a], M_SZ + d, z=a + d).start()

    mark("pairs2")
    for d in (3, 2):

        @pl.when(a + d <= 3)
        def _():
            arrived(qbuf.at[d], M_Q + d)
            pair(d, b)

    lax.fori_loop(2, jnp.where(a <= 1, 4 - a, 2), both_pairs, 0)
    mark("kvwait2")
    arrived(kbuf.at[xo], M_K + 4)
    arrived(vbuf.at[xo], M_K + 5)
    mark("pairs3")

    lane = iota((16, 128), 1)

    def hand_on(d):
        total = jnp.zeros((TOK, HD), F32)
        behind = jnp.zeros((TOK, HD), F32)
        for g in range(3, -1, -1):
            counts = (g <= b) if d == 0 else True
            weight = jnp.exp2(-behind)
            total = total + (jnp.where(counts, weight * pbuf[g, d], 0.0) if d == 0 else weight * pbuf[g, d])
            behind = behind + (jnp.where(counts, tbuf[g, d], 0.0) if d == 0 else tbuf[g, d])
        tiles = []
        for r in range(CH):
            line = jnp.transpose(behind[128 * r : 128 * r + 128])[0:1]
            tiles.append(rows_of(split(line)).astype(F32))
        for r in range(8):
            j, o = (OUT_ROWS * r) // 128, (OUT_ROWS * r) % 128
            tail = pltpu.roll(tiles[j], 128 - o, 1) if o else tiles[j]
            if o + OUT_ROWS > 128:
                tail = jnp.where(lane < 128 - o, tail, pltpu.roll(tiles[j + 1], 128 - o, 1))
            sbuf[d, r, pl.ds(0, OUT_ROWS), :] = total[OUT_ROWS * r : OUT_ROWS * r + OUT_ROWS].astype(BF16)
            sbuf[d, r, pl.ds(OUT_ROWS, 16), :] = tail.astype(BF16)
        for k in range(8):
            r = lax.rem(tp + k, 8)
            if d == 0 and k == 0:
                rbuf[0, tp] = sbuf[0, tp]
            else:
                dev = {"y": r // 2, "c": lax.rem(r, 2)}
                if d:
                    dev["z"] = a + d
                remote(sbuf.at[d, r], rbuf.at[d, tp], M_R + 8 * d + k, **dev).start()

    for d in (2, 3, 1):

        @pl.when(a + d <= 3)
        def _():
            pair(d, xo)
            hand_on(d)

    @pl.when(xo < b)
    def _():
        pair(0, xo)

    hand_on(0)
    mark("linear2")

    @pl.when(a == 0)
    def _():
        linear_inside()

    mark("linfin")
    for d in range(1, 4):

        @pl.when(a >= d)
        def _():
            arrived(sz.at[a - d], M_SZ + d)

    def add_group(g, carried):
        tail = sz[g, pl.ds(HD, 16), :].astype(F32)
        return carried * jnp.exp2(tail[0:1] + tail[1:2]) + sz[g, pl.ds(0, HD), :].astype(F32)

    older = lax.fori_loop(0, a, add_group, jnp.zeros((HD, HD), F32))
    incoming = pre_state + older * jnp.exp2(pre_len)
    raw = lacc[...] + nt(qx[...], incoming.astype(BF16))
    lngl.wait()
    normed = raw * lax.rsqrt(jnp.mean(raw * raw, axis=1, keepdims=True) + EPS) * lng[...]
    gate = lg[...].astype(F32)
    linb[...] = (normed * (gate / (1.0 + jnp.exp2(gate * (-LOG2E))))).astype(BF16)

    def span(r):
        return pl.ds(pl.multiple_of(OUT_ROWS * r, 16), OUT_ROWS)

    mark("linx")
    for k in range(1, 8):
        r = lax.rem(tp + k, 8)
        send(linb.at[span(r)], xl.at[tp], M_LA + k, y=r // 2, c=lax.rem(r, 2))
    xl[tp] = linb[span(tp), :]
    oll.wait()
    for k in range(1, 8):
        arrived(xl.at[lax.rem(tp + 8 - k, 8)], M_LA + k)
    mark("linproj")
    lhs = jnp.concatenate([xl[i] for i in range(8)], axis=1)
    for n in range(4):
        cols = pl.ds(512 * n, 512)
        oacc[:, cols] = mm(lhs, ol[:, cols])

    mark("ret0")
    osl.wait()
    for k in range(1, 8):
        arrived(rbuf.at[0, lax.rem(tp + 8 - k, 8)], M_R + k)
    mark("ret")
    for d in range(1, 4):

        @pl.when(a >= d)
        def _():
            for k in range(8):
                arrived(rbuf.at[d, lax.rem(tp + 8 - k, 8)], M_R + 8 * d + k)

    mark("stproj")
    sub = iota((8, 128), 0)
    behind = jnp.zeros((8, 128), F32)
    heads = [rbuf[0, i, pl.ds(0, OUT_ROWS), :].astype(F32) for i in range(8)]
    for d in range(1, 4):
        for i in range(8):
            tail = rbuf[d - 1, i, pl.ds(OUT_ROWS, 16), :].astype(F32)
            behind = behind + jnp.where(sub == i, tail[0:1] + tail[1:2], 0.0)
        left = jnp.transpose(jnp.exp2(-behind))
        for i in range(8):
            more = left[:OUT_ROWS, i : i + 1] * rbuf[d, i, pl.ds(0, OUT_ROWS), :].astype(F32)
            heads[i] = heads[i] + jnp.where(a >= d, more, 0.0)
    lhs = jnp.concatenate([h.astype(BF16) for h in heads], axis=1)
    for n in range(4):
        cols = pl.ds(512 * n, 512)
        out[:, cols] = (oacc[:, cols] + mm(lhs, os_[:, cols])).astype(BF16)

    mark("drain")
    for src, i in started:
        sent(src, i)

    @pl.when(a >= 1)
    def _():
        sent(qbuf.at[0], M_Q + 1)

    @pl.when(a == 3)
    def _():
        sent(qbuf.at[0], M_Q + 3)

    @pl.when((a >= 1) & (a <= 2))
    def _():
        sent(qbuf.at[1], M_Q + 2)

    for d in range(4):

        @pl.when(a + d <= 3)
        def _():
            if d:
                sent(sz.at[a], M_SZ + d)
            for k in range(0 if d else 1, 8):
                sent(sbuf.at[d, lax.rem(tp + k, 8)], M_R + 8 * d + k)

    mark("")


def per_device(*args):
    args = list(args)
    args[1] = args[1].reshape(16, 128)
    args[6] = args[6].T
    args[9] = args[9].reshape(1, HD)
    vm = pltpu.VMEM
    return pl.pallas_call(
        kernel,
        out_shape=pltpu.VMEM((OUT_ROWS, D), BF16),
        in_specs=[pl.BlockSpec(memory_space=pl.ANY)] * 16,
        out_specs=pl.BlockSpec(memory_space=pltpu.VMEM),
        scratch_shapes=[
            vm((16, TOK, 128), BF16),
            vm((D, 1024), BF16),
            vm((32, D), BF16),
            vm((32, 128), BF16),
            vm((16, 128), BF16),
            vm((16, 128), F32),
            vm((TOK, 1024), F32),
            vm((TOK, 128), F32),
            vm((TOK, 128), F32),
            vm((1, TOK), BF16),
            vm((1, 128), F32),
            vm((1024, D), BF16),
            vm((1024, D), BF16),
            vm((128 * (LEVELS + 2), 128), BF16),
            vm((256, 256), BF16),
            vm((4, TOK + 16, 128), BF16),
            vm((4, TOK, 128), BF16),
            vm((4, TOK, 128), BF16),
            vm((TOK, 128), BF16),
            vm((TOK, 128), BF16),
            vm((TOK, 128), BF16),
            vm((TOK, 128), BF16),
            vm((TOK, 256), BF16),
            vm((TOK, 128), F32),
            vm((TOK, 128), F32),
            vm((CH, 128, 128), BF16),
            vm((TOK, 128), F32),
            vm((TOK, 128), BF16),
            vm((4, 144, 128), BF16),
            vm((4, 144, 128), BF16),
            vm((4, 4, TOK, 128), F32),
            vm((4, 4, TOK, 128), F32),
            vm((4, 8, OUT_ROWS + 16, 128), BF16),
            vm((4, 8, OUT_ROWS + 16, 128), BF16),
            vm((TOK, 128), BF16),
            vm((8, OUT_ROWS, 128), BF16),
            vm((OUT_ROWS, D), F32),
            pltpu.SemaphoreType.DMA((17,)),
            pltpu.SemaphoreType.DMA((N_MSG,)),
            pltpu.SemaphoreType.DMA((N_MSG,)),
        ],
        compiler_params=pltpu.CompilerParams(collective_id=0, has_side_effects=True),
        name="layer",
    )(*args)


def solution(mesh):
    torus = Mesh(mesh.devices.reshape(4, 4, 4, 2), ("z", "x", "y", "c"))
    sp, tp = ("z", "x"), ("y", "c")
    placed = (
        P(sp, tp), P(), P(None, tp), P(None, tp), P(None, tp), P(None, tp), P(), P(), P(sp, tp), P(),
        P(None, tp), P(None, tp), P(None, tp), P(tp, sp), P(), P(),
    )
    return jax.shard_map(
        per_device, mesh=torus, in_specs=placed, out_specs=P(sp + tp, None), check_vma=False
    )
```

```python
import jax
import jax.numpy as jnp
from jax import lax
from jax.experimental import pallas as pl
from jax.experimental.pallas import tpu as pltpu
from jax.sharding import Mesh
from jax.sharding import PartitionSpec as P

MESH = pl.DeviceIdType.MESH
F32 = jnp.float32
BF16 = jnp.bfloat16
LOG2E = 1.4426950408889634
EPS = 1e-6
SOFT = 16.0
TOK = 384
D = 2048
HD = 128
PARTS = 3
ROWS = TOK // PARTS
KPARTS = 2
KROWS = TOK // KPARTS
CH = TOK // 128
LEVELS = 7
OUT_ROWS = TOK // 8

M_A0, M_A1, M_B0, M_B1, M_P0, M_C, M_D, M_P1, M_P2, M_P3, M_P4, M_P5, M_P6 = [PARTS * i for i in range(13)]
M_K = 13 * PARTS
M_SX = M_K + 6 * KPARTS
M_Q = M_SX + 4
M_SZ = M_Q + 4 * KPARTS
M_LA = M_SZ + 4
M_R = M_LA + 8
N_MSG = M_R + 32


PROFILE = False


class Marks:
    current = None

    def __call__(self, name):
        if not PROFILE:
            return
        if self.current is not None:
            self.current.__exit__(None, None, None)
        self.current = jax.named_scope(name) if name else None
        if name:
            self.current.__enter__()


def nt(a, b):
    return lax.dot_general(a, b, (((1,), (1,)), ((), ())), preferred_element_type=F32)


def tn(a, b):
    return lax.dot_general(a, b, (((0,), (0,)), ((), ())), preferred_element_type=F32)


def mm(a, b):
    return jnp.dot(a, b, preferred_element_type=F32)


def iota(shape, dim):
    return lax.broadcasted_iota(jnp.int32, shape, dim)


def split(x):
    hi = x.astype(BF16)
    return hi, (x - hi.astype(F32)).astype(BF16)


def rows_of(pieces):
    io = iota((16, 128), 0)
    out = jnp.zeros((16, 128), F32)
    for r, piece in enumerate(pieces):
        out = jnp.where(io == r, piece.astype(F32), out)
    return out.astype(BF16)


def kernel(
    tokens, gain, w_lq, w_lk, w_lv, w_lg, w_gd, w_gu, dob, lgain, w_sq, w_sk, w_sv, kbias, w_ol, w_os,
    out,
    tok, wbuf, gd, gu, gb, gf, acc, ss, dbuf, kb, lng, ol, os_,
    mcon, tri, kbuf, vbuf, qbuf, lq, lk, lv, lg, gs, ffrom, fall, sthis, lacc, qx, sx, sz, pbuf, tbuf, sbuf, rbuf,
    linb, xl, oacc,
    lsem, ssem, rsem,
):
    mark = Marks()
    a, b = lax.axis_index("z"), lax.axis_index("x")
    y, c = lax.axis_index("y"), lax.axis_index("c")
    tp = 2 * y + c
    oc = 1 - c
    scale = HD ** (-0.5)

    def local(src, dst, i):
        cp = pltpu.make_async_copy(src, dst, lsem.at[i])
        cp.start()
        return cp

    def remote(src, dst, i, **dev):
        return pltpu.make_async_remote_copy(
            src_ref=src, dst_ref=dst, send_sem=ssem.at[i], recv_sem=rsem.at[i],
            device_id=dev, device_id_type=MESH,
        )

    def arrived(dst, i):
        remote(dst, dst, i, c=oc).wait_recv()

    def sent(src, i):
        remote(src, src, i, c=oc).wait_send()

    started = []

    def send(src, dst, i, **dev):
        remote(src, dst, i, **dev).start()
        started.append((src, i))

    mark("load")
    base = 4 * y + 2 * c
    loads = [
        local(tokens.at[:, pl.ds(0, 128)], tok.at[base], 0),
        local(tokens.at[:, pl.ds(128, 128)], tok.at[base + 1], 1),
    ]
    barrier = pltpu.get_barrier_semaphore()
    for k in range(1, 4):
        pl.semaphore_signal(barrier, inc=1, device_id={"x": lax.rem(b + k, 4)}, device_id_type=MESH)

    @pl.when(a <= 2)
    def _():
        pl.semaphore_signal(barrier, inc=1, device_id={"z": a + 1}, device_id_type=MESH)

    @pl.when(a == 0)
    def _():
        pl.semaphore_signal(barrier, inc=1, device_id={"z": 3}, device_id_type=MESH)

    for k in range(1, 8):
        r = lax.rem(tp + k, 8)
        pl.semaphore_signal(
            barrier, inc=1, device_id={"y": r // 2, "c": lax.rem(r, 2)}, device_id_type=MESH
        )
    weights = [w_sk, w_sq, w_sv, w_lk, w_lv, None, w_lq, w_lg]
    wloads = [
        local(w, wbuf.at[:, pl.ds(128 * i, 128)], 2 + i) for i, w in enumerate(weights) if w is not None
    ]
    gdl = local(w_gd, gd, 7)
    gainl = local(gain, gb, 10)
    kbl = local(kbias, kb, 11)
    gul = local(w_gu.at[:, pl.ds(pl.multiple_of(128 * tp, 128), 128)], gu, 12)
    dobl = local(dob, dbuf, 13)
    lngl = local(lgain, lng, 14)
    oll = local(w_ol, ol, 15)
    osl = local(w_os, os_, 16)

    t_i, s_i = iota((128, 128), 0), iota((128, 128), 1)
    mcon[pl.ds(0, 128), :] = jnp.where(s_i <= t_i, 1.0, 0.0).astype(BF16)
    mcon[pl.ds(128, 128), :] = jnp.where(s_i > t_i, 1.0, 0.0).astype(BF16)
    mark("barrier")
    for cp in loads:
        cp.wait()
    pl.semaphore_wait(barrier, 10 + (a + 1) // 2)

    mark("send")
    yp, ym, yo = lax.rem(y + 1, 4), lax.rem(y + 3, 4), lax.rem(y + 2, 4)

    def part(first, count, r):
        return tok.at[pl.ds(first, count), pl.ds(ROWS * r, ROWS), :]

    def send_part(first, count, r, m, **dev):
        ref = part(first, count, r)
        send(ref, ref, m + r, **dev)

    for r in range(PARTS):
        send_part(base, 1, r, M_A0, y=yp)
        send_part(base + 1, 1, r, M_B1, y=ym)
    for r in range(PARTS):
        send_part(base, 2, r, M_P0, c=oc)
    send_part(base + 1, 1, 0, M_A1, y=yp)
    send_part(base, 1, 0, M_B0, y=ym)

    for lev in range(LEVELS):
        same = (t_i >> lev) == (s_i >> lev)
        second = ((t_i >> lev) & 1) == 1
        m = jnp.where(same, jnp.where(second, jnp.where(s_i <= t_i, 1.0, 0.0), jnp.where(s_i > t_i, 1.0, 0.0)), 0.0)
        mcon[pl.ds(256 + 128 * lev, 128), :] = m.astype(BF16)
    tri[...] = jnp.where(iota((256, 256), 0) > iota((256, 256), 1), 1.0, 0.0).astype(BF16)
    for g in range(4):
        pbuf[g, 0] = jnp.zeros((TOK, HD), F32)
        tbuf[g, 0] = jnp.zeros((TOK, HD), F32)
    gainl.wait()
    gf[...] = gb[...].astype(F32)
    kbl.wait()
    kbuf[b, pl.ds(TOK, 16), :] = rows_of([kb[:, pl.ds(128 * r, 128)] for r in range(CH)])
    gdl.wait()
    for i in range(16):
        down = gd[:, pl.ds(128 * i, 128)].astype(F32)
        square = jnp.concatenate([down, jnp.zeros((96, 128), F32)], axis=0)
        wbuf[pl.ds(128 * i, 128), pl.ds(640, 128)] = jnp.transpose(square).astype(BF16)
    for cp in wloads:
        cp.wait()

    def scaled(chip, first=False):
        pieces = []
        for j in range(4):
            x = tok[4 * chip + j].astype(F32)
            sq = x * x
            ss[...] = sq if (first and j == 0) else ss[...] + sq
            pieces.append((x * gf[pl.ds(4 * chip + j, 1), :]).astype(BF16))
        return jnp.concatenate(pieces, axis=1)

    def weight_rows(chip):
        return pl.ds(pl.multiple_of(512 * chip, 512), 512)

    def fold(chip, first=False):
        lhs = scaled(chip, first)
        for n in range(4):
            cols = pl.ds(256 * n, 256)
            add = mm(lhs, wbuf[weight_rows(chip), cols])
            acc[:, cols] = add if first else acc[:, cols] + add

    mark("own")
    for r in range(PARTS):
        arrived(part(4 * y + 2 * oc, 2, r), M_P0 + r)
    fold(y, True)
    mark("fwd")
    for r in range(PARTS):
        arrived(part(4 * ym + 2 * c, 1, r), M_A0 + r)
        send_part(4 * ym + 2 * c, 1, r, M_C, y=yp)
        arrived(part(4 * yp + 2 * c + 1, 1, r), M_B1 + r)
        send_part(4 * yp + 2 * c + 1, 1, r, M_D, y=ym)
        if r + 1 < PARTS:
            send_part(base + 1, 1, r + 1, M_A1, y=yp)
            send_part(base, 1, r + 1, M_B0, y=ym)
        send_part(4 * ym + 2 * c, 1, r, M_P1, c=oc)
        send_part(4 * yp + 2 * c + 1, 1, r, M_P2, c=oc)
    mark("fwd1")
    for r in range(PARTS):
        arrived(part(4 * ym + 2 * c + 1, 1, r), M_A1 + r)
        send_part(4 * ym + 2 * c + 1, 1, r, M_P3, c=oc)
        arrived(part(4 * yp + 2 * c, 1, r), M_B0 + r)
        send_part(4 * yp + 2 * c, 1, r, M_P4, c=oc)
        if r + 1 < PARTS:
            arrived(part(4 * yo + 2 * c, 1, r), M_C + r)
            send_part(4 * yo + 2 * c, 1, r, M_P5, c=oc)
            arrived(part(4 * yo + 2 * c + 1, 1, r), M_D + r)
            send_part(4 * yo + 2 * c + 1, 1, r, M_P6, c=oc)
    mark("fold2")
    for r in range(PARTS):
        arrived(part(4 * ym + 2 * oc, 1, r), M_P1 + r)
        arrived(part(4 * ym + 2 * oc + 1, 1, r), M_P3 + r)
    fold(ym)
    r = PARTS - 1
    arrived(part(4 * yo + 2 * c, 1, r), M_C + r)
    send_part(4 * yo + 2 * c, 1, r, M_P5, c=oc)
    arrived(part(4 * yo + 2 * c + 1, 1, r), M_D + r)
    send_part(4 * yo + 2 * c + 1, 1, r, M_P6, c=oc)
    for r in range(PARTS):
        arrived(part(4 * yp + 2 * oc, 1, r), M_P4 + r)
        arrived(part(4 * yp + 2 * oc + 1, 1, r), M_P2 + r)
    fold(yp)
    mark("fwd2")
    for r in range(PARTS):
        arrived(part(4 * yo + 2 * oc, 1, r), M_P5 + r)
        arrived(part(4 * yo + 2 * oc + 1, 1, r), M_P6 + r)

    xp, xm, xo = lax.rem(b + 1, 4), lax.rem(b + 3, 4), lax.rem(b + 2, 4)

    def krows(g, r):
        return kbuf.at[g, pl.ds(KROWS * r, KROWS + (16 if r == KPARTS - 1 else 0))]

    def vrows(g, r):
        return vbuf.at[g, pl.ds(KROWS * r, KROWS)]

    def qrows(d, r):
        return qbuf.at[d, pl.ds(KROWS * r, KROWS)]

    mark("finish")
    lhs = scaled(yo)
    inv = lax.rsqrt(jnp.sum(ss[...], axis=1, keepdims=True) * (1.0 / D) + EPS)

    def finish(n):
        cols = pl.ds(256 * n, 256)
        total = acc[:, cols] + mm(lhs, wbuf[weight_rows(yo), cols])
        return (total * inv).astype(BF16)

    got = finish(0)
    kbuf[b, pl.ds(0, TOK), :] = got[:, :128]
    qbuf[0] = got[:, 128:]
    for r in range(KPARTS):
        send(krows(b, r), krows(b, r), M_K + r, x=xp)
        send(krows(b, r), krows(b, r), M_K + KPARTS + r, x=xm)

    for r in range(KPARTS):

        @pl.when(a >= 1)
        def _():
            remote(qrows(0, r), qrows(1, r), M_Q + KPARTS + r, z=a - 1).start()

        @pl.when(a == 3)
        def _():
            remote(qrows(0, r), qrows(3, r), M_Q + 3 * KPARTS + r, z=0).start()

    got = finish(1)
    vbuf[b] = got[:, :128]
    lk[...] = got[:, 128:]
    for r in range(KPARTS):
        send(vrows(b, r), vrows(b, r), M_K + 3 * KPARTS + r, x=xm)
        send(vrows(b, r), vrows(b, r), M_K + 2 * KPARTS + r, x=xp)
    got = finish(2)
    lv[...] = got[:, :128]
    low = got[:, 128:160]
    got = finish(3)
    lq[...] = got[:, :128]
    lg[...] = got[:, 128:]

    mark("lstate")
    gul.wait()
    dobl.wait()
    pre = (mm(low, gu[...]) + dbuf[...]) * LOG2E
    decay = (jnp.minimum(pre, 0.0) - jnp.log2(1.0 + jnp.exp2(-jnp.abs(pre)))) * (1.0 / SOFT)
    ghi, glo = split(decay)
    gboth = jnp.concatenate([ghi, glo], axis=1)
    gs[...] = gboth
    state = jnp.zeros((HD, HD), F32)
    before = jnp.zeros((1, HD), F32)
    for n in range(CH):
        rows = slice(128 * n, 128 * n + 128)
        both = mm(mcon[pl.ds(0, 256), :], gboth[rows])
        dist = both[:, :128] + both[:, 128:]
        fade = jnp.exp2(dist)
        ffrom[rows, :] = fade[:128]
        fall[rows, :] = fade[:128] * jnp.exp2(before)
        if n:
            sthis[n] = state.astype(BF16)
        length = dist[127:128]
        ke = (lk[rows, :].astype(F32) * fade[128:]).astype(BF16)
        state = state * jnp.exp2(length) + tn(lv[rows, :], ke)
        before = before + length
    sx[b, pl.ds(0, HD), :] = state.astype(BF16)
    sx[b, pl.ds(HD, 16), :] = rows_of(split(before))
    for k in range(1, 4):
        send(sx.at[b], sx.at[b], M_SX + k, x=lax.rem(b + k, 4))

    def linear_inside():
        apart = t_i ^ s_i
        for n in range(CH):
            rows = slice(128 * n, 128 * n + 128)
            both = mm(mcon[pl.ds(256, 128 * LEVELS), :], gs[rows, :])
            fade = jnp.exp2(both[:, :128] + both[:, 128:])
            qh, kh, vh = lq[rows, :], lk[rows, :], lv[rows, :]
            qf, kf = qh.astype(F32) * scale, kh.astype(F32)
            score = jnp.where(apart == 0, nt(qh, kh) * scale, 0.0)
            for lev in range(LEVELS):
                e = fade[128 * lev : 128 * lev + 128]
                part_score = nt((qf * e).astype(BF16), (kf * e).astype(BF16))
                score = jnp.where(((apart >> lev) == 1) & (t_i > s_i), part_score, score)
            inner = mm(score.astype(BF16), vh)
            if n:
                inner = inner + nt((qf * ffrom[rows, :]).astype(BF16), sthis[n])
            lacc[rows, :] = inner
            qx[rows, :] = (qf * fall[rows, :]).astype(BF16)

    mark("diag")
    def bias_of(g):
        head = kbuf[g, pl.ds(TOK, 16), :].astype(F32) * LOG2E
        return jnp.concatenate([head[r : r + 1] for r in range(CH)], axis=1)

    def pair(d, g, diagonal=False):
        z = nt(qbuf[d], kbuf[g, pl.ds(0, TOK), :]) * (scale * LOG2E) + bias_of(g)
        soft = jnp.maximum(jnp.log2(1.0 + jnp.exp2(jnp.minimum(z, 126.0))), z)
        own = z - soft
        if diagonal:
            seen = iota((TOK, TOK), 1) < iota((TOK, TOK), 0)
            soft = jnp.where(seen, soft, 0.0)
        sb = soft.astype(BF16)
        near = mm(sb[:, 256:], tri[pl.ds(0, 128), pl.ds(0, 128)])
        near_total = near[:, :1] + soft[:, 256:257]
        far = mm(sb[:, :256], tri[...]) + near_total
        whole = far[:, :1] + soft[:, :1]
        share = jnp.exp2(own - jnp.concatenate([far, near], axis=1))
        if diagonal:
            share = jnp.where(seen, share, 0.0)
        pbuf[g, d] = mm(share.astype(BF16), vbuf[g])
        tbuf[g, d] = jnp.broadcast_to(whole, (TOK, HD))

    pair(0, b, True)

    def pass_keys(r):
        arrived(krows(xm, r), M_K + r)
        send(krows(xm, r), krows(xm, r), M_K + 4 * KPARTS + r, x=xp)

    def pass_values(r):
        arrived(vrows(xp, r), M_K + 3 * KPARTS + r)
        send(vrows(xp, r), vrows(xp, r), M_K + 5 * KPARTS + r, x=xm)

    def queries(d):
        for r in range(KPARTS):
            arrived(qrows(d, r), M_Q + KPARTS * d + r)

    def pass_queries(r):
        @pl.when(a <= 2)
        def _():
            arrived(qrows(1, r), M_Q + KPARTS + r)

        @pl.when((a >= 1) & (a <= 2))
        def _():
            remote(qrows(1, r), qrows(2, r), M_Q + 2 * KPARTS + r, z=a - 1).start()

    mark("linear1")
    linear_inside()
    mark("kvfwd")
    for r in range(KPARTS):
        pass_queries(r)
        pass_keys(r)
    mark("q1")

    @pl.when(a == 0)
    def _():
        queries(3)
        pair(1, b)
        pair(3, b)

    @pl.when((a == 1) | (a == 2))
    def _():
        pair(1, b)

    mark("kvwait")
    for r in range(KPARTS):
        pass_values(r)
    for r in range(KPARTS):
        arrived(krows(xp, r), M_K + KPARTS + r)
        arrived(vrows(xm, r), M_K + 2 * KPARTS + r)
    mark("first")

    count = 4 - a
    ahead = jnp.where(a == 0, 2, 1)

    def turn(i):
        far = jnp.where(i == 0, 3, jnp.where(i == 3, 0, i))
        return jnp.where(a == 0, far, jnp.where(i == count - 1, 0, i + 1))

    def ready(i, carry):
        d = turn(i)
        pair(d, xm)
        pair(d, xp)
        return carry

    lax.fori_loop(0, ahead, ready, 0)

    mark("states")
    for k in range(1, 4):
        arrived(sx.at[lax.rem(b + 4 - k, 4)], M_SX + k)
    run = jnp.zeros((HD, HD), F32)
    run_len = jnp.zeros((1, HD), F32)
    pre_state, pre_len = run, run_len
    for g in range(4):
        pre_state = jnp.where(b == g, run, pre_state)
        pre_len = jnp.where(b == g, run_len, pre_len)
        tail = sx[g, pl.ds(HD, 16), :].astype(F32)
        length = tail[0:1] + tail[1:2]
        run = run * jnp.exp2(length) + sx[g, pl.ds(0, HD), :].astype(F32)
        run_len = run_len + length
    sz[a, pl.ds(0, HD), :] = run.astype(BF16)
    sz[a, pl.ds(HD, 16), :] = rows_of(split(run_len))
    for d in (3, 1):

        @pl.when(a + d <= 3)
        def _():
            remote(sz.at[a], sz.at[a], M_SZ + d, z=a + d).start()

    def add_group(g, carried):
        tail = sz[g, pl.ds(HD, 16), :].astype(F32)
        return carried * jnp.exp2(tail[0:1] + tail[1:2]) + sz[g, pl.ds(0, HD), :].astype(F32)

    def span(r):
        return pl.ds(pl.multiple_of(OUT_ROWS * r, 16), OUT_ROWS)

    lngl.wait()

    def linear_out():
        older = lax.fori_loop(0, a, add_group, jnp.zeros((HD, HD), F32))
        incoming = pre_state + older * jnp.exp2(pre_len)
        raw = lacc[...] + nt(qx[...], incoming.astype(BF16))
        normed = raw * lax.rsqrt(jnp.mean(raw * raw, axis=1, keepdims=True) + EPS) * lng[...]
        gate = lg[...].astype(F32)
        linb[...] = (normed * (gate / (1.0 + jnp.exp2(gate * (-LOG2E))))).astype(BF16)
        for k in range(1, 8):
            r = lax.rem(tp + k, 8)
            remote(linb.at[span(r)], xl.at[tp], M_LA + k, y=r // 2, c=lax.rem(r, 2)).start()
        xl[tp] = linb[span(tp), :]

    mark("lout0")

    @pl.when(a == 0)
    def _():
        linear_out()

    mark("q2")

    @pl.when(a <= 1)
    def _():
        queries(2)
        remote(sz.at[a], sz.at[a], M_SZ + 2, z=a + 2).start()
        pair(2, b)

    mark("kvwait2")
    for r in range(KPARTS):
        arrived(krows(xo, r), M_K + 4 * KPARTS + r)
        arrived(vrows(xo, r), M_K + 5 * KPARTS + r)
    mark("serve")

    lane = iota((16, 128), 1)

    def hand_on(d, home):
        total = jnp.zeros((TOK, HD), F32)
        behind = jnp.zeros((TOK, HD), F32)
        for g in range(3, -1, -1):
            counts = (g <= b) if home else True
            weight = jnp.exp2(-behind)
            total = total + (jnp.where(counts, weight * pbuf[g, d], 0.0) if home else weight * pbuf[g, d])
            behind = behind + (jnp.where(counts, tbuf[g, d], 0.0) if home else tbuf[g, d])
        tiles = []
        for r in range(CH):
            line = jnp.transpose(behind[128 * r : 128 * r + 128])[0:1]
            tiles.append(rows_of(split(line)).astype(F32))
        for r in range(8):
            j, o = (OUT_ROWS * r) // 128, (OUT_ROWS * r) % 128
            tail = pltpu.roll(tiles[j], 128 - o, 1) if o else tiles[j]
            if o + OUT_ROWS > 128:
                tail = jnp.where(lane < 128 - o, tail, pltpu.roll(tiles[j + 1], 128 - o, 1))
            sbuf[d, r, pl.ds(0, OUT_ROWS), :] = total[OUT_ROWS * r : OUT_ROWS * r + OUT_ROWS].astype(BF16)
            sbuf[d, r, pl.ds(OUT_ROWS, 16), :] = tail.astype(BF16)
        for k in range(8):
            r = lax.rem(tp + k, 8)
            if home and k == 0:
                rbuf[0, tp] = sbuf[0, tp]
            else:
                dev = {"y": r // 2, "c": lax.rem(r, 2)}
                if not home:
                    dev["z"] = a + d
                remote(sbuf.at[d, r], rbuf.at[d, tp], M_R + 8 * d + k, **dev).start()

    def serve(i, carry):
        d = turn(i)
        pair(d, xo)
        hand_on(d, False)
        ready(i + ahead, 0)
        return carry

    lax.fori_loop(0, count - ahead, serve, 0)
    mark("home")

    @pl.when(a == 0)
    def _():
        pair(2, xo)
        hand_on(2, False)

    pair(0, xo)
    hand_on(0, True)
    mark("lout1")

    @pl.when(a >= 1)
    def _():
        for d in range(1, 4):

            @pl.when(a >= d)
            def _():
                arrived(sz.at[a - d], M_SZ + d)

        linear_out()

    for k in range(1, 8):
        started.append((linb.at[span(lax.rem(tp + k, 8))], M_LA + k))
    mark("linx")
    oll.wait()
    for k in range(1, 8):
        arrived(xl.at[lax.rem(tp + 8 - k, 8)], M_LA + k)
    mark("linproj")
    lhs = jnp.concatenate([xl[i] for i in range(8)], axis=1)
    for n in range(4):
        cols = pl.ds(512 * n, 512)
        oacc[:, cols] = mm(lhs, ol[:, cols])

    mark("ret0")
    osl.wait()
    for k in range(1, 8):
        arrived(rbuf.at[0, lax.rem(tp + 8 - k, 8)], M_R + k)
    mark("ret")
    for d in range(1, 4):

        @pl.when(a >= d)
        def _():
            for k in range(8):
                arrived(rbuf.at[d, lax.rem(tp + 8 - k, 8)], M_R + 8 * d + k)

    mark("stproj")
    sub = iota((8, 128), 0)
    behind = jnp.zeros((8, 128), F32)
    heads = [rbuf[0, i, pl.ds(0, OUT_ROWS), :].astype(F32) for i in range(8)]
    for d in range(1, 4):
        for i in range(8):
            tail = rbuf[d - 1, i, pl.ds(OUT_ROWS, 16), :].astype(F32)
            behind = behind + jnp.where(sub == i, tail[0:1] + tail[1:2], 0.0)
        left = jnp.transpose(jnp.exp2(-behind))
        for i in range(8):
            more = left[:OUT_ROWS, i : i + 1] * rbuf[d, i, pl.ds(0, OUT_ROWS), :].astype(F32)
            heads[i] = heads[i] + jnp.where(a >= d, more, 0.0)
    lhs = jnp.concatenate([h.astype(BF16) for h in heads], axis=1)
    for n in range(4):
        cols = pl.ds(512 * n, 512)
        out[:, cols] = (oacc[:, cols] + mm(lhs, os_[:, cols])).astype(BF16)

    mark("drain")
    for src, i in started:
        sent(src, i)

    for r in range(KPARTS):

        @pl.when(a >= 1)
        def _():
            sent(qrows(0, r), M_Q + KPARTS + r)

        @pl.when(a == 3)
        def _():
            sent(qrows(0, r), M_Q + 3 * KPARTS + r)

        @pl.when((a >= 1) & (a <= 2))
        def _():
            sent(qrows(1, r), M_Q + 2 * KPARTS + r)

    for d in range(4):

        @pl.when(a + d <= 3)
        def _():
            if d:
                sent(sz.at[a], M_SZ + d)
            for k in range(0 if d else 1, 8):
                sent(sbuf.at[d, lax.rem(tp + k, 8)], M_R + 8 * d + k)

    mark("")


def per_device(*args):
    args = list(args)
    args[1] = args[1].reshape(16, 128)
    args[6] = args[6].T
    args[9] = args[9].reshape(1, HD)
    vm = pltpu.VMEM
    return pl.pallas_call(
        kernel,
        out_shape=pltpu.VMEM((OUT_ROWS, D), BF16),
        in_specs=[pl.BlockSpec(memory_space=pl.ANY)] * 16,
        out_specs=pl.BlockSpec(memory_space=pltpu.VMEM),
        scratch_shapes=[
            vm((16, TOK, 128), BF16),
            vm((D, 1024), BF16),
            vm((32, D), BF16),
            vm((32, 128), BF16),
            vm((16, 128), BF16),
            vm((16, 128), F32),
            vm((TOK, 1024), F32),
            vm((TOK, 128), F32),
            vm((TOK, 128), F32),
            vm((1, TOK), BF16),
            vm((1, 128), F32),
            vm((1024, D), BF16),
            vm((1024, D), BF16),
            vm((128 * (LEVELS + 2), 128), BF16),
            vm((256, 256), BF16),
            vm((4, TOK + 16, 128), BF16),
            vm((4, TOK, 128), BF16),
            vm((4, TOK, 128), BF16),
            vm((TOK, 128), BF16),
            vm((TOK, 128), BF16),
            vm((TOK, 128), BF16),
            vm((TOK, 128), BF16),
            vm((TOK, 256), BF16),
            vm((TOK, 128), F32),
            vm((TOK, 128), F32),
            vm((CH, 128, 128), BF16),
            vm((TOK, 128), F32),
            vm((TOK, 128), BF16),
            vm((4, 144, 128), BF16),
            vm((4, 144, 128), BF16),
            vm((4, 4, TOK, 128), F32),
            vm((4, 4, TOK, 128), F32),
            vm((4, 8, OUT_ROWS + 16, 128), BF16),
            vm((4, 8, OUT_ROWS + 16, 128), BF16),
            vm((TOK, 128), BF16),
            vm((8, OUT_ROWS, 128), BF16),
            vm((OUT_ROWS, D), F32),
            pltpu.SemaphoreType.DMA((17,)),
            pltpu.SemaphoreType.DMA((N_MSG,)),
            pltpu.SemaphoreType.DMA((N_MSG,)),
        ],
        compiler_params=pltpu.CompilerParams(collective_id=0, has_side_effects=True),
        name="layer",
    )(*args)


def solution(mesh):
    torus = Mesh(mesh.devices.reshape(4, 4, 4, 2), ("z", "x", "y", "c"))
    sp, tp = ("z", "x"), ("y", "c")
    placed = (
        P(sp, tp), P(), P(None, tp), P(None, tp), P(None, tp), P(None, tp), P(), P(), P(sp, tp), P(),
        P(None, tp), P(None, tp), P(None, tp), P(tp, sp), P(), P(),
    )
    return jax.shard_map(
        per_device, mesh=torus, in_specs=placed, out_specs=P(sp + tp, None), check_vma=False
    )
```

```python
import jax
import jax.numpy as jnp
from jax import lax
from jax.experimental import pallas as pl
from jax.experimental.pallas import tpu as pltpu
from jax.sharding import Mesh
from jax.sharding import PartitionSpec as P

MESH = pl.DeviceIdType.MESH
F32 = jnp.float32
BF16 = jnp.bfloat16
LOG2E = 1.4426950408889634
EPS = 1e-6
SOFT = 16.0
TOK = 384
D = 2048
HD = 128
PARTS = 3
ROWS = TOK // PARTS
KPARTS = 2
KROWS = TOK // KPARTS
CH = TOK // 128
LEVELS = 7
TAIL = 8
OUT_ROWS = TOK // 8

S_TOK, S_K, S_V, S_Q, S_SX, S_SZ, S_LA, S_R, N_S = range(9)
R_AB, R_BA, R_CD = 0, PARTS, 2 * PARTS
R_P0, R_PM, R_PP, R_PO, R_KN, R_VN, R_KF, R_VF, R_SX, R_Q2, R_Q3, R_SZ, R_LA = [3 * PARTS + i for i in range(13)]
R_K = R_LA + 1
R_V = R_K + KPARTS
R_Q = R_V + KPARTS
R_R = R_Q + KPARTS
N_R = R_R + 4


PROFILE = False


class Marks:
    current = None

    def __call__(self, name):
        if not PROFILE:
            return
        if self.current is not None:
            self.current.__exit__(None, None, None)
        self.current = jax.named_scope(name) if name else None
        if name:
            self.current.__enter__()


def nt(a, b):
    return lax.dot_general(a, b, (((1,), (1,)), ((), ())), preferred_element_type=F32)


def tn(a, b):
    return lax.dot_general(a, b, (((0,), (0,)), ((), ())), preferred_element_type=F32)


def mm(a, b):
    return jnp.dot(a, b, preferred_element_type=F32)


def iota(shape, dim):
    return lax.broadcasted_iota(jnp.int32, shape, dim)


def split(x):
    hi = x.astype(BF16)
    return hi, (x - hi.astype(F32)).astype(BF16)


def rows_of(pieces):
    io = iota((16, 128), 0)
    out = jnp.zeros((16, 128), F32)
    for r, piece in enumerate(pieces):
        out = jnp.where(io == r, piece.astype(F32), out)
    return out.astype(BF16)


def kernel(
    tokens, gain, w_lq, w_lk, w_lv, w_lg, w_gd, w_gu, dob, lgain, w_sq, w_sk, w_sv, kbias, w_ol, w_os,
    out,
    tok, wbuf, gd, gu, gb, gf, acc, ss, dbuf, kb, lng, ol, os_,
    mcon, tri, kbuf, vbuf, qbuf, lq, lk, lv, lg, gs, ffrom, fall, sthis, lacc, qx, sx, sz, pbuf, tbuf, sbuf, rbuf,
    linb, xl, oacc,
    lsem, ssem, rsem,
):
    mark = Marks()
    a, b = lax.axis_index("z"), lax.axis_index("x")
    y, c = lax.axis_index("y"), lax.axis_index("c")
    tp = 2 * y + c
    oc = 1 - c
    scale = HD ** (-0.5)

    def local(src, dst, i):
        cp = pltpu.make_async_copy(src, dst, lsem.at[i])
        cp.start()
        return cp

    def remote(src, dst, i, j, **dev):
        return pltpu.make_async_remote_copy(
            src_ref=src, dst_ref=dst, send_sem=ssem.at[i], recv_sem=rsem.at[j],
            device_id=dev, device_id_type=MESH,
        )

    def send(src, dst, i, j, **dev):
        remote(src, dst, i, j, **dev).start()

    def arrived(dst, j):
        remote(dst, dst, 0, j, c=oc).wait_recv()

    def sent(src, i):
        remote(src, src, i, 0, c=oc).wait_send()

    mark("load")
    base = 4 * y + 2 * c
    local(tokens.at[:, pl.ds(0, 128)], tok.at[base], 0)
    local(tokens.at[:, pl.ds(128, 128)], tok.at[base + 1], 0)
    barrier = pltpu.get_barrier_semaphore()
    for k in range(1, 4):
        pl.semaphore_signal(barrier, inc=1, device_id={"x": lax.rem(b + k, 4)}, device_id_type=MESH)

    @pl.when(a <= 2)
    def _():
        pl.semaphore_signal(barrier, inc=1, device_id={"z": a + 1}, device_id_type=MESH)

    @pl.when(a == 0)
    def _():
        pl.semaphore_signal(barrier, inc=1, device_id={"z": 3}, device_id_type=MESH)

    for k in range(1, 8):
        r = lax.rem(tp + k, 8)
        pl.semaphore_signal(
            barrier, inc=1, device_id={"y": r // 2, "c": lax.rem(r, 2)}, device_id_type=MESH
        )
    weights = [w_sk, w_sq, w_sv, w_lk, w_lv, None, w_lq, w_lg]
    for i, w in enumerate(weights):
        if w is not None:
            local(w, wbuf.at[:, pl.ds(128 * i, 128)], 1)
    gdl = local(w_gd, gd, 2)
    gainl = local(gain, gb, 3)
    kbl = local(kbias, kb, 4)
    gul = local(w_gu.at[:, pl.ds(pl.multiple_of(128 * tp, 128), 128)], gu, 5)
    dobl = local(dob, dbuf, 6)
    lngl = local(lgain, lng, 7)
    oll = local(w_ol, ol, 8)
    osl = local(w_os, os_, 9)

    t_i, s_i = iota((128, 128), 0), iota((128, 128), 1)
    mcon[pl.ds(0, 128), :] = jnp.where(s_i <= t_i, 1.0, 0.0).astype(BF16)
    mcon[pl.ds(128, 128), :] = jnp.where(s_i > t_i, 1.0, 0.0).astype(BF16)
    mark("barrier")
    own = tok.at[pl.ds(base, 2)]
    pltpu.make_async_copy(own, own, lsem.at[0]).wait()
    pl.semaphore_wait(barrier, 10 + (a + 1) // 2)

    mark("send")
    yp, ym, yo = lax.rem(y + 1, 4), lax.rem(y + 3, 4), lax.rem(y + 2, 4)

    def part(first, count, r):
        return tok.at[pl.ds(first, count), pl.ds(ROWS * r, ROWS), :]

    def send_part(first, count, r, j, **dev):
        ref = part(first, count, r)
        send(ref, ref, S_TOK, j, **dev)

    for r in range(PARTS):
        send_part(base, 1, r, R_AB + r, y=yp)
        send_part(base + 1, 1, r, R_AB + r, y=ym)
    for r in range(PARTS):
        send_part(base, 2, r, R_P0, c=oc)
    send_part(base + 1, 1, 0, R_BA, y=yp)
    send_part(base, 1, 0, R_BA, y=ym)

    for lev in range(LEVELS):
        same = (t_i >> lev) == (s_i >> lev)
        second = ((t_i >> lev) & 1) == 1
        m = jnp.where(same, jnp.where(second, jnp.where(s_i <= t_i, 1.0, 0.0), jnp.where(s_i > t_i, 1.0, 0.0)), 0.0)
        mcon[pl.ds(256 + 128 * lev, 128), :] = m.astype(BF16)
    tri[...] = jnp.where(iota((256, 256), 0) > iota((256, 256), 1), 1.0, 0.0).astype(BF16)
    for g in range(4):
        pbuf[g, 0] = jnp.zeros((TOK, HD), F32)
        tbuf[g, 0] = jnp.zeros((TOK, HD), F32)
    gainl.wait()
    gf[...] = gb[...].astype(F32)
    kbl.wait()
    kbuf[b, pl.ds(TOK, 16), :] = rows_of([kb[:, pl.ds(128 * r, 128)] for r in range(CH)])
    gdl.wait()
    for i in range(16):
        down = gd[:, pl.ds(128 * i, 128)].astype(F32)
        square = jnp.concatenate([down, jnp.zeros((96, 128), F32)], axis=0)
        wbuf[pl.ds(128 * i, 128), pl.ds(640, 128)] = jnp.transpose(square).astype(BF16)
    seven = wbuf.at[:, pl.ds(0, 896)]
    pltpu.make_async_copy(seven, seven, lsem.at[1]).wait()

    def scaled(block, count, first=False):
        pieces = []
        for j in range(count):
            x = tok[block + j].astype(F32)
            sq = x * x
            ss[...] = sq if (first and j == 0) else ss[...] + sq
            pieces.append((x * gf[pl.ds(block + j, 1), :]).astype(BF16))
        return jnp.concatenate(pieces, axis=1)

    def weight_rows(block, count):
        return pl.ds(pl.multiple_of(128 * block, 256), 128 * count)

    def fold_blocks(block, count, first=False):
        lhs = scaled(block, count, first)
        for n in range(4):
            cols = pl.ds(256 * n, 256)
            add = mm(lhs, wbuf[weight_rows(block, count), cols])
            acc[:, cols] = add if first else acc[:, cols] + add

    def fold(chip, first=False):
        fold_blocks(4 * chip, 4, first)

    def fold_half(chip, core):
        fold_blocks(4 * chip + 2 * core, 2)

    mark("own")

    def partner(chip, j):
        arrived(tok.at[pl.ds(4 * chip + 2 * oc, 2)], j)

    def pass_far(r):
        arrived(part(4 * yo + 2 * c, 2, r), R_CD + r)
        send_part(4 * yo + 2 * c, 2, r, R_PO, c=oc)

    partner(y, R_P0)
    fold(y, True)
    mark("fwd")
    for r in range(PARTS):
        arrived(part(4 * ym + 2 * c, 2, r), R_AB + r)
        send_part(4 * ym + 2 * c, 1, r, R_CD + r, y=yp)
        send_part(4 * yp + 2 * c + 1, 1, r, R_CD + r, y=ym)
        if r + 1 < PARTS:
            send_part(base + 1, 1, r + 1, R_BA + r + 1, y=yp)
            send_part(base, 1, r + 1, R_BA + r + 1, y=ym)
        send_part(4 * ym + 2 * c, 1, r, R_PM, c=oc)
        send_part(4 * yp + 2 * c + 1, 1, r, R_PP, c=oc)
    mark("fwd1")
    for r in range(PARTS):
        arrived(part(4 * ym + 2 * c, 2, r), R_BA + r)
        send_part(4 * ym + 2 * c + 1, 1, r, R_PM, c=oc)
        send_part(4 * yp + 2 * c, 1, r, R_PP, c=oc)
        pass_far(r)
    mark("fold2")
    partner(ym, R_PM)
    fold(ym)
    partner(yp, R_PP)
    fold(yp)
    fold_half(yo, c)
    mark("fwd2")
    partner(yo, R_PO)

    xp, xm, xo = lax.rem(b + 1, 4), lax.rem(b + 3, 4), lax.rem(b + 2, 4)

    def krows(g, r):
        return kbuf.at[g, pl.ds(KROWS * r, KROWS + (16 if r == KPARTS - 1 else 0))]

    def vrows(g, r):
        return vbuf.at[g, pl.ds(KROWS * r, KROWS)]

    def qrows(d, r):
        return qbuf.at[d, pl.ds(KROWS * r, KROWS)]

    mark("finish")
    last = 4 * yo + 2 * oc
    lhs = scaled(last, 2)
    inv = lax.rsqrt(jnp.sum(ss[...], axis=1, keepdims=True) * (1.0 / D) + EPS)

    def finish(n):
        cols = pl.ds(256 * n, 256)
        total = acc[:, cols] + mm(lhs, wbuf[weight_rows(last, 2), cols])
        return (total * inv).astype(BF16)

    got = finish(0)
    kbuf[b, pl.ds(0, TOK), :] = got[:, :128]
    qbuf[0] = got[:, 128:]
    for r in range(KPARTS):
        send(krows(b, r), krows(b, r), S_K, R_K + r, x=xp)
        send(krows(b, r), krows(b, r), S_K, R_KN, x=xm)

    @pl.when(a >= 1)
    def _():
        for r in range(KPARTS):
            send(qrows(0, r), qrows(1, r), S_Q, R_Q + r, z=a - 1)

    @pl.when(a == 3)
    def _():
        send(qbuf.at[0], qbuf.at[3], S_Q, R_Q3, z=0)

    got = finish(1)
    vbuf[b] = got[:, :128]
    lk[...] = got[:, 128:]
    for r in range(KPARTS):
        send(vrows(b, r), vrows(b, r), S_V, R_V + r, x=xm)
        send(vrows(b, r), vrows(b, r), S_V, R_VN, x=xp)
    got = finish(2)
    lv[...] = got[:, :128]
    low = got[:, 128:160]
    got = finish(3)
    lq[...] = got[:, :128]
    lg[...] = got[:, 128:]

    mark("lstate")
    gul.wait()
    dobl.wait()
    pre = (mm(low, gu[...]) + dbuf[...]) * LOG2E
    decay = (jnp.minimum(pre, 0.0) - jnp.log2(1.0 + jnp.exp2(-jnp.abs(pre)))) * (1.0 / SOFT)
    ghi, glo = split(decay)
    gboth = jnp.concatenate([ghi, glo], axis=1)
    gs[...] = gboth
    state = jnp.zeros((HD, HD), F32)
    before = jnp.zeros((1, HD), F32)
    for n in range(CH):
        rows = slice(128 * n, 128 * n + 128)
        both = mm(mcon[pl.ds(0, 256), :], gboth[rows])
        dist = both[:, :128] + both[:, 128:]
        fade = jnp.exp2(dist)
        ffrom[rows, :] = fade[:128]
        fall[rows, :] = fade[:128] * jnp.exp2(before)
        if n:
            sthis[n] = state.astype(BF16)
        length = dist[127:128]
        ke = (lk[rows, :].astype(F32) * fade[128:]).astype(BF16)
        state = state * jnp.exp2(length) + tn(lv[rows, :], ke)
        before = before + length
    sx[b, pl.ds(0, HD), :] = state.astype(BF16)
    sx[b, pl.ds(HD, 16), :] = rows_of(split(before))
    for k in range(1, 4):
        send(sx.at[b], sx.at[b], S_SX, R_SX, x=lax.rem(b + k, 4))

    def linear_inside():
        apart = t_i ^ s_i
        for n in range(CH):
            rows = slice(128 * n, 128 * n + 128)
            both = mm(mcon[pl.ds(256, 128 * LEVELS), :], gs[rows, :])
            fade = jnp.exp2(both[:, :128] + both[:, 128:])
            qh, kh, vh = lq[rows, :], lk[rows, :], lv[rows, :]
            qf, kf = qh.astype(F32) * scale, kh.astype(F32)
            score = jnp.where(apart == 0, nt(qh, kh) * scale, 0.0)
            for lev in range(LEVELS):
                e = fade[128 * lev : 128 * lev + 128]
                part_score = nt((qf * e).astype(BF16), (kf * e).astype(BF16))
                score = jnp.where(((apart >> lev) == 1) & (t_i > s_i), part_score, score)
            inner = mm(score.astype(BF16), vh)
            if n:
                inner = inner + nt((qf * ffrom[rows, :]).astype(BF16), sthis[n])
            lacc[rows, :] = inner
            qx[rows, :] = (qf * fall[rows, :]).astype(BF16)

    mark("diag")
    def bias_of(g):
        head = kbuf[g, pl.ds(TOK, 16), :].astype(F32) * LOG2E
        return jnp.concatenate([head[r : r + 1] for r in range(CH)], axis=1)

    def pair(d, g, diagonal=False):
        z = nt(qbuf[d], kbuf[g, pl.ds(0, TOK), :]) * (scale * LOG2E) + bias_of(g)
        soft = jnp.maximum(jnp.log2(1.0 + jnp.exp2(jnp.minimum(z, 126.0))), z)
        own = z - soft
        if diagonal:
            seen = iota((TOK, TOK), 1) < iota((TOK, TOK), 0)
            soft = jnp.where(seen, soft, 0.0)
        sb = soft.astype(BF16)
        near = mm(sb[:, 256:], tri[pl.ds(0, 128), pl.ds(0, 128)])
        near_total = near[:, :1] + soft[:, 256:257]
        far = mm(sb[:, :256], tri[...]) + near_total
        whole = far[:, :1] + soft[:, :1]
        share = jnp.exp2(own - jnp.concatenate([far, near], axis=1))
        if diagonal:
            share = jnp.where(seen, share, 0.0)
        pbuf[g, d] = mm(share.astype(BF16), vbuf[g])
        tbuf[g, d] = jnp.broadcast_to(whole, (TOK, HD))

    pair(0, b, True)

    def pass_keys(r):
        arrived(krows(xm, r), R_K + r)
        send(krows(xm, r), krows(xm, r), S_K, R_KF, x=xp)

    def pass_values(r):
        arrived(vrows(xp, r), R_V + r)
        send(vrows(xp, r), vrows(xp, r), S_V, R_VF, x=xm)

    def pass_queries(r):
        @pl.when(a <= 2)
        def _():
            arrived(qrows(1, r), R_Q + r)

        @pl.when((a >= 1) & (a <= 2))
        def _():
            send(qrows(1, r), qrows(2, r), S_Q, R_Q2, z=a - 1)

    lane = iota((16, 128), 1)

    def hand_on(d, home):
        total = jnp.zeros((TOK, HD), F32)
        behind = jnp.zeros((TOK, HD), F32)
        for g in range(3, -1, -1):
            counts = (g <= b) if home else True
            weight = jnp.exp2(-behind)
            total = total + (jnp.where(counts, weight * pbuf[g, d], 0.0) if home else weight * pbuf[g, d])
            behind = behind + (jnp.where(counts, tbuf[g, d], 0.0) if home else tbuf[g, d])
        for r in range(8):
            sbuf[8 * d + r, pl.ds(0, OUT_ROWS), :] = total[OUT_ROWS * r : OUT_ROWS * r + OUT_ROWS].astype(BF16)

        def leave(rows):
            for k in range(8):
                r = lax.rem(tp + k, 8)
                if home and k == 0:
                    rbuf[tp] = sbuf[tp]
                else:
                    dev = {"y": r // 2, "c": lax.rem(r, 2)}
                    if not home:
                        dev["z"] = a + d
                    send(sbuf.at[8 * d + r, pl.ds(0, rows)], rbuf.at[8 * d + tp, pl.ds(0, rows)], S_R, R_R + d, **dev)

        @pl.when(a == 0)
        def _():
            leave(OUT_ROWS)

        @pl.when(a > 0)
        def _():
            tiles = []
            for r in range(CH):
                line = jnp.transpose(behind[128 * r : 128 * r + 128])[0:1]
                tiles.append(rows_of(split(line)).astype(F32))
            for r in range(8):
                j, o = (OUT_ROWS * r) // 128, (OUT_ROWS * r) % 128
                tail = pltpu.roll(tiles[j], 128 - o, 1) if o else tiles[j]
                if o + OUT_ROWS > 128:
                    tail = jnp.where(lane < 128 - o, tail, pltpu.roll(tiles[j + 1], 128 - o, 1))
                sbuf[8 * d + r, pl.ds(OUT_ROWS, TAIL), :] = tail[:TAIL].astype(BF16)
            leave(OUT_ROWS + TAIL)

    mark("home0")

    @pl.when(b == 0)
    def _():
        hand_on(0, True)

    mark("linear1")
    linear_inside()
    mark("kvfwd")
    for r in range(KPARTS):
        pass_queries(r)
        pass_keys(r)
    mark("q1")

    @pl.when(a <= 2)
    def _():
        pair(1, b)

    mark("kvwait")
    for r in range(KPARTS):
        pass_values(r)
    arrived(kbuf.at[xp], R_KN)
    arrived(vbuf.at[xm], R_VN)
    mark("first")
    nearest = jnp.where(a <= 2, 1, 0)
    pair(nearest, xm)
    pair(nearest, xp)
    mark("q3")

    @pl.when(a == 0)
    def _():
        arrived(qbuf.at[3], R_Q3)
        pair(3, b)

    mark("states")
    arrived(sx.at[pl.ds(0, 3)], R_SX)
    run = jnp.zeros((HD, HD), F32)
    run_len = jnp.zeros((1, HD), F32)
    pre_state, pre_len = run, run_len
    for g in range(4):
        pre_state = jnp.where(b == g, run, pre_state)
        pre_len = jnp.where(b == g, run_len, pre_len)
        tail = sx[g, pl.ds(HD, 16), :].astype(F32)
        length = tail[0:1] + tail[1:2]
        run = run * jnp.exp2(length) + sx[g, pl.ds(0, HD), :].astype(F32)
        run_len = run_len + length
    sz[a, pl.ds(0, HD), :] = run.astype(BF16)
    sz[a, pl.ds(HD, 16), :] = rows_of(split(run_len))
    for d in (3, 1):

        @pl.when(a + d <= 3)
        def _():
            send(sz.at[a], sz.at[a], S_SZ, R_SZ, z=a + d)

    def add_group(g, carried):
        tail = sz[g, pl.ds(HD, 16), :].astype(F32)
        return carried * jnp.exp2(tail[0:1] + tail[1:2]) + sz[g, pl.ds(0, HD), :].astype(F32)

    def span(r):
        return pl.ds(pl.multiple_of(OUT_ROWS * r, 16), OUT_ROWS)

    lngl.wait()

    def linear_out():
        older = lax.fori_loop(0, a, add_group, jnp.zeros((HD, HD), F32))
        incoming = pre_state + older * jnp.exp2(pre_len)
        raw = lacc[...] + nt(qx[...], incoming.astype(BF16))
        normed = raw * lax.rsqrt(jnp.mean(raw * raw, axis=1, keepdims=True) + EPS) * lng[...]
        gate = lg[...].astype(F32)
        linb[...] = (normed * (gate / (1.0 + jnp.exp2(gate * (-LOG2E))))).astype(BF16)
        for k in range(1, 8):
            r = lax.rem(tp + k, 8)
            send(linb.at[span(r)], xl.at[tp], S_LA, R_LA, y=r // 2, c=lax.rem(r, 2))
        xl[tp] = linb[span(tp), :]

    mark("lout0")

    @pl.when(a == 0)
    def _():
        linear_out()
        pair(3, xm)
        pair(3, xp)

    mark("q2")

    @pl.when(a <= 1)
    def _():
        arrived(qbuf.at[2], R_Q2)
        send(sz.at[a], sz.at[a], S_SZ, R_SZ, z=a + 2)
        pair(2, b)

    @pl.when(a == 1)
    def _():
        pair(2, xm)
        pair(2, xp)

    mark("kvwait2")
    arrived(kbuf.at[xo], R_KF)
    arrived(vbuf.at[xo], R_VF)
    mark("serve")

    other = jnp.where(a == 0, 3, 2)

    @pl.when(a <= 1)
    def _():
        pair(1, xo)
        pair(other, xo)

    @pl.when(a == 2)
    def _():
        pair(1, xo)

    mark("lout1")

    @pl.when(a >= 1)
    def _():
        for d in range(1, 4):

            @pl.when(a == d)
            def _():
                arrived(sz.at[pl.ds(0, d)], R_SZ)

        linear_out()

    mark("hand")

    @pl.when(a <= 1)
    def _():
        hand_on(1, False)
        hand_on(other, False)

    @pl.when(a == 2)
    def _():
        hand_on(1, False)

    mark("home")

    @pl.when((a <= 2) & (b > 0))
    def _():
        pair(0, xm)
        pair(0, xp)
        pair(0, xo)

    @pl.when((a == 3) & (b > 0))
    def _():
        pair(0, xo)

    @pl.when(b > 0)
    def _():
        hand_on(0, True)

    mark("two")

    @pl.when(a == 0)
    def _():
        pair(2, xm)
        pair(2, xp)
        pair(2, xo)
        hand_on(2, False)

    mark("linx")
    oll.wait()
    arrived(xl.at[pl.ds(0, 7)], R_LA)
    mark("linproj")
    lhs = jnp.concatenate([xl[i] for i in range(8)], axis=1)
    for n in range(4):
        cols = pl.ds(512 * n, 512)
        oacc[:, cols] = mm(lhs, ol[:, cols])

    mark("ret0")
    osl.wait()
    def returned(d, first, count):
        @pl.when(a == d)
        def _():
            arrived(rbuf.at[pl.ds(first, count), pl.ds(0, OUT_ROWS)], R_R + d)

        @pl.when(a > d)
        def _():
            arrived(rbuf.at[pl.ds(first, count)], R_R + d)

    returned(0, 0, 7)
    mark("ret")
    for d in range(1, 4):
        returned(d, 8 * d, 8)

    mark("stproj")
    sub = iota((8, 128), 0)
    behind = jnp.zeros((8, 128), F32)
    heads = [rbuf[i, pl.ds(0, OUT_ROWS), :].astype(F32) for i in range(8)]
    for d in range(1, 4):
        for i in range(8):
            tail = rbuf[8 * d - 8 + i, pl.ds(OUT_ROWS, TAIL), :].astype(F32)
            behind = behind + jnp.where(sub == i, tail[0:1] + tail[1:2], 0.0)
        left = jnp.transpose(jnp.exp2(-behind))
        for i in range(8):
            more = left[:OUT_ROWS, i : i + 1] * rbuf[8 * d + i, pl.ds(0, OUT_ROWS), :].astype(F32)
            heads[i] = heads[i] + jnp.where(a >= d, more, 0.0)
    lhs = jnp.concatenate([h.astype(BF16) for h in heads], axis=1)
    for n in range(4):
        cols = pl.ds(512 * n, 512)
        out[:, cols] = (oacc[:, cols] + mm(lhs, os_[:, cols])).astype(BF16)

    mark("drain")
    sent(tok.at[pl.ds(0, 14)], S_TOK)
    sent(kbuf.at[pl.ds(0, 3)], S_K)
    sent(vbuf.at[pl.ds(0, 3)], S_V)
    sent(sx.at[pl.ds(0, 3)], S_SX)
    sent(xl.at[pl.ds(0, 7)], S_LA)

    @pl.when(a >= 1)
    def _():
        sent(qbuf.at[pl.ds(0, 2)], S_Q)

    for d in range(4):

        @pl.when(a == 3 - d)
        def _():
            if d:
                sent(sz.at[pl.ds(0, d)], S_SZ)
            pieces = sbuf.at[pl.ds(0, 7 + 8 * d)]
            sent(pieces if d < 3 else sbuf.at[pl.ds(0, 31), pl.ds(0, OUT_ROWS)], S_R)

    mark("")


def per_device(*args):
    args = list(args)
    args[1] = args[1].reshape(16, 128)
    args[6] = args[6].T
    args[9] = args[9].reshape(1, HD)
    vm = pltpu.VMEM
    return pl.pallas_call(
        kernel,
        out_shape=pltpu.VMEM((OUT_ROWS, D), BF16),
        in_specs=[pl.BlockSpec(memory_space=pl.ANY)] * 16,
        out_specs=pl.BlockSpec(memory_space=pltpu.VMEM),
        scratch_shapes=[
            vm((16, TOK, 128), BF16),
            vm((D, 1024), BF16),
            vm((32, D), BF16),
            vm((32, 128), BF16),
            vm((16, 128), BF16),
            vm((16, 128), F32),
            vm((TOK, 1024), F32),
            vm((TOK, 128), F32),
            vm((TOK, 128), F32),
            vm((1, TOK), BF16),
            vm((1, 128), F32),
            vm((1024, D), BF16),
            vm((1024, D), BF16),
            vm((128 * (LEVELS + 2), 128), BF16),
            vm((256, 256), BF16),
            vm((4, TOK + 16, 128), BF16),
            vm((4, TOK, 128), BF16),
            vm((4, TOK, 128), BF16),
            vm((TOK, 128), BF16),
            vm((TOK, 128), BF16),
            vm((TOK, 128), BF16),
            vm((TOK, 128), BF16),
            vm((TOK, 256), BF16),
            vm((TOK, 128), F32),
            vm((TOK, 128), F32),
            vm((CH, 128, 128), BF16),
            vm((TOK, 128), F32),
            vm((TOK, 128), BF16),
            vm((4, 144, 128), BF16),
            vm((4, 144, 128), BF16),
            vm((4, 4, TOK, 128), F32),
            vm((4, 4, TOK, 128), F32),
            vm((32, OUT_ROWS + TAIL, 128), BF16),
            vm((32, OUT_ROWS + TAIL, 128), BF16),
            vm((TOK, 128), BF16),
            vm((8, OUT_ROWS, 128), BF16),
            vm((OUT_ROWS, D), F32),
            pltpu.SemaphoreType.DMA((10,)),
            pltpu.SemaphoreType.DMA((N_S,)),
            pltpu.SemaphoreType.DMA((N_R,)),
        ],
        compiler_params=pltpu.CompilerParams(collective_id=0, has_side_effects=True),
        name="layer",
    )(*args)


def solution(mesh):
    torus = Mesh(mesh.devices.reshape(4, 4, 4, 2), ("z", "x", "y", "c"))
    sp, tp = ("z", "x"), ("y", "c")
    placed = (
        P(sp, tp), P(), P(None, tp), P(None, tp), P(None, tp), P(None, tp), P(), P(), P(sp, tp), P(),
        P(None, tp), P(None, tp), P(None, tp), P(tp, sp), P(), P(),
    )
    return jax.shard_map(
        per_device, mesh=torus, in_specs=placed, out_specs=P(sp + tp, None), check_vma=False
    )
```

```python
import jax
import jax.numpy as jnp
from jax import lax
from jax.experimental import pallas as pl
from jax.experimental.pallas import tpu as pltpu
from jax.sharding import Mesh
from jax.sharding import PartitionSpec as P

MESH = pl.DeviceIdType.MESH
F32 = jnp.float32
BF16 = jnp.bfloat16
LOG2E = 1.4426950408889634
EPS = 1e-6
SOFT = 16.0
TOK = 384
D = 2048
HD = 128
PARTS = 3
ROWS = TOK // PARTS
KPARTS = 2
KROWS = TOK // KPARTS
CH = TOK // 128
LEVELS = 7
TAIL = 8
OUT_ROWS = TOK // 8

S_TOK, S_K, S_V, S_Q, S_SX, S_SZ, S_LA, S_R, N_S = range(9)
R_AB, R_BA, R_CD = 0, PARTS, 2 * PARTS
R_P0, R_PM, R_PP, R_PO, R_KN, R_VN, R_KF, R_VF, R_SX, R_Q2, R_Q3, R_SZ, R_LA = [3 * PARTS + i for i in range(13)]
R_K = R_LA + 1
R_V = R_K + KPARTS
R_Q = R_V + KPARTS
R_R = R_Q + KPARTS
N_R = R_R + 16


PROFILE = False


class Marks:
    current = None

    def __call__(self, name):
        if not PROFILE:
            return
        if self.current is not None:
            self.current.__exit__(None, None, None)
        self.current = jax.named_scope(name) if name else None
        if name:
            self.current.__enter__()


def nt(a, b):
    return lax.dot_general(a, b, (((1,), (1,)), ((), ())), preferred_element_type=F32)


def tn(a, b):
    return lax.dot_general(a, b, (((0,), (0,)), ((), ())), preferred_element_type=F32)


def mm(a, b):
    return jnp.dot(a, b, preferred_element_type=F32)


def iota(shape, dim):
    return lax.broadcasted_iota(jnp.int32, shape, dim)


def split(x):
    hi = x.astype(BF16)
    return hi, (x - hi.astype(F32)).astype(BF16)


def rows_of(pieces):
    io = iota((16, 128), 0)
    out = jnp.zeros((16, 128), F32)
    for r, piece in enumerate(pieces):
        out = jnp.where(io == r, piece.astype(F32), out)
    return out.astype(BF16)


def kernel(
    tokens, gain, w_lq, w_lk, w_lv, w_lg, w_gd, w_gu, dob, lgain, w_sq, w_sk, w_sv, kbias, w_ol, w_os,
    out,
    tok, wbuf, gd, gu, gb, gf, acc, ss, dbuf, kb, lng, ol, os_,
    mcon, tri, kbuf, vbuf, qbuf, lq, lk, lv, lg, gs, ffrom, fall, sthis, lacc, qx, sx, sz, pbuf, tbuf, shares, sbuf, rbuf,
    linb, xl, oacc,
    lsem, ssem, rsem,
):
    mark = Marks()
    a, b = lax.axis_index("z"), lax.axis_index("x")
    y, c = lax.axis_index("y"), lax.axis_index("c")
    tp = 2 * y + c
    oc = 1 - c
    scale = HD ** (-0.5)

    def local(src, dst, i):
        cp = pltpu.make_async_copy(src, dst, lsem.at[i])
        cp.start()
        return cp

    def remote(src, dst, i, j, **dev):
        return pltpu.make_async_remote_copy(
            src_ref=src, dst_ref=dst, send_sem=ssem.at[i], recv_sem=rsem.at[j],
            device_id=dev, device_id_type=MESH,
        )

    def send(src, dst, i, j, **dev):
        remote(src, dst, i, j, **dev).start()

    def arrived(dst, j):
        remote(dst, dst, 0, j, c=oc).wait_recv()

    def sent(src, i):
        remote(src, src, i, 0, c=oc).wait_send()

    mark("load")
    base = 4 * y + 2 * c
    local(tokens.at[:, pl.ds(0, 128)], tok.at[base], 0)
    local(tokens.at[:, pl.ds(128, 128)], tok.at[base + 1], 0)
    barrier = pltpu.get_barrier_semaphore()
    for k in range(1, 4):
        pl.semaphore_signal(barrier, inc=1, device_id={"x": lax.rem(b + k, 4)}, device_id_type=MESH)

    @pl.when(a <= 2)
    def _():
        pl.semaphore_signal(barrier, inc=1, device_id={"z": a + 1}, device_id_type=MESH)

    @pl.when(a == 0)
    def _():
        pl.semaphore_signal(barrier, inc=1, device_id={"z": 3}, device_id_type=MESH)

    for k in range(1, 8):
        r = lax.rem(tp + k, 8)
        pl.semaphore_signal(
            barrier, inc=1, device_id={"y": r // 2, "c": lax.rem(r, 2)}, device_id_type=MESH
        )
    weights = [w_sk, w_sq, w_sv, w_lk, w_lv, None, w_lq, w_lg]
    for i, w in enumerate(weights):
        if w is not None:
            local(w, wbuf.at[:, pl.ds(128 * i, 128)], 1)
    gdl = local(w_gd, gd, 2)
    gainl = local(gain, gb, 3)
    kbl = local(kbias, kb, 4)
    gul = local(w_gu.at[:, pl.ds(pl.multiple_of(128 * tp, 128), 128)], gu, 5)
    dobl = local(dob, dbuf, 6)
    lngl = local(lgain, lng, 7)
    oll = local(w_ol, ol, 8)
    osl = local(w_os, os_, 9)

    t_i, s_i = iota((128, 128), 0), iota((128, 128), 1)
    mcon[pl.ds(0, 128), :] = jnp.where(s_i <= t_i, 1.0, 0.0).astype(BF16)
    mcon[pl.ds(128, 128), :] = jnp.where(s_i > t_i, 1.0, 0.0).astype(BF16)
    mark("barrier")
    own = tok.at[pl.ds(base, 2)]
    pltpu.make_async_copy(own, own, lsem.at[0]).wait()
    pl.semaphore_wait(barrier, 10 + (a + 1) // 2)

    mark("send")
    yp, ym, yo = lax.rem(y + 1, 4), lax.rem(y + 3, 4), lax.rem(y + 2, 4)

    def part(first, count, r):
        return tok.at[pl.ds(first, count), pl.ds(ROWS * r, ROWS), :]

    def send_part(first, count, r, j, **dev):
        ref = part(first, count, r)
        send(ref, ref, S_TOK, j, **dev)

    for r in range(PARTS):
        send_part(base, 1, r, R_AB + r, y=yp)
        send_part(base + 1, 1, r, R_AB + r, y=ym)
    for r in range(PARTS):
        send_part(base, 2, r, R_P0, c=oc)
    send_part(base + 1, 1, 0, R_BA, y=yp)
    send_part(base, 1, 0, R_BA, y=ym)

    for lev in range(LEVELS):
        same = (t_i >> lev) == (s_i >> lev)
        second = ((t_i >> lev) & 1) == 1
        m = jnp.where(same, jnp.where(second, jnp.where(s_i <= t_i, 1.0, 0.0), jnp.where(s_i > t_i, 1.0, 0.0)), 0.0)
        mcon[pl.ds(256 + 128 * lev, 128), :] = m.astype(BF16)
    tri[...] = jnp.where(iota((256, 256), 0) > iota((256, 256), 1), 1.0, 0.0).astype(BF16)
    for g in range(4):
        pbuf[g, 0] = jnp.zeros((TOK, HD), F32)
        tbuf[g, 0] = jnp.zeros((TOK, HD), F32)
    gainl.wait()
    gf[...] = gb[...].astype(F32)
    kbl.wait()
    kbuf[b, pl.ds(TOK, 16), :] = rows_of([kb[:, pl.ds(128 * r, 128)] for r in range(CH)])
    gdl.wait()
    for i in range(16):
        down = gd[:, pl.ds(128 * i, 128)].astype(F32)
        square = jnp.concatenate([down, jnp.zeros((96, 128), F32)], axis=0)
        wbuf[pl.ds(128 * i, 128), pl.ds(640, 128)] = jnp.transpose(square).astype(BF16)
    seven = wbuf.at[:, pl.ds(0, 896)]
    pltpu.make_async_copy(seven, seven, lsem.at[1]).wait()

    def scaled(block, count, first=False):
        pieces = []
        for j in range(count):
            x = tok[block + j].astype(F32)
            sq = x * x
            ss[...] = sq if (first and j == 0) else ss[...] + sq
            pieces.append((x * gf[pl.ds(block + j, 1), :]).astype(BF16))
        return jnp.concatenate(pieces, axis=1)

    def weight_rows(block, count):
        return pl.ds(pl.multiple_of(128 * block, 128), 128 * count)

    def fold_blocks(block, count, first=False):
        lhs = scaled(block, count, first)
        for n in range(4):
            cols = pl.ds(256 * n, 256)
            add = mm(lhs, wbuf[weight_rows(block, count), cols])
            acc[:, cols] = add if first else acc[:, cols] + add

    def fold(chip, first=False):
        fold_blocks(4 * chip, 4, first)

    def fold_two(one, two):
        lhs = scaled(one, 1), scaled(two, 1)
        for n in range(4):
            cols = pl.ds(256 * n, 256)
            add = mm(lhs[0], wbuf[weight_rows(one, 1), cols]) + mm(lhs[1], wbuf[weight_rows(two, 1), cols])
            acc[:, cols] = acc[:, cols] + add

    def fold_half(chip, core):
        fold_blocks(4 * chip + 2 * core, 2)

    mark("own")

    def partner(chip, j):
        arrived(tok.at[pl.ds(4 * chip + 2 * oc, 2)], j)

    def pass_far(r):
        arrived(part(4 * yo + 2 * c, 2, r), R_CD + r)
        send_part(4 * yo + 2 * c, 2, r, R_PO, c=oc)

    partner(y, R_P0)
    fold(y, True)
    mark("fwd")
    for r in range(PARTS):
        arrived(part(4 * ym + 2 * c, 2, r), R_AB + r)
        send_part(4 * ym + 2 * c, 1, r, R_CD + r, y=yp)
        send_part(4 * yp + 2 * c + 1, 1, r, R_CD + r, y=ym)
        if r + 1 < PARTS:
            send_part(base + 1, 1, r + 1, R_BA + r + 1, y=yp)
            send_part(base, 1, r + 1, R_BA + r + 1, y=ym)
        send_part(4 * ym + 2 * c, 1, r, R_PM, c=oc)
        send_part(4 * yp + 2 * c + 1, 1, r, R_PP, c=oc)
    mark("fold1")
    fold_two(4 * ym + 2 * c, 4 * yp + 2 * c + 1)
    mark("fwd1")
    for r in range(PARTS):
        arrived(part(4 * ym + 2 * c, 2, r), R_BA + r)
        send_part(4 * ym + 2 * c + 1, 1, r, R_PM, c=oc)
        send_part(4 * yp + 2 * c, 1, r, R_PP, c=oc)
        pass_far(r)
    mark("fold2")
    fold_two(4 * ym + 2 * c + 1, 4 * yp + 2 * c)
    fold_half(yo, c)
    mark("fold3")
    partner(ym, R_PM)
    fold_half(ym, oc)
    partner(yp, R_PP)
    fold_half(yp, oc)
    mark("fwd2")
    partner(yo, R_PO)

    xp, xm, xo = lax.rem(b + 1, 4), lax.rem(b + 3, 4), lax.rem(b + 2, 4)

    def krows(g, r):
        return kbuf.at[g, pl.ds(KROWS * r, KROWS + (16 if r == KPARTS - 1 else 0))]

    def vrows(g, r):
        return vbuf.at[g, pl.ds(KROWS * r, KROWS)]

    def qrows(d, r):
        return qbuf.at[d, pl.ds(KROWS * r, KROWS)]

    mark("finish")
    last = 4 * yo + 2 * oc
    lhs = scaled(last, 2)
    inv = lax.rsqrt(jnp.sum(ss[...], axis=1, keepdims=True) * (1.0 / D) + EPS)

    def finish(n):
        cols = pl.ds(256 * n, 256)
        total = acc[:, cols] + mm(lhs, wbuf[weight_rows(last, 2), cols])
        return (total * inv).astype(BF16)

    got = finish(0)
    kbuf[b, pl.ds(0, TOK), :] = got[:, :128]
    qbuf[0] = got[:, 128:]
    for r in range(KPARTS):
        send(krows(b, r), krows(b, r), S_K, R_K + r, x=xp)
        send(krows(b, r), krows(b, r), S_K, R_KN, x=xm)

    @pl.when(a >= 1)
    def _():
        for r in range(KPARTS):
            send(qrows(0, r), qrows(1, r), S_Q, R_Q + r, z=a - 1)

    @pl.when(a == 3)
    def _():
        send(qbuf.at[0], qbuf.at[3], S_Q, R_Q3, z=0)

    got = finish(1)
    vbuf[b] = got[:, :128]
    lk[...] = got[:, 128:]
    for r in range(KPARTS):
        send(vrows(b, r), vrows(b, r), S_V, R_V + r, x=xm)
        send(vrows(b, r), vrows(b, r), S_V, R_VN, x=xp)
    got = finish(2)
    lv[...] = got[:, :128]
    low = got[:, 128:160]
    got = finish(3)
    lq[...] = got[:, :128]
    lg[...] = got[:, 128:]

    mark("lstate")
    gul.wait()
    dobl.wait()
    pre = (mm(low, gu[...]) + dbuf[...]) * LOG2E
    decay = (jnp.minimum(pre, 0.0) - jnp.log2(1.0 + jnp.exp2(-jnp.abs(pre)))) * (1.0 / SOFT)
    ghi, glo = split(decay)
    gboth = jnp.concatenate([ghi, glo], axis=1)
    gs[...] = gboth
    state = jnp.zeros((HD, HD), F32)
    before = jnp.zeros((1, HD), F32)
    for n in range(CH):
        rows = slice(128 * n, 128 * n + 128)
        both = mm(mcon[pl.ds(0, 256), :], gboth[rows])
        dist = both[:, :128] + both[:, 128:]
        fade = jnp.exp2(dist)
        ffrom[rows, :] = fade[:128]
        fall[rows, :] = fade[:128] * jnp.exp2(before)
        if n:
            sthis[n] = state.astype(BF16)
        length = dist[127:128]
        ke = (lk[rows, :].astype(F32) * fade[128:]).astype(BF16)
        state = state * jnp.exp2(length) + tn(lv[rows, :], ke)
        before = before + length
    sx[b, pl.ds(0, HD), :] = state.astype(BF16)
    sx[b, pl.ds(HD, 16), :] = rows_of(split(before))
    for k in range(1, 4):
        send(sx.at[b], sx.at[b], S_SX, R_SX, x=lax.rem(b + k, 4))

    def linear_inside():
        apart = t_i ^ s_i
        for n in range(CH):
            rows = slice(128 * n, 128 * n + 128)
            both = mm(mcon[pl.ds(256, 128 * LEVELS), :], gs[rows, :])
            fade = jnp.exp2(both[:, :128] + both[:, 128:])
            qh, kh, vh = lq[rows, :], lk[rows, :], lv[rows, :]
            qf, kf = qh.astype(F32) * scale, kh.astype(F32)
            score = jnp.where(apart == 0, nt(qh, kh) * scale, 0.0)
            for lev in range(LEVELS):
                e = fade[128 * lev : 128 * lev + 128]
                part_score = nt((qf * e).astype(BF16), (kf * e).astype(BF16))
                score = jnp.where(((apart >> lev) == 1) & (t_i > s_i), part_score, score)
            inner = mm(score.astype(BF16), vh)
            if n:
                inner = inner + nt((qf * ffrom[rows, :]).astype(BF16), sthis[n])
            lacc[rows, :] = inner
            qx[rows, :] = (qf * fall[rows, :]).astype(BF16)

    mark("diag")
    def bias_of(g):
        head = kbuf[g, pl.ds(TOK, 16), :].astype(F32) * LOG2E
        return jnp.concatenate([head[r : r + 1] for r in range(CH)], axis=1)

    def pair(d, g, diagonal=False, slot=None):
        z = nt(qbuf[d], kbuf[g, pl.ds(0, TOK), :]) * (scale * LOG2E) + bias_of(g)
        soft = jnp.maximum(jnp.log2(1.0 + jnp.exp2(jnp.minimum(z, 126.0))), z)
        own = z - soft
        if diagonal:
            seen = iota((TOK, TOK), 1) < iota((TOK, TOK), 0)
            soft = jnp.where(seen, soft, 0.0)
        sb = soft.astype(BF16)
        near = mm(sb[:, 256:], tri[pl.ds(0, 128), pl.ds(0, 128)])
        near_total = near[:, :1] + soft[:, 256:257]
        far = mm(sb[:, :256], tri[...]) + near_total
        whole = far[:, :1] + soft[:, :1]
        share = jnp.exp2(own - jnp.concatenate([far, near], axis=1))
        if diagonal:
            share = jnp.where(seen, share, 0.0)
        tbuf[g, d] = jnp.broadcast_to(whole, (TOK, HD))
        if slot is None:
            pbuf[g, d] = mm(share.astype(BF16), vbuf[g])
        else:
            shares[slot] = share.astype(BF16)

    pair(0, b, True)

    def pass_keys(r):
        arrived(krows(xm, r), R_K + r)
        send(krows(xm, r), krows(xm, r), S_K, R_KF, x=xp)

    def pass_values(r):
        arrived(vrows(xp, r), R_V + r)
        send(vrows(xp, r), vrows(xp, r), S_V, R_VF, x=xm)

    def pass_queries(r):
        @pl.when(a <= 2)
        def _():
            arrived(qrows(1, r), R_Q + r)

        @pl.when((a >= 1) & (a <= 2))
        def _():
            send(qrows(1, r), qrows(2, r), S_Q, R_Q2, z=a - 1)

    lane = iota((16, 128), 1)

    def hand_on(d, home, oldest):
        total = jnp.zeros((TOK, HD), F32)
        behind = jnp.zeros((TOK, HD), F32)
        for g in range(3, -1, -1):
            counts = (g <= b) if home else True
            weight = jnp.exp2(-behind)
            total = total + (jnp.where(counts, weight * pbuf[g, d], 0.0) if home else weight * pbuf[g, d])
            behind = behind + (jnp.where(counts, tbuf[g, d], 0.0) if home else tbuf[g, d])
        for r in range(8):
            sbuf[8 * d + r, pl.ds(0, OUT_ROWS), :] = total[OUT_ROWS * r : OUT_ROWS * r + OUT_ROWS].astype(BF16)

        def leave(rows):
            for far in range(4):
                for flip in range(2):
                    to_y, to_c = lax.rem(y + 4 - far, 4), c if flip == 0 else oc
                    r = 2 * to_y + to_c
                    if home and far == 0 and flip == 0:
                        rbuf[tp] = sbuf[tp]
                        continue
                    dev = {"y": to_y, "c": to_c}
                    if not home:
                        dev["z"] = a + d
                    src, dst = sbuf.at[8 * d + r, pl.ds(0, rows)], rbuf.at[8 * d + tp, pl.ds(0, rows)]
                    send(src, dst, S_R, R_R + 4 * d + far, **dev)

        if oldest:
            leave(OUT_ROWS)
            return
        tiles = []
        for r in range(CH):
            line = jnp.transpose(behind[128 * r : 128 * r + 128])[0:1]
            tiles.append(rows_of(split(line)).astype(F32))
        for r in range(8):
            j, o = (OUT_ROWS * r) // 128, (OUT_ROWS * r) % 128
            tail = pltpu.roll(tiles[j], 128 - o, 1) if o else tiles[j]
            if o + OUT_ROWS > 128:
                tail = jnp.where(lane < 128 - o, tail, pltpu.roll(tiles[j + 1], 128 - o, 1))
            sbuf[8 * d + r, pl.ds(OUT_ROWS, TAIL), :] = tail[:TAIL].astype(BF16)
        leave(OUT_ROWS + TAIL)

    mark("home0")

    @pl.when((b == 0) & (a == 0))
    def _():
        hand_on(0, True, True)

    @pl.when((b == 0) & (a > 0))
    def _():
        hand_on(0, True, False)

    mark("linear1")
    linear_inside()
    mark("kvfwd")
    for r in range(KPARTS):
        pass_queries(r)
        pass_keys(r)
    mark("first")
    arrived(kbuf.at[xp], R_KN)

    @pl.when(a <= 2)
    def _():
        pair(1, b)
        pair(1, xm, slot=0)
        pair(1, xp, slot=1)

    @pl.when(a == 3)
    def _():
        pair(0, xm, slot=0)
        pair(0, xp, slot=1)

    mark("kvwait")
    for r in range(KPARTS):
        pass_values(r)
    mark("q3")

    @pl.when(a == 0)
    def _():
        arrived(qbuf.at[3], R_Q3)
        pair(3, b)

    arrived(vbuf.at[xm], R_VN)

    def values_in(d):
        pbuf[xm, d] = mm(shares[0], vbuf[xm])
        pbuf[xp, d] = mm(shares[1], vbuf[xp])

    mark("more")

    @pl.when(a == 0)
    def _():
        values_in(1)
        pair(3, xm)
        pair(3, xp)
        arrived(qbuf.at[2], R_Q2)
        pair(2, b)

    @pl.when((a == 1) | (a == 2))
    def _():
        values_in(1)

    @pl.when(a == 3)
    def _():
        values_in(0)

    mark("states")
    arrived(sx.at[pl.ds(0, 3)], R_SX)
    run = jnp.zeros((HD, HD), F32)
    run_len = jnp.zeros((1, HD), F32)
    pre_state, pre_len = run, run_len
    for g in range(4):
        pre_state = jnp.where(b == g, run, pre_state)
        pre_len = jnp.where(b == g, run_len, pre_len)
        tail = sx[g, pl.ds(HD, 16), :].astype(F32)
        length = tail[0:1] + tail[1:2]
        run = run * jnp.exp2(length) + sx[g, pl.ds(0, HD), :].astype(F32)
        run_len = run_len + length
    sz[a, pl.ds(0, HD), :] = run.astype(BF16)
    sz[a, pl.ds(HD, 16), :] = rows_of(split(run_len))
    for d in (3, 1):

        @pl.when(a + d <= 3)
        def _():
            send(sz.at[a], sz.at[a], S_SZ, R_SZ, z=a + d)

    @pl.when(a == 1)
    def _():
        arrived(qbuf.at[2], R_Q2)

    @pl.when(a <= 1)
    def _():
        send(sz.at[a], sz.at[a], S_SZ, R_SZ, z=a + 2)

    def add_group(g, carried):
        tail = sz[g, pl.ds(HD, 16), :].astype(F32)
        return carried * jnp.exp2(tail[0:1] + tail[1:2]) + sz[g, pl.ds(0, HD), :].astype(F32)

    def span(r):
        return pl.ds(pl.multiple_of(OUT_ROWS * r, 16), OUT_ROWS)

    lngl.wait()

    def linear_out():
        older = lax.fori_loop(0, a, add_group, jnp.zeros((HD, HD), F32))
        incoming = pre_state + older * jnp.exp2(pre_len)
        raw = lacc[...] + nt(qx[...], incoming.astype(BF16))
        normed = raw * lax.rsqrt(jnp.mean(raw * raw, axis=1, keepdims=True) + EPS) * lng[...]
        gate = lg[...].astype(F32)
        linb[...] = (normed * (gate / (1.0 + jnp.exp2(gate * (-LOG2E))))).astype(BF16)
        for k in range(1, 8):
            r = lax.rem(tp + k, 8)
            send(linb.at[span(r)], xl.at[tp], S_LA, R_LA, y=r // 2, c=lax.rem(r, 2))
        xl[tp] = linb[span(tp), :]

    mark("lout0")

    @pl.when(a == 1)
    def _():
        pair(2, b)
        pair(2, xm)
        pair(2, xp)

    @pl.when(a == 0)
    def _():
        linear_out()
        pair(2, xm)
        pair(2, xp)

    mark("kvwait2")
    arrived(kbuf.at[xo], R_KF)
    arrived(vbuf.at[xo], R_VF)
    mark("serve")

    @pl.when(a == 0)
    def _():
        pair(1, xo)
        pair(3, xo)
        hand_on(1, False, True)
        hand_on(3, False, True)

    @pl.when(a == 1)
    def _():
        pair(1, xo)
        pair(2, xo)

    @pl.when(a == 2)
    def _():
        pair(1, xo)

    mark("lout1")

    @pl.when(a >= 1)
    def _():
        for d in range(1, 4):

            @pl.when(a == d)
            def _():
                arrived(sz.at[pl.ds(0, d)], R_SZ)

        linear_out()

    mark("hand")

    @pl.when(a == 1)
    def _():
        hand_on(1, False, False)
        hand_on(2, False, False)

    @pl.when(a == 2)
    def _():
        hand_on(1, False, False)

    mark("home")

    def triple(d):
        pair(d, xm)
        pair(d, xp)
        pair(d, xo)

    @pl.when((a == 0) & (b > 0))
    def _():
        pair(2, xo)
        hand_on(2, False, True)
        triple(0)
        hand_on(0, True, True)

    @pl.when((a == 0) & (b == 0))
    def _():
        pair(2, xo)
        hand_on(2, False, True)

    @pl.when(((a == 1) | (a == 2)) & (b > 0))
    def _():
        triple(0)
        hand_on(0, True, False)

    @pl.when((a == 3) & (b > 0))
    def _():
        pair(0, xo)
        hand_on(0, True, False)

    mark("linx")
    oll.wait()
    arrived(xl.at[pl.ds(0, 7)], R_LA)
    mark("linproj")
    lhs = jnp.concatenate([xl[i] for i in range(8)], axis=1)
    for n in range(4):
        cols = pl.ds(512 * n, 512)
        oacc[:, cols] = mm(lhs, ol[:, cols])

    mark("ret0")
    osl.wait()
    def returned(d, far):
        chip = lax.rem(y + far, 4)
        first, count = (2 * chip, 2) if d or far else (0, 1)

        @pl.when(a == d)
        def _():
            arrived(rbuf.at[pl.ds(8 * d + first, count), pl.ds(0, OUT_ROWS)], R_R + 4 * d + far)

        @pl.when(a > d)
        def _():
            arrived(rbuf.at[pl.ds(8 * d + first, count)], R_R + 4 * d + far)

    sub = iota((8, 128), 0)

    mark("stproj")

    @pl.when(a == 0)
    def _():
        for far in (0, 1, 3, 2):
            returned(0, far)
            first = 2 * lax.rem(y + far, 4)
            lhs = jnp.concatenate([rbuf[first + i, pl.ds(0, OUT_ROWS), :] for i in range(2)], axis=1)
            for n in range(4):
                cols = pl.ds(512 * n, 512)
                rows = pl.ds(pl.multiple_of(128 * first, 256), 256)
                total = oacc[:, cols] + mm(lhs, os_[rows, cols])
                if far == 2:
                    out[:, cols] = total.astype(BF16)
                else:
                    oacc[:, cols] = total

    @pl.when(a > 0)
    def _():
        for far in range(4):
            for d in range(4):
                returned(d, far)
        behind = jnp.zeros((8, 128), F32)
        heads = [rbuf[i, pl.ds(0, OUT_ROWS), :].astype(F32) for i in range(8)]
        for d in range(1, 4):
            for i in range(8):
                tail = rbuf[8 * d - 8 + i, pl.ds(OUT_ROWS, TAIL), :].astype(F32)
                behind = behind + jnp.where(sub == i, tail[0:1] + tail[1:2], 0.0)
            left = jnp.transpose(jnp.exp2(-behind))
            for i in range(8):
                more = left[:OUT_ROWS, i : i + 1] * rbuf[8 * d + i, pl.ds(0, OUT_ROWS), :].astype(F32)
                heads[i] = heads[i] + jnp.where(a >= d, more, 0.0)
        lhs = jnp.concatenate([h.astype(BF16) for h in heads], axis=1)
        for n in range(4):
            cols = pl.ds(512 * n, 512)
            out[:, cols] = (oacc[:, cols] + mm(lhs, os_[:, cols])).astype(BF16)

    mark("drain")
    sent(tok.at[pl.ds(0, 14)], S_TOK)
    sent(kbuf.at[pl.ds(0, 3)], S_K)
    sent(vbuf.at[pl.ds(0, 3)], S_V)
    sent(sx.at[pl.ds(0, 3)], S_SX)
    sent(xl.at[pl.ds(0, 7)], S_LA)

    @pl.when(a >= 1)
    def _():
        sent(qbuf.at[pl.ds(0, 2)], S_Q)

    for d in range(4):

        @pl.when(a == 3 - d)
        def _():
            if d:
                sent(sz.at[pl.ds(0, d)], S_SZ)
            pieces = sbuf.at[pl.ds(0, 7 + 8 * d)]
            sent(pieces if d < 3 else sbuf.at[pl.ds(0, 31), pl.ds(0, OUT_ROWS)], S_R)

    mark("")


def per_device(*args):
    args = list(args)
    args[1] = args[1].reshape(16, 128)
    args[6] = args[6].T
    args[9] = args[9].reshape(1, HD)
    vm = pltpu.VMEM
    return pl.pallas_call(
        kernel,
        out_shape=pltpu.VMEM((OUT_ROWS, D), BF16),
        in_specs=[pl.BlockSpec(memory_space=pl.ANY)] * 16,
        out_specs=pl.BlockSpec(memory_space=pltpu.VMEM),
        scratch_shapes=[
            vm((16, TOK, 128), BF16),
            vm((D, 1024), BF16),
            vm((32, D), BF16),
            vm((32, 128), BF16),
            vm((16, 128), BF16),
            vm((16, 128), F32),
            vm((TOK, 1024), F32),
            vm((TOK, 128), F32),
            vm((TOK, 128), F32),
            vm((1, TOK), BF16),
            vm((1, 128), F32),
            vm((1024, D), BF16),
            vm((1024, D), BF16),
            vm((128 * (LEVELS + 2), 128), BF16),
            vm((256, 256), BF16),
            vm((4, TOK + 16, 128), BF16),
            vm((4, TOK, 128), BF16),
            vm((4, TOK, 128), BF16),
            vm((TOK, 128), BF16),
            vm((TOK, 128), BF16),
            vm((TOK, 128), BF16),
            vm((TOK, 128), BF16),
            vm((TOK, 256), BF16),
            vm((TOK, 128), F32),
            vm((TOK, 128), F32),
            vm((CH, 128, 128), BF16),
            vm((TOK, 128), F32),
            vm((TOK, 128), BF16),
            vm((4, 144, 128), BF16),
            vm((4, 144, 128), BF16),
            vm((4, 4, TOK, 128), F32),
            vm((4, 4, TOK, 128), F32),
            vm((2, TOK, TOK), BF16),
            vm((32, OUT_ROWS + TAIL, 128), BF16),
            vm((32, OUT_ROWS + TAIL, 128), BF16),
            vm((TOK, 128), BF16),
            vm((8, OUT_ROWS, 128), BF16),
            vm((OUT_ROWS, D), F32),
            pltpu.SemaphoreType.DMA((10,)),
            pltpu.SemaphoreType.DMA((N_S,)),
            pltpu.SemaphoreType.DMA((N_R,)),
        ],
        compiler_params=pltpu.CompilerParams(collective_id=0, has_side_effects=True),
        name="layer",
    )(*args)


def solution(mesh):
    torus = Mesh(mesh.devices.reshape(4, 4, 4, 2), ("z", "x", "y", "c"))
    sp, tp = ("z", "x"), ("y", "c")
    placed = (
        P(sp, tp), P(), P(None, tp), P(None, tp), P(None, tp), P(None, tp), P(), P(), P(sp, tp), P(),
        P(None, tp), P(None, tp), P(None, tp), P(tp, sp), P(), P(),
    )
    return jax.shard_map(
        per_device, mesh=torus, in_specs=placed, out_specs=P(sp + tp, None), check_vma=False
    )
```

```python
import jax
import jax.numpy as jnp
from jax import lax
from jax.experimental import pallas as pl
from jax.experimental.pallas import tpu as pltpu
from jax.sharding import Mesh
from jax.sharding import PartitionSpec as P

MESH = pl.DeviceIdType.MESH
F32 = jnp.float32
BF16 = jnp.bfloat16
LOG2E = 1.4426950408889634
EPS = 1e-6
SOFT = 16.0
TOK = 384
D = 2048
HD = 128
PARTS = 3
ROWS = TOK // PARTS
KPARTS = 2
KROWS = TOK // KPARTS
CH = TOK // 128
LEVELS = 7
TAIL = 8
OUT_ROWS = TOK // 8

S_TOK, S_K, S_V, S_Q, S_SX, S_SZ, S_LA, S_R, N_S = range(9)
R_AB, R_BA, R_CD = 0, PARTS, 2 * PARTS
R_P0, R_PM, R_PP, R_PO, R_KN, R_VN, R_KF, R_VF, R_SX, R_Q2, R_Q3, R_SZ, R_LA = [3 * PARTS + i for i in range(13)]
R_K = R_LA + 1
R_V = R_K + KPARTS
R_Q = R_V + KPARTS
R_R = R_Q + KPARTS
N_R = R_R + 16


PROFILE = False


class Marks:
    current = None

    def __call__(self, name):
        if not PROFILE:
            return
        if self.current is not None:
            self.current.__exit__(None, None, None)
        self.current = jax.named_scope(name) if name else None
        if name:
            self.current.__enter__()


def nt(a, b):
    return lax.dot_general(a, b, (((1,), (1,)), ((), ())), preferred_element_type=F32)


def tn(a, b):
    return lax.dot_general(a, b, (((0,), (0,)), ((), ())), preferred_element_type=F32)


def mm(a, b):
    return jnp.dot(a, b, preferred_element_type=F32)


def iota(shape, dim):
    return lax.broadcasted_iota(jnp.int32, shape, dim)


def split(x):
    hi = x.astype(BF16)
    return hi, (x - hi.astype(F32)).astype(BF16)


def rows_of(pieces):
    io = iota((16, 128), 0)
    out = jnp.zeros((16, 128), F32)
    for r, piece in enumerate(pieces):
        out = jnp.where(io == r, piece.astype(F32), out)
    return out.astype(BF16)


def kernel(
    tokens, gain, w_lq, w_lk, w_lv, w_lg, w_gd, w_gu, dob, lgain, w_sq, w_sk, w_sv, kbias, w_ol, w_os,
    out,
    tok, wbuf, gd, gu, gb, gf, acc, ss, dbuf, kb, lng, ol, os_,
    mcon, tri, kbuf, vbuf, qbuf, lq, lk, lv, lg, gs, ffrom, fall, sthis, lacc, qx, sx, sz, pbuf, tbuf, shares, sbuf, rbuf,
    linb, xl, oacc,
    lsem, ssem, rsem,
):
    mark = Marks()
    a, b = lax.axis_index("z"), lax.axis_index("x")
    y, c = lax.axis_index("y"), lax.axis_index("c")
    tp = 2 * y + c
    oc = 1 - c
    scale = HD ** (-0.5)

    def local(src, dst, i):
        cp = pltpu.make_async_copy(src, dst, lsem.at[i])
        cp.start()
        return cp

    def remote(src, dst, i, j, **dev):
        return pltpu.make_async_remote_copy(
            src_ref=src, dst_ref=dst, send_sem=ssem.at[i], recv_sem=rsem.at[j],
            device_id=dev, device_id_type=MESH,
        )

    def send(src, dst, i, j, **dev):
        remote(src, dst, i, j, **dev).start()

    def arrived(dst, j):
        remote(dst, dst, 0, j, c=oc).wait_recv()

    def sent(src, i):
        remote(src, src, i, 0, c=oc).wait_send()

    mark("load")
    base = 4 * y + 2 * c
    local(tokens.at[:, pl.ds(0, 128)], tok.at[base], 0)
    local(tokens.at[:, pl.ds(128, 128)], tok.at[base + 1], 0)
    barrier = pltpu.get_barrier_semaphore()
    for k in range(1, 4):
        pl.semaphore_signal(barrier, inc=1, device_id={"x": lax.rem(b + k, 4)}, device_id_type=MESH)

    @pl.when(a <= 2)
    def _():
        pl.semaphore_signal(barrier, inc=1, device_id={"z": a + 1}, device_id_type=MESH)

    @pl.when(a == 0)
    def _():
        pl.semaphore_signal(barrier, inc=1, device_id={"z": 3}, device_id_type=MESH)

    for k in range(1, 8):
        r = lax.rem(tp + k, 8)
        pl.semaphore_signal(
            barrier, inc=1, device_id={"y": r // 2, "c": lax.rem(r, 2)}, device_id_type=MESH
        )
    weights = [w_sk, w_sq, w_sv, w_lk, w_lv, None, w_lq, w_lg]
    for i, w in enumerate(weights):
        if w is not None:
            local(w, wbuf.at[:, pl.ds(128 * i, 128)], 1)
    gdl = local(w_gd, gd, 2)
    gainl = local(gain, gb, 3)
    kbl = local(kbias, kb, 4)
    gul = local(w_gu.at[:, pl.ds(pl.multiple_of(128 * tp, 128), 128)], gu, 5)
    dobl = local(dob, dbuf, 6)
    lngl = local(lgain, lng, 7)
    oll = local(w_ol, ol, 8)
    osl = local(w_os, os_, 9)

    t_i, s_i = iota((128, 128), 0), iota((128, 128), 1)
    mcon[pl.ds(0, 128), :] = jnp.where(s_i <= t_i, 1.0, 0.0).astype(BF16)
    mcon[pl.ds(128, 128), :] = jnp.where(s_i > t_i, 1.0, 0.0).astype(BF16)
    mark("barrier")
    own = tok.at[pl.ds(base, 2)]
    pltpu.make_async_copy(own, own, lsem.at[0]).wait()
    pl.semaphore_wait(barrier, 10 + (a + 1) // 2)

    mark("send")
    yp, ym, yo = lax.rem(y + 1, 4), lax.rem(y + 3, 4), lax.rem(y + 2, 4)

    def part(first, count, r):
        return tok.at[pl.ds(first, count), pl.ds(ROWS * r, ROWS), :]

    def send_part(first, count, r, j, **dev):
        ref = part(first, count, r)
        send(ref, ref, S_TOK, j, **dev)

    for r in range(PARTS):
        send_part(base, 1, r, R_AB + r, y=yp)
        send_part(base + 1, 1, r, R_AB + r, y=ym)
    for r in range(PARTS):
        send_part(base, 2, r, R_P0, c=oc)
    send_part(base + 1, 1, 0, R_BA, y=yp)
    send_part(base, 1, 0, R_BA, y=ym)

    for lev in range(LEVELS):
        same = (t_i >> lev) == (s_i >> lev)
        second = ((t_i >> lev) & 1) == 1
        m = jnp.where(same, jnp.where(second, jnp.where(s_i <= t_i, 1.0, 0.0), jnp.where(s_i > t_i, 1.0, 0.0)), 0.0)
        mcon[pl.ds(256 + 128 * lev, 128), :] = m.astype(BF16)
    tri[...] = jnp.where(iota((256, 256), 0) > iota((256, 256), 1), 1.0, 0.0).astype(BF16)
    for g in range(4):
        pbuf[g, 0] = jnp.zeros((TOK, HD), F32)
        tbuf[g, 0] = jnp.zeros((TOK, HD), F32)
    gainl.wait()
    gf[...] = gb[...].astype(F32)
    kbl.wait()
    kbuf[b, pl.ds(TOK, 16), :] = rows_of([kb[:, pl.ds(128 * r, 128)] for r in range(CH)])
    gdl.wait()
    for i in range(16):
        down = gd[:, pl.ds(128 * i, 128)].astype(F32)
        square = jnp.concatenate([down, jnp.zeros((96, 128), F32)], axis=0)
        wbuf[pl.ds(128 * i, 128), pl.ds(640, 128)] = jnp.transpose(square).astype(BF16)
    seven = wbuf.at[:, pl.ds(0, 896)]
    pltpu.make_async_copy(seven, seven, lsem.at[1]).wait()

    def scaled(block, count, first=False):
        pieces = []
        for j in range(count):
            x = tok[block + j].astype(F32)
            sq = x * x
            ss[...] = sq if (first and j == 0) else ss[...] + sq
            pieces.append((x * gf[pl.ds(block + j, 1), :]).astype(BF16))
        return jnp.concatenate(pieces, axis=1)

    def weight_rows(block, count):
        return pl.ds(pl.multiple_of(128 * block, 128), 128 * count)

    def fold_blocks(block, count, first=False):
        lhs = scaled(block, count, first)
        for n in range(4):
            cols = pl.ds(256 * n, 256)
            add = mm(lhs, wbuf[weight_rows(block, count), cols])
            acc[:, cols] = add if first else acc[:, cols] + add

    def fold(chip, first=False):
        fold_blocks(4 * chip, 4, first)

    def fold_two(one, two):
        lhs = scaled(one, 1), scaled(two, 1)
        for n in range(4):
            cols = pl.ds(256 * n, 256)
            add = mm(lhs[0], wbuf[weight_rows(one, 1), cols]) + mm(lhs[1], wbuf[weight_rows(two, 1), cols])
            acc[:, cols] = acc[:, cols] + add

    def fold_half(chip, core):
        fold_blocks(4 * chip + 2 * core, 2)

    mark("own")

    def partner(chip, j):
        arrived(tok.at[pl.ds(4 * chip + 2 * oc, 2)], j)

    def pass_far(r):
        arrived(part(4 * yo + 2 * c, 2, r), R_CD + r)
        send_part(4 * yo + 2 * c, 2, r, R_PO, c=oc)

    partner(y, R_P0)
    fold(y, True)
    mark("fwd")
    for r in range(PARTS):
        arrived(part(4 * ym + 2 * c, 2, r), R_AB + r)
        send_part(4 * ym + 2 * c, 1, r, R_CD + r, y=yp)
        send_part(4 * yp + 2 * c + 1, 1, r, R_CD + r, y=ym)
        if r + 1 < PARTS:
            send_part(base + 1, 1, r + 1, R_BA + r + 1, y=yp)
            send_part(base, 1, r + 1, R_BA + r + 1, y=ym)
        send_part(4 * ym + 2 * c, 1, r, R_PM, c=oc)
        send_part(4 * yp + 2 * c + 1, 1, r, R_PP, c=oc)
    mark("fold1")
    fold_two(4 * ym + 2 * c, 4 * yp + 2 * c + 1)
    mark("fwd1")
    for r in range(PARTS):
        arrived(part(4 * ym + 2 * c, 2, r), R_BA + r)
        send_part(4 * ym + 2 * c + 1, 1, r, R_PM, c=oc)
        send_part(4 * yp + 2 * c, 1, r, R_PP, c=oc)
        pass_far(r)
    mark("fold2")
    fold_two(4 * ym + 2 * c + 1, 4 * yp + 2 * c)
    fold_half(yo, c)
    mark("fold3")
    partner(ym, R_PM)
    fold_half(ym, oc)
    partner(yp, R_PP)
    fold_half(yp, oc)
    mark("fwd2")
    partner(yo, R_PO)

    xp, xm, xo = lax.rem(b + 1, 4), lax.rem(b + 3, 4), lax.rem(b + 2, 4)

    def krows(g, r):
        return kbuf.at[g, pl.ds(KROWS * r, KROWS + (16 if r == KPARTS - 1 else 0))]

    def vrows(g, r):
        return vbuf.at[g, pl.ds(KROWS * r, KROWS)]

    def qrows(d, r):
        return qbuf.at[d, pl.ds(KROWS * r, KROWS)]

    mark("finish")
    last = 4 * yo + 2 * oc
    lhs = scaled(last, 2)
    inv = lax.rsqrt(jnp.sum(ss[...], axis=1, keepdims=True) * (1.0 / D) + EPS)

    def finish(n):
        cols = pl.ds(256 * n, 256)
        total = acc[:, cols] + mm(lhs, wbuf[weight_rows(last, 2), cols])
        return (total * inv).astype(BF16)

    got = finish(0)
    kbuf[b, pl.ds(0, TOK), :] = got[:, :128]
    qbuf[0] = got[:, 128:]
    for r in range(KPARTS):
        send(krows(b, r), krows(b, r), S_K, R_K + r, x=xp)
        send(krows(b, r), krows(b, r), S_K, R_KN, x=xm)

    @pl.when(a >= 1)
    def _():
        for r in range(KPARTS):
            send(qrows(0, r), qrows(1, r), S_Q, R_Q + r, z=a - 1)

    @pl.when(a == 3)
    def _():
        send(qbuf.at[0], qbuf.at[3], S_Q, R_Q3, z=0)

    got = finish(1)
    vbuf[b] = got[:, :128]
    lk[...] = got[:, 128:]
    for r in range(KPARTS):
        send(vrows(b, r), vrows(b, r), S_V, R_V + r, x=xm)
        send(vrows(b, r), vrows(b, r), S_V, R_VN, x=xp)
    got = finish(2)
    lv[...] = got[:, :128]
    low = got[:, 128:160]
    got = finish(3)
    lq[...] = got[:, :128]
    lg[...] = got[:, 128:]

    mark("lstate")
    gul.wait()
    dobl.wait()
    pre = (mm(low, gu[...]) + dbuf[...]) * LOG2E
    decay = (jnp.minimum(pre, 0.0) - jnp.log2(1.0 + jnp.exp2(-jnp.abs(pre)))) * (1.0 / SOFT)
    ghi, glo = split(decay)
    gboth = jnp.concatenate([ghi, glo], axis=1)
    gs[...] = gboth
    state = jnp.zeros((HD, HD), F32)
    before = jnp.zeros((1, HD), F32)
    for n in range(CH):
        rows = slice(128 * n, 128 * n + 128)
        both = mm(mcon[pl.ds(0, 256), :], gboth[rows])
        dist = both[:, :128] + both[:, 128:]
        fade = jnp.exp2(dist)
        ffrom[rows, :] = fade[:128]
        fall[rows, :] = fade[:128] * jnp.exp2(before)
        if n:
            sthis[n] = state.astype(BF16)
        length = dist[127:128]
        ke = (lk[rows, :].astype(F32) * fade[128:]).astype(BF16)
        state = state * jnp.exp2(length) + tn(lv[rows, :], ke)
        before = before + length
    sx[b, pl.ds(0, HD), :] = state.astype(BF16)
    sx[b, pl.ds(HD, 16), :] = rows_of(split(before))
    for k in range(1, 4):
        send(sx.at[b], sx.at[b], S_SX, R_SX, x=lax.rem(b + k, 4))

    def linear_inside():
        apart = t_i ^ s_i
        for n in range(CH):
            rows = slice(128 * n, 128 * n + 128)
            both = mm(mcon[pl.ds(256, 128 * LEVELS), :], gs[rows, :])
            fade = jnp.exp2(both[:, :128] + both[:, 128:])
            qh, kh, vh = lq[rows, :], lk[rows, :], lv[rows, :]
            qf, kf = qh.astype(F32) * scale, kh.astype(F32)
            score = jnp.where(apart == 0, nt(qh, kh) * scale, 0.0)
            for lev in range(LEVELS):
                e = fade[128 * lev : 128 * lev + 128]
                part_score = nt((qf * e).astype(BF16), (kf * e).astype(BF16))
                score = jnp.where(((apart >> lev) == 1) & (t_i > s_i), part_score, score)
            inner = mm(score.astype(BF16), vh)
            if n:
                inner = inner + nt((qf * ffrom[rows, :]).astype(BF16), sthis[n])
            lacc[rows, :] = inner
            qx[rows, :] = (qf * fall[rows, :]).astype(BF16)

    mark("diag")
    def bias_of(g):
        head = kbuf[g, pl.ds(TOK, 16), :].astype(F32) * LOG2E
        return jnp.concatenate([head[r : r + 1] for r in range(CH)], axis=1)

    def pair(d, g, diagonal=False, slot=None):
        z = nt(qbuf[d], kbuf[g, pl.ds(0, TOK), :]) * (scale * LOG2E) + bias_of(g)
        soft = jnp.maximum(jnp.log2(1.0 + jnp.exp2(jnp.minimum(z, 126.0))), z)
        own = z - soft
        if diagonal:
            seen = iota((TOK, TOK), 1) < iota((TOK, TOK), 0)
            soft = jnp.where(seen, soft, 0.0)
        sb = soft.astype(BF16)
        near = mm(sb[:, 256:], tri[pl.ds(0, 128), pl.ds(0, 128)])
        near_total = near[:, :1] + soft[:, 256:257]
        far = mm(sb[:, :256], tri[...]) + near_total
        whole = far[:, :1] + soft[:, :1]
        share = jnp.exp2(own - jnp.concatenate([far, near], axis=1))
        if diagonal:
            share = jnp.where(seen, share, 0.0)
        tbuf[g, d] = jnp.broadcast_to(whole, (TOK, HD))
        if slot is None:
            pbuf[g, d] = mm(share.astype(BF16), vbuf[g])
        else:
            shares[slot] = share.astype(BF16)

    pair(0, b, True)

    def pass_keys(r):
        arrived(krows(xm, r), R_K + r)
        send(krows(xm, r), krows(xm, r), S_K, R_KF, x=xp)

    def pass_values(r):
        arrived(vrows(xp, r), R_V + r)
        send(vrows(xp, r), vrows(xp, r), S_V, R_VF, x=xm)

    def pass_queries(r):
        @pl.when(a <= 2)
        def _():
            arrived(qrows(1, r), R_Q + r)

        @pl.when((a >= 1) & (a <= 2))
        def _():
            send(qrows(1, r), qrows(2, r), S_Q, R_Q2, z=a - 1)

    lane = iota((16, 128), 1)

    def hand_on(d, home, oldest):
        def counted(g, value):
            return jnp.where(g <= b, value, 0.0) if home else value

        total, behind = counted(3, pbuf[3, d]), counted(3, tbuf[3, d])
        for g in range(2, -1, -1):
            total = total + counted(g, jnp.exp2(-behind) * pbuf[g, d])
            if g or not oldest:
                behind = behind + counted(g, tbuf[g, d])
        for r in range(8):
            sbuf[8 * d + r, pl.ds(0, OUT_ROWS), :] = total[OUT_ROWS * r : OUT_ROWS * r + OUT_ROWS].astype(BF16)

        def leave(rows):
            for far in range(4):
                for flip in range(2):
                    to_y, to_c = lax.rem(y + 4 - far, 4), c if flip == 0 else oc
                    r = 2 * to_y + to_c
                    if home and far == 0 and flip == 0:
                        rbuf[tp] = sbuf[tp]
                        continue
                    dev = {"y": to_y, "c": to_c}
                    if not home:
                        dev["z"] = a + d
                    src, dst = sbuf.at[8 * d + r, pl.ds(0, rows)], rbuf.at[8 * d + tp, pl.ds(0, rows)]
                    send(src, dst, S_R, R_R + 4 * d + far, **dev)

        if oldest:
            leave(OUT_ROWS)
            return
        tiles = []
        for r in range(CH):
            line = jnp.transpose(behind[128 * r : 128 * r + 128])[0:1]
            tiles.append(rows_of(split(line)).astype(F32))
        for r in range(8):
            j, o = (OUT_ROWS * r) // 128, (OUT_ROWS * r) % 128
            tail = pltpu.roll(tiles[j], 128 - o, 1) if o else tiles[j]
            if o + OUT_ROWS > 128:
                tail = jnp.where(lane < 128 - o, tail, pltpu.roll(tiles[j + 1], 128 - o, 1))
            sbuf[8 * d + r, pl.ds(OUT_ROWS, TAIL), :] = tail[:TAIL].astype(BF16)
        leave(OUT_ROWS + TAIL)

    mark("home0")

    @pl.when((b == 0) & (a == 0))
    def _():
        hand_on(0, True, True)

    @pl.when((b == 0) & (a > 0))
    def _():
        hand_on(0, True, False)

    mark("linear1")
    linear_inside()
    mark("kvfwd")
    for r in range(KPARTS):
        pass_queries(r)
        pass_keys(r)
    mark("first")
    arrived(kbuf.at[xp], R_KN)

    @pl.when(a <= 2)
    def _():
        pair(1, b)
        pair(1, xm, slot=0)
        pair(1, xp, slot=1)

    @pl.when(a == 3)
    def _():
        pair(0, xm, slot=0)
        pair(0, xp, slot=1)

    mark("kvwait")
    for r in range(KPARTS):
        pass_values(r)
    mark("q3")

    @pl.when(a == 0)
    def _():
        arrived(qbuf.at[3], R_Q3)
        pair(3, b)

    arrived(vbuf.at[xm], R_VN)

    def values_in(d):
        pbuf[xm, d] = mm(shares[0], vbuf[xm])
        pbuf[xp, d] = mm(shares[1], vbuf[xp])

    mark("more")

    @pl.when(a == 0)
    def _():
        values_in(1)
        pair(3, xm)
        pair(3, xp)
        arrived(qbuf.at[2], R_Q2)
        pair(2, b)

    @pl.when((a == 1) | (a == 2))
    def _():
        values_in(1)

    @pl.when(a == 3)
    def _():
        values_in(0)

    mark("states")
    arrived(sx.at[pl.ds(0, 3)], R_SX)
    run = jnp.zeros((HD, HD), F32)
    run_len = jnp.zeros((1, HD), F32)
    pre_state, pre_len = run, run_len
    for g in range(4):
        pre_state = jnp.where(b == g, run, pre_state)
        pre_len = jnp.where(b == g, run_len, pre_len)
        tail = sx[g, pl.ds(HD, 16), :].astype(F32)
        length = tail[0:1] + tail[1:2]
        run = run * jnp.exp2(length) + sx[g, pl.ds(0, HD), :].astype(F32)
        run_len = run_len + length
    sz[a, pl.ds(0, HD), :] = run.astype(BF16)
    sz[a, pl.ds(HD, 16), :] = rows_of(split(run_len))
    for d in (3, 1):

        @pl.when(a + d <= 3)
        def _():
            send(sz.at[a], sz.at[a], S_SZ, R_SZ, z=a + d)

    @pl.when(a == 1)
    def _():
        arrived(qbuf.at[2], R_Q2)

    @pl.when(a <= 1)
    def _():
        send(sz.at[a], sz.at[a], S_SZ, R_SZ, z=a + 2)

    def add_group(g, carried):
        tail = sz[g, pl.ds(HD, 16), :].astype(F32)
        return carried * jnp.exp2(tail[0:1] + tail[1:2]) + sz[g, pl.ds(0, HD), :].astype(F32)

    def span(r):
        return pl.ds(pl.multiple_of(OUT_ROWS * r, 16), OUT_ROWS)

    lngl.wait()

    def linear_out():
        older = lax.fori_loop(0, a, add_group, jnp.zeros((HD, HD), F32))
        incoming = pre_state + older * jnp.exp2(pre_len)
        raw = lacc[...] + nt(qx[...], incoming.astype(BF16))
        normed = raw * lax.rsqrt(jnp.mean(raw * raw, axis=1, keepdims=True) + EPS) * lng[...]
        gate = lg[...].astype(F32)
        linb[...] = (normed * (gate / (1.0 + jnp.exp2(gate * (-LOG2E))))).astype(BF16)
        for k in range(1, 8):
            r = lax.rem(tp + k, 8)
            send(linb.at[span(r)], xl.at[tp], S_LA, R_LA, y=r // 2, c=lax.rem(r, 2))
        xl[tp] = linb[span(tp), :]

    mark("lout0")

    @pl.when(a == 1)
    def _():
        pair(2, b)
        pair(2, xm)
        pair(2, xp)

    @pl.when(a == 0)
    def _():
        linear_out()
        pair(2, xm)
        pair(2, xp)

    mark("kvwait2")
    arrived(kbuf.at[xo], R_KF)
    arrived(vbuf.at[xo], R_VF)
    mark("serve")

    @pl.when(a == 0)
    def _():
        pair(1, xo)
        pair(3, xo)
        hand_on(1, False, True)
        hand_on(3, False, True)

    @pl.when(a == 1)
    def _():
        pair(1, xo)
        pair(2, xo)

    @pl.when(a == 2)
    def _():
        pair(1, xo)

    mark("lout1")

    @pl.when(a >= 1)
    def _():
        for d in range(1, 4):

            @pl.when(a == d)
            def _():
                arrived(sz.at[pl.ds(0, d)], R_SZ)

        linear_out()

    mark("hand")

    @pl.when(a == 1)
    def _():
        hand_on(1, False, False)
        hand_on(2, False, False)

    @pl.when(a == 2)
    def _():
        hand_on(1, False, False)

    mark("home")

    def triple(d):
        pair(d, xm)
        pair(d, xp)
        pair(d, xo)

    @pl.when((a == 0) & (b > 0))
    def _():
        pair(2, xo)
        hand_on(2, False, True)
        triple(0)
        hand_on(0, True, True)

    @pl.when((a == 0) & (b == 0))
    def _():
        pair(2, xo)
        hand_on(2, False, True)

    @pl.when(((a == 1) | (a == 2)) & (b > 0))
    def _():
        triple(0)
        hand_on(0, True, False)

    @pl.when((a == 3) & (b > 0))
    def _():
        pair(0, xo)
        hand_on(0, True, False)

    mark("linx")
    oll.wait()
    arrived(xl.at[pl.ds(0, 7)], R_LA)
    mark("linproj")
    lhs = jnp.concatenate([xl[i] for i in range(8)], axis=1)
    for n in range(4):
        cols = pl.ds(512 * n, 512)
        oacc[:, cols] = mm(lhs, ol[:, cols])

    mark("ret0")
    osl.wait()
    def returned(d, far):
        chip = lax.rem(y + far, 4)
        first, count = (2 * chip, 2) if d or far else (0, 1)

        @pl.when(a == d)
        def _():
            arrived(rbuf.at[pl.ds(8 * d + first, count), pl.ds(0, OUT_ROWS)], R_R + 4 * d + far)

        @pl.when(a > d)
        def _():
            arrived(rbuf.at[pl.ds(8 * d + first, count)], R_R + 4 * d + far)

    sub = iota((8, 128), 0)

    mark("stproj")

    @pl.when(a == 0)
    def _():
        for far in (0, 1, 3, 2):
            returned(0, far)
            first = 2 * lax.rem(y + far, 4)
            lhs = jnp.concatenate([rbuf[first + i, pl.ds(0, OUT_ROWS), :] for i in range(2)], axis=1)
            for n in range(4):
                cols = pl.ds(512 * n, 512)
                rows = pl.ds(pl.multiple_of(128 * first, 256), 256)
                total = oacc[:, cols] + mm(lhs, os_[rows, cols])
                if far == 2:
                    out[:, cols] = total.astype(BF16)
                else:
                    oacc[:, cols] = total

    @pl.when(a > 0)
    def _():
        for far in range(4):
            for d in range(4):
                returned(d, far)
        behind = jnp.zeros((8, 128), F32)
        heads = [rbuf[i, pl.ds(0, OUT_ROWS), :].astype(F32) for i in range(8)]
        for d in range(1, 4):
            for i in range(8):
                tail = rbuf[8 * d - 8 + i, pl.ds(OUT_ROWS, TAIL), :].astype(F32)
                behind = behind + jnp.where(sub == i, tail[0:1] + tail[1:2], 0.0)
            left = jnp.transpose(jnp.exp2(-behind))
            for i in range(8):
                more = left[:OUT_ROWS, i : i + 1] * rbuf[8 * d + i, pl.ds(0, OUT_ROWS), :].astype(F32)
                heads[i] = heads[i] + jnp.where(a >= d, more, 0.0)
        lhs = jnp.concatenate([h.astype(BF16) for h in heads], axis=1)
        for n in range(4):
            cols = pl.ds(512 * n, 512)
            out[:, cols] = (oacc[:, cols] + mm(lhs, os_[:, cols])).astype(BF16)

    mark("drain")
    sent(tok.at[pl.ds(0, 14)], S_TOK)
    sent(kbuf.at[pl.ds(0, 3)], S_K)
    sent(vbuf.at[pl.ds(0, 3)], S_V)
    sent(sx.at[pl.ds(0, 3)], S_SX)
    sent(xl.at[pl.ds(0, 7)], S_LA)

    @pl.when(a >= 1)
    def _():
        sent(qbuf.at[pl.ds(0, 2)], S_Q)

    for d in range(4):

        @pl.when(a == 3 - d)
        def _():
            if d:
                sent(sz.at[pl.ds(0, d)], S_SZ)
            pieces = sbuf.at[pl.ds(0, 7 + 8 * d)]
            sent(pieces if d < 3 else sbuf.at[pl.ds(0, 31), pl.ds(0, OUT_ROWS)], S_R)

    mark("")


def per_device(*args):
    args = list(args)
    args[1] = args[1].reshape(16, 128)
    args[6] = args[6].T
    args[9] = args[9].reshape(1, HD)
    vm = pltpu.VMEM
    return pl.pallas_call(
        kernel,
        out_shape=pltpu.VMEM((OUT_ROWS, D), BF16),
        in_specs=[pl.BlockSpec(memory_space=pl.ANY)] * 16,
        out_specs=pl.BlockSpec(memory_space=pltpu.VMEM),
        scratch_shapes=[
            vm((16, TOK, 128), BF16),
            vm((D, 1024), BF16),
            vm((32, D), BF16),
            vm((32, 128), BF16),
            vm((16, 128), BF16),
            vm((16, 128), F32),
            vm((TOK, 1024), F32),
            vm((TOK, 128), F32),
            vm((TOK, 128), F32),
            vm((1, TOK), BF16),
            vm((1, 128), F32),
            vm((1024, D), BF16),
            vm((1024, D), BF16),
            vm((128 * (LEVELS + 2), 128), BF16),
            vm((256, 256), BF16),
            vm((4, TOK + 16, 128), BF16),
            vm((4, TOK, 128), BF16),
            vm((4, TOK, 128), BF16),
            vm((TOK, 128), BF16),
            vm((TOK, 128), BF16),
            vm((TOK, 128), BF16),
            vm((TOK, 128), BF16),
            vm((TOK, 256), BF16),
            vm((TOK, 128), F32),
            vm((TOK, 128), F32),
            vm((CH, 128, 128), BF16),
            vm((TOK, 128), F32),
            vm((TOK, 128), BF16),
            vm((4, 144, 128), BF16),
            vm((4, 144, 128), BF16),
            vm((4, 4, TOK, 128), F32),
            vm((4, 4, TOK, 128), F32),
            vm((2, TOK, TOK), BF16),
            vm((32, OUT_ROWS + TAIL, 128), BF16),
            vm((32, OUT_ROWS + TAIL, 128), BF16),
            vm((TOK, 128), BF16),
            vm((8, OUT_ROWS, 128), BF16),
            vm((OUT_ROWS, D), F32),
            pltpu.SemaphoreType.DMA((10,)),
            pltpu.SemaphoreType.DMA((N_S,)),
            pltpu.SemaphoreType.DMA((N_R,)),
        ],
        compiler_params=pltpu.CompilerParams(collective_id=0, has_side_effects=True),
        name="layer",
    )(*args)


def solution(mesh):
    torus = Mesh(mesh.devices.reshape(4, 4, 4, 2), ("z", "x", "y", "c"))
    sp, tp = ("z", "x"), ("y", "c")
    placed = (
        P(sp, tp), P(), P(None, tp), P(None, tp), P(None, tp), P(None, tp), P(), P(), P(sp, tp), P(),
        P(None, tp), P(None, tp), P(None, tp), P(tp, sp), P(), P(),
    )
    return jax.shard_map(
        per_device, mesh=torus, in_specs=placed, out_specs=P(sp + tp, None), check_vma=False
    )
```

```python
import jax
import jax.numpy as jnp
from jax import lax
from jax.experimental import pallas as pl
from jax.experimental.pallas import tpu as pltpu
from jax.sharding import Mesh
from jax.sharding import PartitionSpec as P

MESH = pl.DeviceIdType.MESH
F32 = jnp.float32
BF16 = jnp.bfloat16
LOG2E = 1.4426950408889634
EPS = 1e-6
SOFT = 16.0
TOK = 384
D = 2048
HD = 128
PARTS = 3
ROWS = TOK // PARTS
KPARTS = 1
KROWS = TOK // KPARTS
CH = TOK // 128
LEVELS = 7
TAIL = 8
OUT_ROWS = TOK // 8

S_TOK, S_K, S_V, S_Q, S_SX, S_SZ, S_LA, S_R, N_S = range(9)
R_AB, R_BA, R_CD = 0, PARTS, 2 * PARTS
R_P0, R_PM, R_PP, R_PO, R_KN, R_VN, R_KF, R_VF, R_SX, R_Q2, R_Q3, R_SZ, R_LA = [3 * PARTS + i for i in range(13)]
R_K = R_LA + 1
R_V = R_K + KPARTS
R_Q = R_V + KPARTS
R_R = R_Q + KPARTS
N_R = R_R + 16


PROFILE = False


class Marks:
    current = None

    def __call__(self, name):
        if not PROFILE:
            return
        if self.current is not None:
            self.current.__exit__(None, None, None)
        self.current = jax.named_scope(name) if name else None
        if name:
            self.current.__enter__()


def nt(a, b):
    return lax.dot_general(a, b, (((1,), (1,)), ((), ())), preferred_element_type=F32)


def tn(a, b):
    return lax.dot_general(a, b, (((0,), (0,)), ((), ())), preferred_element_type=F32)


def mm(a, b):
    return jnp.dot(a, b, preferred_element_type=F32)


def iota(shape, dim):
    return lax.broadcasted_iota(jnp.int32, shape, dim)


def split(x):
    hi = x.astype(BF16)
    return hi, (x - hi.astype(F32)).astype(BF16)


def rows_of(pieces):
    io = iota((16, 128), 0)
    out = jnp.zeros((16, 128), F32)
    for r, piece in enumerate(pieces):
        out = jnp.where(io == r, piece.astype(F32), out)
    return out.astype(BF16)


def kernel(
    tokens, gain, w_lq, w_lk, w_lv, w_lg, w_gd, w_gu, dob, lgain, w_sq, w_sk, w_sv, kbias, w_ol, w_os,
    out,
    tok, wbuf, gd, gu, gb, gf, acc, ss, dbuf, kb, lng, ol, os_,
    mcon, tri, kbuf, vbuf, qbuf, lq, lk, lv, lg, gs, ffrom, fall, sthis, lacc, qx, sx, sz, pbuf, tbuf, shares, sbuf, rbuf,
    linb, xl, oacc,
    lsem, ssem, rsem,
):
    mark = Marks()
    a, b = lax.axis_index("z"), lax.axis_index("x")
    y, c = lax.axis_index("y"), lax.axis_index("c")
    tp = 2 * y + c
    oc = 1 - c
    scale = HD ** (-0.5)

    def local(src, dst, i):
        cp = pltpu.make_async_copy(src, dst, lsem.at[i])
        cp.start()
        return cp

    def remote(src, dst, i, j, **dev):
        return pltpu.make_async_remote_copy(
            src_ref=src, dst_ref=dst, send_sem=ssem.at[i], recv_sem=rsem.at[j],
            device_id=dev, device_id_type=MESH,
        )

    def send(src, dst, i, j, **dev):
        remote(src, dst, i, j, **dev).start()

    def arrived(dst, j):
        remote(dst, dst, 0, j, c=oc).wait_recv()

    def sent(src, i):
        remote(src, src, i, 0, c=oc).wait_send()

    mark("load")
    base = 4 * y + 2 * c
    local(tokens.at[:, pl.ds(0, 128)], tok.at[base], 0)
    local(tokens.at[:, pl.ds(128, 128)], tok.at[base + 1], 0)
    barrier = pltpu.get_barrier_semaphore()
    for k in range(1, 4):
        pl.semaphore_signal(barrier, inc=1, device_id={"x": lax.rem(b + k, 4)}, device_id_type=MESH)

    @pl.when(a <= 2)
    def _():
        pl.semaphore_signal(barrier, inc=1, device_id={"z": a + 1}, device_id_type=MESH)

    @pl.when(a == 0)
    def _():
        pl.semaphore_signal(barrier, inc=1, device_id={"z": 3}, device_id_type=MESH)

    for k in range(1, 8):
        r = lax.rem(tp + k, 8)
        pl.semaphore_signal(
            barrier, inc=1, device_id={"y": r // 2, "c": lax.rem(r, 2)}, device_id_type=MESH
        )
    weights = [w_sk, w_sq, w_sv, w_lk, w_lv, None, w_lq, w_lg]
    for i, w in enumerate(weights):
        if w is not None:
            local(w, wbuf.at[:, pl.ds(128 * i, 128)], 1)
    gdl = local(w_gd, gd, 2)
    gainl = local(gain, gb, 3)
    kbl = local(kbias, kb, 4)
    gul = local(w_gu.at[:, pl.ds(pl.multiple_of(128 * tp, 128), 128)], gu, 5)
    dobl = local(dob, dbuf, 6)
    lngl = local(lgain, lng, 7)
    oll = local(w_ol, ol, 8)
    osl = local(w_os, os_, 9)

    t_i, s_i = iota((128, 128), 0), iota((128, 128), 1)
    mcon[pl.ds(0, 128), :] = jnp.where(s_i <= t_i, 1.0, 0.0).astype(BF16)
    mcon[pl.ds(128, 128), :] = jnp.where(s_i > t_i, 1.0, 0.0).astype(BF16)
    mark("barrier")
    own = tok.at[pl.ds(base, 2)]
    pltpu.make_async_copy(own, own, lsem.at[0]).wait()
    pl.semaphore_wait(barrier, 10 + (a + 1) // 2)

    mark("send")
    yp, ym, yo = lax.rem(y + 1, 4), lax.rem(y + 3, 4), lax.rem(y + 2, 4)

    def part(first, count, r):
        return tok.at[pl.ds(first, count), pl.ds(ROWS * r, ROWS), :]

    def send_part(first, count, r, j, **dev):
        ref = part(first, count, r)
        send(ref, ref, S_TOK, j, **dev)

    for r in range(PARTS):
        send_part(base, 1, r, R_AB + r, y=yp)
        send_part(base + 1, 1, r, R_AB + r, y=ym)
    for r in range(PARTS):
        send_part(base, 2, r, R_P0, c=oc)
    send_part(base + 1, 1, 0, R_BA, y=yp)
    send_part(base, 1, 0, R_BA, y=ym)

    for lev in range(LEVELS):
        same = (t_i >> lev) == (s_i >> lev)
        second = ((t_i >> lev) & 1) == 1
        m = jnp.where(same, jnp.where(second, jnp.where(s_i <= t_i, 1.0, 0.0), jnp.where(s_i > t_i, 1.0, 0.0)), 0.0)
        mcon[pl.ds(256 + 128 * lev, 128), :] = m.astype(BF16)
    tri[...] = jnp.where(iota((256, 256), 0) > iota((256, 256), 1), 1.0, 0.0).astype(BF16)
    for g in range(4):
        pbuf[g, 0] = jnp.zeros((TOK, HD), F32)
        tbuf[g, 0] = jnp.zeros((TOK, HD), F32)
    gainl.wait()
    gf[...] = gb[...].astype(F32)
    kbl.wait()
    kbuf[b, pl.ds(TOK, 16), :] = rows_of([kb[:, pl.ds(128 * r, 128)] for r in range(CH)])
    gdl.wait()
    for i in range(16):
        down = gd[:, pl.ds(128 * i, 128)].astype(F32)
        square = jnp.concatenate([down, jnp.zeros((96, 128), F32)], axis=0)
        wbuf[pl.ds(128 * i, 128), pl.ds(640, 128)] = jnp.transpose(square).astype(BF16)
    seven = wbuf.at[:, pl.ds(0, 896)]
    pltpu.make_async_copy(seven, seven, lsem.at[1]).wait()

    def scaled(block, count, first=False):
        pieces = []
        for j in range(count):
            x = tok[block + j].astype(F32)
            sq = x * x
            ss[...] = sq if (first and j == 0) else ss[...] + sq
            pieces.append((x * gf[pl.ds(block + j, 1), :]).astype(BF16))
        return jnp.concatenate(pieces, axis=1)

    def weight_rows(block, count):
        return pl.ds(pl.multiple_of(128 * block, 128), 128 * count)

    def fold_blocks(block, count, first=False):
        lhs = scaled(block, count, first)
        for n in range(4):
            cols = pl.ds(256 * n, 256)
            add = mm(lhs, wbuf[weight_rows(block, count), cols])
            acc[:, cols] = add if first else acc[:, cols] + add

    def fold(chip, first=False):
        fold_blocks(4 * chip, 4, first)

    def fold_two(one, two):
        lhs = scaled(one, 1), scaled(two, 1)
        for n in range(4):
            cols = pl.ds(256 * n, 256)
            add = mm(lhs[0], wbuf[weight_rows(one, 1), cols]) + mm(lhs[1], wbuf[weight_rows(two, 1), cols])
            acc[:, cols] = acc[:, cols] + add

    def fold_half(chip, core):
        fold_blocks(4 * chip + 2 * core, 2)

    mark("own")

    def partner(chip, j):
        arrived(tok.at[pl.ds(4 * chip + 2 * oc, 2)], j)

    def pass_far(r):
        arrived(part(4 * yo + 2 * c, 2, r), R_CD + r)
        send_part(4 * yo + 2 * c, 2, r, R_PO, c=oc)

    partner(y, R_P0)
    fold(y, True)
    mark("fwd")
    for r in range(PARTS):
        arrived(part(4 * ym + 2 * c, 2, r), R_AB + r)
        send_part(4 * ym + 2 * c, 1, r, R_CD + r, y=yp)
        send_part(4 * yp + 2 * c + 1, 1, r, R_CD + r, y=ym)
        if r + 1 < PARTS:
            send_part(base + 1, 1, r + 1, R_BA + r + 1, y=yp)
            send_part(base, 1, r + 1, R_BA + r + 1, y=ym)
        send_part(4 * ym + 2 * c, 1, r, R_PM, c=oc)
        send_part(4 * yp + 2 * c + 1, 1, r, R_PP, c=oc)
    mark("fold1")
    fold_two(4 * ym + 2 * c, 4 * yp + 2 * c + 1)
    mark("fwd1")
    for r in range(PARTS):
        arrived(part(4 * ym + 2 * c, 2, r), R_BA + r)
        send_part(4 * ym + 2 * c + 1, 1, r, R_PM, c=oc)
        send_part(4 * yp + 2 * c, 1, r, R_PP, c=oc)
        pass_far(r)
    mark("fold2")
    fold_two(4 * ym + 2 * c + 1, 4 * yp + 2 * c)
    fold_half(yo, c)
    mark("fold3")
    partner(ym, R_PM)
    fold_half(ym, oc)
    partner(yp, R_PP)
    fold_half(yp, oc)
    mark("fwd2")
    partner(yo, R_PO)

    xp, xm, xo = lax.rem(b + 1, 4), lax.rem(b + 3, 4), lax.rem(b + 2, 4)

    def krows(g, r):
        return kbuf.at[g, pl.ds(KROWS * r, KROWS + (16 if r == KPARTS - 1 else 0))]

    def vrows(g, r):
        return vbuf.at[g, pl.ds(KROWS * r, KROWS)]

    def qrows(d, r):
        return qbuf.at[d, pl.ds(KROWS * r, KROWS)]

    mark("finish")
    last = 4 * yo + 2 * oc
    lhs = scaled(last, 2)
    inv = lax.rsqrt(jnp.sum(ss[...], axis=1, keepdims=True) * (1.0 / D) + EPS)

    def finish(n):
        cols = pl.ds(256 * n, 256)
        total = acc[:, cols] + mm(lhs, wbuf[weight_rows(last, 2), cols])
        return (total * inv).astype(BF16)

    got = finish(0)
    kbuf[b, pl.ds(0, TOK), :] = got[:, :128]
    qbuf[0] = got[:, 128:]
    for r in range(KPARTS):
        send(krows(b, r), krows(b, r), S_K, R_K + r, x=xp)
        send(krows(b, r), krows(b, r), S_K, R_KN, x=xm)

    @pl.when(a >= 1)
    def _():
        for r in range(KPARTS):
            send(qrows(0, r), qrows(1, r), S_Q, R_Q + r, z=a - 1)

    @pl.when(a == 3)
    def _():
        send(qbuf.at[0], qbuf.at[3], S_Q, R_Q3, z=0)

    got = finish(1)
    vbuf[b] = got[:, :128]
    lk[...] = got[:, 128:]
    for r in range(KPARTS):
        send(vrows(b, r), vrows(b, r), S_V, R_V + r, x=xm)
        send(vrows(b, r), vrows(b, r), S_V, R_VN, x=xp)
    got = finish(2)
    lv[...] = got[:, :128]
    low = got[:, 128:160]
    got = finish(3)
    lq[...] = got[:, :128]
    lg[...] = got[:, 128:]

    mark("lstate")
    gul.wait()
    dobl.wait()
    pre = (mm(low, gu[...]) + dbuf[...]) * LOG2E
    decay = (jnp.minimum(pre, 0.0) - jnp.log2(1.0 + jnp.exp2(-jnp.abs(pre)))) * (1.0 / SOFT)
    ghi, glo = split(decay)
    gboth = jnp.concatenate([ghi, glo], axis=1)
    gs[...] = gboth
    state = jnp.zeros((HD, HD), F32)
    before = jnp.zeros((1, HD), F32)
    for n in range(CH):
        rows = slice(128 * n, 128 * n + 128)
        both = mm(mcon[pl.ds(0, 256), :], gboth[rows])
        dist = both[:, :128] + both[:, 128:]
        fade = jnp.exp2(dist)
        ffrom[rows, :] = fade[:128]
        fall[rows, :] = fade[:128] * jnp.exp2(before)
        if n:
            sthis[n] = state.astype(BF16)
        length = dist[127:128]
        ke = (lk[rows, :].astype(F32) * fade[128:]).astype(BF16)
        state = state * jnp.exp2(length) + tn(lv[rows, :], ke)
        before = before + length
    sx[b, pl.ds(0, HD), :] = state.astype(BF16)
    sx[b, pl.ds(HD, 16), :] = rows_of(split(before))
    for k in range(1, 4):
        send(sx.at[b], sx.at[b], S_SX, R_SX, x=lax.rem(b + k, 4))

    def linear_inside():
        apart = t_i ^ s_i
        for n in range(CH):
            rows = slice(128 * n, 128 * n + 128)
            both = mm(mcon[pl.ds(256, 128 * LEVELS), :], gs[rows, :])
            fade = jnp.exp2(both[:, :128] + both[:, 128:])
            qh, kh, vh = lq[rows, :], lk[rows, :], lv[rows, :]
            qf, kf = qh.astype(F32) * scale, kh.astype(F32)
            score = jnp.where(apart == 0, nt(qh, kh) * scale, 0.0)
            for lev in range(LEVELS):
                e = fade[128 * lev : 128 * lev + 128]
                part_score = nt((qf * e).astype(BF16), (kf * e).astype(BF16))
                score = jnp.where(((apart >> lev) == 1) & (t_i > s_i), part_score, score)
            inner = mm(score.astype(BF16), vh)
            if n:
                inner = inner + nt((qf * ffrom[rows, :]).astype(BF16), sthis[n])
            lacc[rows, :] = inner
            qx[rows, :] = (qf * fall[rows, :]).astype(BF16)

    mark("diag")
    def bias_of(g):
        head = kbuf[g, pl.ds(TOK, 16), :].astype(F32) * LOG2E
        return jnp.concatenate([head[r : r + 1] for r in range(CH)], axis=1)

    def pair(d, g, diagonal=False, slot=None):
        z = nt(qbuf[d], kbuf[g, pl.ds(0, TOK), :]) * (scale * LOG2E) + bias_of(g)
        soft = jnp.maximum(jnp.log2(1.0 + jnp.exp2(jnp.minimum(z, 126.0))), z)
        own = z - soft
        if diagonal:
            seen = iota((TOK, TOK), 1) < iota((TOK, TOK), 0)
            soft = jnp.where(seen, soft, 0.0)
        sb = soft.astype(BF16)
        near = mm(sb[:, 256:], tri[pl.ds(0, 128), pl.ds(0, 128)])
        near_total = near[:, :1] + soft[:, 256:257]
        far = mm(sb[:, :256], tri[...]) + near_total
        whole = far[:, :1] + soft[:, :1]
        share = jnp.exp2(own - jnp.concatenate([far, near], axis=1))
        if diagonal:
            share = jnp.where(seen, share, 0.0)
        tbuf[g, d] = jnp.broadcast_to(whole, (TOK, HD))
        if slot is None:
            pbuf[g, d] = mm(share.astype(BF16), vbuf[g])
        else:
            shares[slot] = share.astype(BF16)

    pair(0, b, True)

    def pass_keys(r):
        arrived(krows(xm, r), R_K + r)
        send(krows(xm, r), krows(xm, r), S_K, R_KF, x=xp)

    def pass_values(r):
        arrived(vrows(xp, r), R_V + r)
        send(vrows(xp, r), vrows(xp, r), S_V, R_VF, x=xm)

    def pass_queries(r):
        @pl.when(a <= 2)
        def _():
            arrived(qrows(1, r), R_Q + r)

        @pl.when((a >= 1) & (a <= 2))
        def _():
            send(qrows(1, r), qrows(2, r), S_Q, R_Q2, z=a - 1)

    lane = iota((16, 128), 1)

    def hand_on(d, home, oldest):
        def counted(g, value):
            return jnp.where(g <= b, value, 0.0) if home else value

        total, behind = counted(3, pbuf[3, d]), counted(3, tbuf[3, d])
        for g in range(2, -1, -1):
            total = total + counted(g, jnp.exp2(-behind) * pbuf[g, d])
            if g or not oldest:
                behind = behind + counted(g, tbuf[g, d])
        for r in range(8):
            sbuf[8 * d + r, pl.ds(0, OUT_ROWS), :] = total[OUT_ROWS * r : OUT_ROWS * r + OUT_ROWS].astype(BF16)

        def leave(rows):
            for far in range(4):
                for flip in range(2):
                    to_y, to_c = lax.rem(y + 4 - far, 4), c if flip == 0 else oc
                    r = 2 * to_y + to_c
                    if home and far == 0 and flip == 0:
                        rbuf[tp] = sbuf[tp]
                        continue
                    dev = {"y": to_y, "c": to_c}
                    if not home:
                        dev["z"] = a + d
                    src, dst = sbuf.at[8 * d + r, pl.ds(0, rows)], rbuf.at[8 * d + tp, pl.ds(0, rows)]
                    send(src, dst, S_R, R_R + 4 * d + far, **dev)

        if oldest:
            leave(OUT_ROWS)
            return
        tiles = []
        for r in range(CH):
            line = jnp.transpose(behind[128 * r : 128 * r + 128])[0:1]
            tiles.append(rows_of(split(line)).astype(F32))
        for r in range(8):
            j, o = (OUT_ROWS * r) // 128, (OUT_ROWS * r) % 128
            tail = pltpu.roll(tiles[j], 128 - o, 1) if o else tiles[j]
            if o + OUT_ROWS > 128:
                tail = jnp.where(lane < 128 - o, tail, pltpu.roll(tiles[j + 1], 128 - o, 1))
            sbuf[8 * d + r, pl.ds(OUT_ROWS, TAIL), :] = tail[:TAIL].astype(BF16)
        leave(OUT_ROWS + TAIL)

    mark("home0")

    @pl.when((b == 0) & (a == 0))
    def _():
        hand_on(0, True, True)

    @pl.when((b == 0) & (a > 0))
    def _():
        hand_on(0, True, False)

    mark("linear1")
    linear_inside()
    mark("kvfwd")
    for r in range(KPARTS):
        pass_queries(r)
        pass_keys(r)
    mark("first")
    arrived(kbuf.at[xp], R_KN)

    @pl.when(a <= 2)
    def _():
        pair(1, b)
        pair(1, xm, slot=0)
        pair(1, xp, slot=1)

    @pl.when(a == 3)
    def _():
        pair(0, xm, slot=0)
        pair(0, xp, slot=1)

    mark("kvwait")
    for r in range(KPARTS):
        pass_values(r)
    mark("q3")

    @pl.when(a == 0)
    def _():
        arrived(qbuf.at[3], R_Q3)
        pair(3, b)

    arrived(vbuf.at[xm], R_VN)

    def values_in(d):
        pbuf[xm, d] = mm(shares[0], vbuf[xm])
        pbuf[xp, d] = mm(shares[1], vbuf[xp])

    mark("more")

    @pl.when(a == 0)
    def _():
        values_in(1)
        pair(3, xm)
        pair(3, xp)
        arrived(qbuf.at[2], R_Q2)
        pair(2, b)

    @pl.when((a == 1) | (a == 2))
    def _():
        values_in(1)

    @pl.when(a == 3)
    def _():
        values_in(0)

    mark("states")
    arrived(sx.at[pl.ds(0, 3)], R_SX)
    run = jnp.zeros((HD, HD), F32)
    run_len = jnp.zeros((1, HD), F32)
    pre_state, pre_len = run, run_len
    for g in range(4):
        pre_state = jnp.where(b == g, run, pre_state)
        pre_len = jnp.where(b == g, run_len, pre_len)
        tail = sx[g, pl.ds(HD, 16), :].astype(F32)
        length = tail[0:1] + tail[1:2]
        run = run * jnp.exp2(length) + sx[g, pl.ds(0, HD), :].astype(F32)
        run_len = run_len + length
    sz[a, pl.ds(0, HD), :] = run.astype(BF16)
    sz[a, pl.ds(HD, 16), :] = rows_of(split(run_len))
    for d in (3, 1):

        @pl.when(a + d <= 3)
        def _():
            send(sz.at[a], sz.at[a], S_SZ, R_SZ, z=a + d)

    @pl.when(a == 1)
    def _():
        arrived(qbuf.at[2], R_Q2)

    @pl.when(a <= 1)
    def _():
        send(sz.at[a], sz.at[a], S_SZ, R_SZ, z=a + 2)

    def add_group(g, carried):
        tail = sz[g, pl.ds(HD, 16), :].astype(F32)
        return carried * jnp.exp2(tail[0:1] + tail[1:2]) + sz[g, pl.ds(0, HD), :].astype(F32)

    def span(r):
        return pl.ds(pl.multiple_of(OUT_ROWS * r, 16), OUT_ROWS)

    lngl.wait()

    def linear_out():
        older = lax.fori_loop(0, a, add_group, jnp.zeros((HD, HD), F32))
        incoming = pre_state + older * jnp.exp2(pre_len)
        raw = lacc[...] + nt(qx[...], incoming.astype(BF16))
        normed = raw * lax.rsqrt(jnp.mean(raw * raw, axis=1, keepdims=True) + EPS) * lng[...]
        gate = lg[...].astype(F32)
        linb[...] = (normed * (gate / (1.0 + jnp.exp2(gate * (-LOG2E))))).astype(BF16)
        for k in range(1, 8):
            r = lax.rem(tp + k, 8)
            send(linb.at[span(r)], xl.at[tp], S_LA, R_LA, y=r // 2, c=lax.rem(r, 2))
        xl[tp] = linb[span(tp), :]

    mark("lout0")

    @pl.when(a == 1)
    def _():
        pair(2, b)
        pair(2, xm)
        pair(2, xp)

    @pl.when(a == 0)
    def _():
        linear_out()
        pair(2, xm)
        pair(2, xp)

    mark("kvwait2")
    arrived(kbuf.at[xo], R_KF)
    arrived(vbuf.at[xo], R_VF)
    mark("serve")

    @pl.when(a == 0)
    def _():
        pair(1, xo)
        pair(3, xo)
        hand_on(1, False, True)
        hand_on(3, False, True)

    @pl.when(a == 1)
    def _():
        pair(1, xo)
        pair(2, xo)

    @pl.when(a == 2)
    def _():
        pair(1, xo)

    mark("lout1")

    @pl.when(a >= 1)
    def _():
        for d in range(1, 4):

            @pl.when(a == d)
            def _():
                arrived(sz.at[pl.ds(0, d)], R_SZ)

        linear_out()

    mark("hand")

    @pl.when(a == 1)
    def _():
        hand_on(1, False, False)
        hand_on(2, False, False)

    @pl.when(a == 2)
    def _():
        hand_on(1, False, False)

    mark("home")

    def triple(d):
        pair(d, xm)
        pair(d, xp)
        pair(d, xo)

    @pl.when((a == 0) & (b > 0))
    def _():
        pair(2, xo)
        hand_on(2, False, True)
        triple(0)
        hand_on(0, True, True)

    @pl.when((a == 0) & (b == 0))
    def _():
        pair(2, xo)
        hand_on(2, False, True)

    @pl.when(((a == 1) | (a == 2)) & (b > 0))
    def _():
        triple(0)
        hand_on(0, True, False)

    @pl.when((a == 3) & (b > 0))
    def _():
        pair(0, xo)
        hand_on(0, True, False)

    mark("linx")
    oll.wait()
    arrived(xl.at[pl.ds(0, 7)], R_LA)
    mark("linproj")
    lhs = jnp.concatenate([xl[i] for i in range(8)], axis=1)
    for n in range(4):
        cols = pl.ds(512 * n, 512)
        oacc[:, cols] = mm(lhs, ol[:, cols])

    mark("ret0")
    osl.wait()
    def returned(d, far):
        chip = lax.rem(y + far, 4)
        first, count = (2 * chip, 2) if d or far else (0, 1)

        @pl.when(a == d)
        def _():
            arrived(rbuf.at[pl.ds(8 * d + first, count), pl.ds(0, OUT_ROWS)], R_R + 4 * d + far)

        @pl.when(a > d)
        def _():
            arrived(rbuf.at[pl.ds(8 * d + first, count)], R_R + 4 * d + far)

    sub = iota((8, 128), 0)

    mark("stproj")

    @pl.when(a == 0)
    def _():
        for far in (0, 1, 3, 2):
            returned(0, far)
            first = 2 * lax.rem(y + far, 4)
            lhs = jnp.concatenate([rbuf[first + i, pl.ds(0, OUT_ROWS), :] for i in range(2)], axis=1)
            for n in range(4):
                cols = pl.ds(512 * n, 512)
                rows = pl.ds(pl.multiple_of(128 * first, 256), 256)
                total = oacc[:, cols] + mm(lhs, os_[rows, cols])
                if far == 2:
                    out[:, cols] = total.astype(BF16)
                else:
                    oacc[:, cols] = total

    @pl.when(a > 0)
    def _():
        for far in range(4):
            for d in range(4):
                returned(d, far)
        behind = jnp.zeros((8, 128), F32)
        heads = [rbuf[i, pl.ds(0, OUT_ROWS), :].astype(F32) for i in range(8)]
        for d in range(1, 4):
            for i in range(8):
                tail = rbuf[8 * d - 8 + i, pl.ds(OUT_ROWS, TAIL), :].astype(F32)
                behind = behind + jnp.where(sub == i, tail[0:1] + tail[1:2], 0.0)
            left = jnp.transpose(jnp.exp2(-behind))
            for i in range(8):
                more = left[:OUT_ROWS, i : i + 1] * rbuf[8 * d + i, pl.ds(0, OUT_ROWS), :].astype(F32)
                heads[i] = heads[i] + jnp.where(a >= d, more, 0.0)
        lhs = jnp.concatenate([h.astype(BF16) for h in heads], axis=1)
        for n in range(4):
            cols = pl.ds(512 * n, 512)
            out[:, cols] = (oacc[:, cols] + mm(lhs, os_[:, cols])).astype(BF16)

    mark("drain")
    sent(tok.at[pl.ds(0, 14)], S_TOK)
    sent(kbuf.at[pl.ds(0, 3)], S_K)
    sent(vbuf.at[pl.ds(0, 3)], S_V)
    sent(sx.at[pl.ds(0, 3)], S_SX)
    sent(xl.at[pl.ds(0, 7)], S_LA)

    @pl.when(a >= 1)
    def _():
        sent(qbuf.at[pl.ds(0, 2)], S_Q)

    for d in range(4):

        @pl.when(a == 3 - d)
        def _():
            if d:
                sent(sz.at[pl.ds(0, d)], S_SZ)
            pieces = sbuf.at[pl.ds(0, 7 + 8 * d)]
            sent(pieces if d < 3 else sbuf.at[pl.ds(0, 31), pl.ds(0, OUT_ROWS)], S_R)

    mark("")


def per_device(*args):
    args = list(args)
    args[1] = args[1].reshape(16, 128)
    args[6] = args[6].T
    args[9] = args[9].reshape(1, HD)
    vm = pltpu.VMEM
    return pl.pallas_call(
        kernel,
        out_shape=pltpu.VMEM((OUT_ROWS, D), BF16),
        in_specs=[pl.BlockSpec(memory_space=pl.ANY)] * 16,
        out_specs=pl.BlockSpec(memory_space=pltpu.VMEM),
        scratch_shapes=[
            vm((16, TOK, 128), BF16),
            vm((D, 1024), BF16),
            vm((32, D), BF16),
            vm((32, 128), BF16),
            vm((16, 128), BF16),
            vm((16, 128), F32),
            vm((TOK, 1024), F32),
            vm((TOK, 128), F32),
            vm((TOK, 128), F32),
            vm((1, TOK), BF16),
            vm((1, 128), F32),
            vm((1024, D), BF16),
            vm((1024, D), BF16),
            vm((128 * (LEVELS + 2), 128), BF16),
            vm((256, 256), BF16),
            vm((4, TOK + 16, 128), BF16),
            vm((4, TOK, 128), BF16),
            vm((4, TOK, 128), BF16),
            vm((TOK, 128), BF16),
            vm((TOK, 128), BF16),
            vm((TOK, 128), BF16),
            vm((TOK, 128), BF16),
            vm((TOK, 256), BF16),
            vm((TOK, 128), F32),
            vm((TOK, 128), F32),
            vm((CH, 128, 128), BF16),
            vm((TOK, 128), F32),
            vm((TOK, 128), BF16),
            vm((4, 144, 128), BF16),
            vm((4, 144, 128), BF16),
            vm((4, 4, TOK, 128), F32),
            vm((4, 4, TOK, 128), F32),
            vm((2, TOK, TOK), BF16),
            vm((32, OUT_ROWS + TAIL, 128), BF16),
            vm((32, OUT_ROWS + TAIL, 128), BF16),
            vm((TOK, 128), BF16),
            vm((8, OUT_ROWS, 128), BF16),
            vm((OUT_ROWS, D), F32),
            pltpu.SemaphoreType.DMA((10,)),
            pltpu.SemaphoreType.DMA((N_S,)),
            pltpu.SemaphoreType.DMA((N_R,)),
        ],
        compiler_params=pltpu.CompilerParams(collective_id=0, has_side_effects=True),
        name="layer",
    )(*args)


def solution(mesh):
    torus = Mesh(mesh.devices.reshape(4, 4, 4, 2), ("z", "x", "y", "c"))
    sp, tp = ("z", "x"), ("y", "c")
    placed = (
        P(sp, tp), P(), P(None, tp), P(None, tp), P(None, tp), P(None, tp), P(), P(), P(sp, tp), P(),
        P(None, tp), P(None, tp), P(None, tp), P(tp, sp), P(), P(),
    )
    return jax.shard_map(
        per_device, mesh=torus, in_specs=placed, out_specs=P(sp + tp, None), check_vma=False
    )
```
